1024 devices in a mesh: ep: 64 (over z, y), tp: 16 (over x, core).
Axes of the slice: x: 8, y: 8, z: 8, core: 2. Of those that a mesh axis runs over, the one named last changes fastest.
Arguments:
- tokens: bfloat16 [8192, 2048], P('ep'), may hold values from -6 to 6
- cotangent: bfloat16 [8192, 2048], P('ep'), may hold values from -0.796875 to 0.796875
- mix_weights: bfloat16 [8192, 2], P('ep'), may hold values from 0.049804688 to 1
- routes: int32 [8192, 2], P('ep'), may hold values from 0 to 63, all different within a row; in each aligned block of 128 rows (0 to 127, 128 to 255, ...) at most 5 rows name the same one
- gate_proj: bfloat16 [64, 2048, 2048], P('ep', None, 'tp'), may hold values from -0.125 to 0.125
- up_proj: bfloat16 [64, 2048, 2048], P('ep', None, 'tp'), may hold values from -0.125 to 0.125
- down_proj: bfloat16 [64, 2048, 2048], P('ep', 'tp'), may hold values from -0.125 to 0.125
Outputs:
- token_grad: bfloat16 [8192, 2048], P('ep', 'tp')
- mix_grad: bfloat16 [8192, 2], P('ep')
- gate_grad: bfloat16 [64, 2048, 2048], P('ep', None, 'tp')
- up_grad: bfloat16 [64, 2048, 2048], P('ep', None, 'tp')
- down_grad: bfloat16 [64, 2048, 2048], P('ep', 'tp')
The draws below stay inside these ranges and needn't reach their ends.
Inputs may be any that keep to these rules, and one draw needn't show every extreme that they name: `routes`: each row names 2 different experts; in each aligned block of 128 rows (the rows of one device) no expert is named more than 5 times, a bound that some block reaches.
All inputs are finite; a program needn't handle non-finite values.
Results may differ from the reference program's by a relative error of at most 0.018.
Values may be sent and summed in bfloat16 or wider, within the bound.
A program may use at most 128 MiB of HBM per device.

```python
import math
import jax
import jax.numpy as jnp
import numpy as np
from jax import lax

D = 2048
FF = 2048
TOPK = 2
TOK_DEV = 128
EXPERTS = 64
TOKENS = 8192
CAP = 5
FF_DEV = 128
N_EP = 64
N_TP = 16


def steps_of(rng, shape, shards, low, top_value):
    loudness = 1.0
    for dim, shards_of in shards:
        heights = jax.random.uniform(jax.random.fold_in(jax.random.fold_in(rng, 6), dim), (shards_of,), jnp.float32, low / len(shards), top_value / len(shards))
        loudness = loudness * jnp.repeat(jnp.exp(heights), shape[dim] // shards_of).reshape((-1,) + (1,) * (len(shape) - 1 - dim))
    return loudness


def routed_block(own_key, own, number, rows, count, top, bound, slope):
    order = jax.random.permutation(own_key, count)
    heavy_load, usual = portions_of(count, rows * top, bound, slope, True), portions_of(count, rows * top, bound, slope, False)
    places = jnp.arange(count)

    def named(lengths, rotation):
        used = int((lengths > 0).sum())
        fixed = max(1, used // 4)
        shifted = fixed + (places - fixed + rotation * (used - fixed)) % max(1, count - fixed)
        return jnp.zeros((count,), jnp.int32).at[order[jnp.where(places < fixed, places, shifted)]].set(jnp.asarray(lengths, jnp.int32))

    lengths = jnp.where(number % 4 == 0, named(heavy_load, number // 4), named(usual, number - number // 4 - 1))
    mixed = jax.random.permutation(jax.random.fold_in(own, 3), count)
    giver, taker = mixed[0:count // 2 * 2:2], mixed[1:count // 2 * 2:2]
    room = jnp.minimum(lengths[giver] - 1, bound - lengths[taker]) // 2
    room = jnp.where((giver == order[0]) | (taker == order[0]) | (lengths[taker] == 0), 0, jnp.maximum(room, 0))
    shifted = jax.random.randint(jax.random.fold_in(own, 4), (count // 2,), 0, 1 << 20) % (room + 1)
    lengths = lengths.at[giver].add(-shifted).at[taker].add(shifted)
    labels = jnp.searchsorted(jnp.cumsum(lengths), jnp.arange(rows * top), side="right").astype(jnp.int32)
    listing = labels.reshape(top, rows).T
    listing = listing[jax.random.permutation(jax.random.fold_in(own, 1), rows)]
    rotation = jax.random.randint(jax.random.fold_in(own, 2), (rows, 1), 0, top)
    return jnp.take_along_axis(listing, (jnp.arange(top)[None, :] + rotation) % top, axis=1)


def portions_of(amount, total, reach, slope, full):
    loads = [(1 << 20) // math.isqrt(rank ** slope) + 1 for rank in range(1, amount + 1)]
    largest = reach if full else min(reach, max(-(-total // amount), total * loads[0] // sum(loads)))
    least = 1 if total - largest >= amount - 1 else 0
    counts, spare = [largest] + [least] * (amount - 1), total - largest - least * (amount - 1)
    while spare > 0:
        candidates = [i for i in range(1, amount) if counts[i] < largest] or [i for i in range(1, amount) if counts[i] < reach]
        pool, budget = sum([loads[i] for i in candidates]), spare
        for i in candidates:
            addition = min(reach - counts[i], max(1, budget * loads[i] // pool), spare)
            counts[i] = counts[i] + addition
            spare = spare - addition
    return np.array(counts)


def noise(stream_key, shape, deviation, bound, split=(), kind=jnp.bfloat16):
    result = deviation * jax.random.normal(stream_key, shape, jnp.float32)
    if split:
        result = result * steps_of(stream_key, shape, split, -0.22, 0.18)
    return jnp.clip(result, -bound, bound).astype(kind)


def setup_inputs(seed: int = 0) -> dict:
    arg_keys = jax.random.split(jax.random.key(seed), 8)
    tokens = noise(arg_keys[0], (TOKENS, D), 1.0, 6.0, ((0, 64),))
    cotangent = noise(arg_keys[1], (TOKENS, D), 0.1, 0.796875, ((0, 64),))
    mix_weights = jnp.clip(jnp.exp(math.log(1.0) - 2.9996462 * jax.random.uniform(arg_keys[2], (TOKENS, TOPK), jnp.float32) ** steps_of(arg_keys[2], (TOKENS, TOPK), ((0, 64),), -0.2, 0.2)), 0.049804688, 1.0).astype(jnp.bfloat16)
    routes_keys = jax.random.split(jax.random.fold_in(arg_keys[3], 1), TOKENS // TOK_DEV)
    routes_turns = jax.random.permutation(jax.random.fold_in(arg_keys[3], 3), TOKENS // TOK_DEV)
    routes = jax.vmap(lambda own, number: routed_block(jax.random.fold_in(arg_keys[3], 2), own, number, TOK_DEV, EXPERTS, TOPK, CAP, 1))(routes_keys, routes_turns).reshape((TOKENS, TOPK))
    gate_proj = noise(arg_keys[4], (EXPERTS, D, FF), D ** -0.5, 0.125, ((0, 64), (2, 16)))
    up_proj = noise(arg_keys[5], (EXPERTS, D, FF), D ** -0.5, 0.125, ((0, 64), (2, 16)))
    down_proj = noise(arg_keys[6], (EXPERTS, FF, D), FF ** -0.5, 0.125, ((0, 64), (1, 16)))
    return {"tokens": tokens, "cotangent": cotangent, "mix_weights": mix_weights, "routes": routes, "gate_proj": gate_proj, "up_proj": up_proj, "down_proj": down_proj}


def silu_slope(pre):
    sig = jax.nn.sigmoid(pre)
    return sig * (1.0 + pre * (1.0 - sig))


def pair_table(routes):
    pairs = TOKENS * TOPK
    flat = routes.reshape(-1).astype(jnp.int32)
    onehot = (flat[:, None] == jnp.arange(EXPERTS, dtype=jnp.int32)[None, :]).astype(jnp.int32)
    blocks = onehot.reshape(N_EP, TOK_DEV * TOPK, EXPERTS)
    before = jnp.cumsum(blocks, axis=1) - blocks
    rank = jnp.sum(before * blocks, axis=2).reshape(-1).astype(jnp.int32)
    source = jnp.arange(pairs, dtype=jnp.int32) // (TOK_DEV * TOPK)
    position = (source * CAP + rank).astype(jnp.int32)
    table = jnp.full((EXPERTS, N_EP * CAP), pairs, jnp.int32)
    return table.at[flat, position].set(jnp.arange(pairs, dtype=jnp.int32))


def reference(tokens, cotangent, mix_weights, routes, gate_proj, up_proj, down_proj):
    pairs = TOKENS * TOPK
    table = pair_table(routes)
    zero_row = jnp.zeros((1, D), jnp.bfloat16)
    token_pad = jnp.concatenate([tokens, zero_row], 0)
    back_pad = jnp.concatenate([cotangent, zero_row], 0)
    mix_pad = jnp.concatenate([mix_weights.reshape(-1), jnp.zeros((1,), jnp.bfloat16)], 0)

    def one_expert(inputs):
        ids, gate_w, up_w, down_w = inputs
        rows = token_pad[ids // TOPK]
        backs = back_pad[ids // TOPK]
        weight = mix_pad[ids].astype(jnp.float32)[:, None]
        pre_gate = jnp.dot(rows, gate_w, preferred_element_type=jnp.float32)
        pre_up = jnp.dot(rows, up_w, preferred_element_type=jnp.float32)
        active = jax.nn.silu(pre_gate)
        hidden = (active * pre_up).astype(jnp.bfloat16)
        back_hidden = lax.dot_general(backs, down_w, (((1,), (1,)), ((), ())), preferred_element_type=jnp.float32)
        pair_mix = jnp.sum(hidden.astype(jnp.float32) * back_hidden, axis=1).astype(jnp.bfloat16)
        weighted = (weight * hidden.astype(jnp.float32)).astype(jnp.bfloat16)
        down_e = lax.dot_general(weighted, backs, (((0,), (0,)), ((), ())), preferred_element_type=jnp.float32).astype(jnp.bfloat16)
        scaled = weight * back_hidden
        back_gate = (scaled * pre_up * silu_slope(pre_gate)).astype(jnp.bfloat16)
        back_up = (scaled * active).astype(jnp.bfloat16)
        gate_e = lax.dot_general(rows, back_gate, (((0,), (0,)), ((), ())), preferred_element_type=jnp.float32).astype(jnp.bfloat16)
        up_e = lax.dot_general(rows, back_up, (((0,), (0,)), ((), ())), preferred_element_type=jnp.float32).astype(jnp.bfloat16)
        count = ids.shape[0]
        split_gate = back_gate.astype(jnp.float32).reshape(count, N_TP, FF_DEV)
        split_up = back_up.astype(jnp.float32).reshape(count, N_TP, FF_DEV)
        gate_cols = gate_w.astype(jnp.float32).reshape(D, N_TP, FF_DEV)
        up_cols = up_w.astype(jnp.float32).reshape(D, N_TP, FF_DEV)
        parts = jnp.einsum('rtf,dtf->trd', split_gate, gate_cols) + jnp.einsum('rtf,dtf->trd', split_up, up_cols)
        parts = lax.optimization_barrier(parts.astype(jnp.bfloat16))
        pair_grad = jnp.sum(parts.astype(jnp.float32), axis=0).astype(jnp.bfloat16)
        return pair_grad, pair_mix, gate_e, up_e, down_e

    pair_grad, pair_mix, gate_grad, up_grad, down_grad = lax.map(one_expert, (table, gate_proj, up_proj, down_proj))
    ids = table.reshape(-1)
    summed = jnp.zeros((pairs + 1, D), jnp.float32).at[ids].add(pair_grad.reshape(-1, D).astype(jnp.float32))
    token_grad = jnp.sum(summed[:pairs].reshape(TOKENS, TOPK, D), axis=1).astype(jnp.bfloat16)
    mix_flat = jnp.zeros((pairs + 1,), jnp.bfloat16).at[ids].set(pair_mix.reshape(-1))
    mix_grad = mix_flat[:pairs].reshape(TOKENS, TOPK)
    return token_grad, mix_grad, gate_grad, up_grad, down_grad
```

```python
import functools

import jax
import jax.numpy as jnp
from jax import lax
from jax.experimental import pallas as pl
from jax.experimental.pallas import tpu as pltpu
from jax.sharding import PartitionSpec as P

MESH = pl.DeviceIdType.MESH
BF = jnp.bfloat16
F32 = jnp.float32
CAP = 5
LANES = 128
GROUPS = 4
MSG = 2 * CAP


def iota(shape, dim):
    return lax.broadcasted_iota(jnp.int32, shape, dim)


def dot(a, b):
    return jnp.dot(a, b, preferred_element_type=F32)


def dot_nt(a, b):
    return lax.dot_general(a, b, (((1,), (1,)), ((), ())), preferred_element_type=F32)


def dot_tn(a, b):
    return lax.dot_general(a, b, (((0,), (0,)), ((), ())), preferred_element_type=F32)


def div5(v):
    return (v * 205) >> 10


def kernel(
    nep, nx, ny, stage,
    tok_hbm, cot_hbm, routes_ref, mix_ref, gate_hbm, up_hbm, down_hbm,
    tg_ref, mg_ref, gt_ref, ut_ref, dg_ref,
    share, msg, rcv, rows, gate, up, down, acc, p8, aux, perm, bgu, hid,
    pown, psend, psib, sbr, sbl, rl, rr, mixv, mixs, ret, out,
    sh_sem, w_sem, d_send, d_recv, ag_rs, ag_rh, ag_ls, ag_lh, ag_ss, ag_l, ag_r, ag_s,
    ps_send, ps_recv, rs_send, rs_l, rs_r, mx_ss, mx_sr, mx_send, mx_recv, rt_send, rt_recv,
):
    e = lax.axis_index("ep")
    t = lax.axis_index("tp")
    x = t // 2
    c = t % 2
    nz = nep // ny
    z, y = e // ny, e % ny
    per = nep // GROUPS
    rpg = per * CAP
    tokn = share.shape[1]
    far = nx // 2

    def chip(d):
        return lax.rem(x + d + nx, nx)

    right = chip(1) * 2 + c
    left = chip(-1) * 2 + c
    sib = x * 2 + (1 - c)

    col = pl.multiple_of(t * LANES, LANES)
    share_copies = [
        pltpu.make_async_copy(tok_hbm.at[:, pl.ds(col, LANES)], share.at[0], sh_sem.at[0]),
        pltpu.make_async_copy(cot_hbm.at[:, pl.ds(col, LANES)], share.at[1], sh_sem.at[1]),
    ]
    for cp in share_copies:
        cp.start()
    weight_copies = [
        pltpu.make_async_copy(gate_hbm.at[0], gate, w_sem.at[0]),
        pltpu.make_async_copy(up_hbm.at[0], up, w_sem.at[1]),
        pltpu.make_async_copy(down_hbm.at[0], down, w_sem.at[2]),
    ]

    rcv[...] = jnp.zeros_like(rcv)
    mixv[...] = jnp.zeros_like(mixv)

    barrier = pltpu.get_barrier_semaphore()

    def order(j, n):
        half = (j + 1) // 2
        return lax.rem(n // 2 + (1 - 2 * (j % 2)) * half + n, n)

    def peer(j):
        dz, dy = order(j // ny, nz), order(j % ny, ny)
        return lax.rem(z + dz, nz) * ny + lax.rem(y + dy, ny)

    def greet(j, carry):
        pl.semaphore_signal(barrier, inc=1, device_id=(peer(j), t), device_id_type=MESH)
        return carry

    lax.fori_loop(0, nep - 1, greet, 0)
    for d in range(1, nx):
        pl.semaphore_signal(barrier, inc=1, device_id=(e, chip(d) * 2 + c), device_id_type=MESH)
    pl.semaphore_signal(barrier, inc=1, device_id=(e, sib), device_id_type=MESH)

    for cp in weight_copies:
        cp.start()

    r0, r1 = routes_ref[0:1, :], routes_ref[1:2, :]
    w = mix_ref[...].astype(F32)
    w0, w1 = w[0:1, :], w[1:2, :]
    upper = (iota((tokn, tokn), 0) < iota((tokn, tokn), 1)).astype(BF)
    er = iota((nep, tokn), 0)
    oh0, oh1 = er == r0, er == r1
    ranks = dot((oh0 | oh1).astype(BF), upper)
    aux[0:1, :] = jnp.sum(jnp.where(oh0, ranks, 0.0), axis=0, keepdims=True)
    aux[1:2, :] = jnp.sum(jnp.where(oh1, ranks, 0.0), axis=0, keepdims=True)

    blk = 128
    for b in range(nep * 8 // blk):
        rw = iota((blk, tokn), 0) + b * blk
        hit = ((rw >> 3) == r0) | ((rw >> 3) == r1)
        rk = dot(hit.astype(BF), upper)
        s = rw & 7
        p8[pl.ds(b * blk, blk), :] = (hit & (rk == s.astype(F32)) & (s < CAP)).astype(BF)

    pr, pc = iota((2 * rpg, 16 * per), 0), iota((2 * rpg, 16 * per), 1)
    second = pr >= rpg
    rr_ = pr - jnp.where(second, rpg, 0)
    src = div5(rr_)
    perm[...] = (pc == src * 16 + (rr_ - src * CAP) + jnp.where(second, CAP, 0)).astype(BF)

    for cp in share_copies:
        cp.wait()
    both = share[...].reshape(2 * tokn, LANES)
    blk = 256
    for b in range(nep * 16 // blk):
        rw = iota((blk, tokn), 0) + b * blk
        ex = rw >> 4
        q = rw & 15
        h0, h1 = ex == r0, ex == r1
        rk = dot((h0 | h1).astype(BF), upper)
        wt = jnp.where(h0, w0, 0.0) + jnp.where(h1, w1, 0.0)
        hit = h0 | h1
        one = jnp.where(hit & (rk == q.astype(F32)) & (q < CAP), 1.0, 0.0)
        two = jnp.where(hit & (rk == (q - CAP).astype(F32)) & (q >= CAP), wt, 0.0)
        sel = jnp.concatenate([one.astype(BF), two.astype(BF)], axis=1)
        msg[pl.ds(b * (blk // 16), blk // 16)] = dot(sel, both).astype(BF).reshape(blk // 16, 16, LANES)

    pl.semaphore_wait(barrier, nep - 1 + nx - 1 + 1)

    def give(j, carry):
        p = peer(j)
        pltpu.make_async_remote_copy(
            src_ref=msg.at[p, pl.ds(0, MSG)], dst_ref=rcv.at[e, pl.ds(0, MSG)],
            send_sem=d_send, recv_sem=d_recv.at[e // per],
            device_id=(p, t), device_id_type=MESH,
        ).start()
        return carry

    lax.fori_loop(0, nep - 1, give, 0)
    rcv[e] = msg[e]

    def remote(src, dst, ssem, rsem, to):
        return pltpu.make_async_remote_copy(
            src_ref=src, dst_ref=dst, send_sem=ssem, recv_sem=rsem, device_id=(e, to), device_id_type=MESH)

    def await_bytes(ref, sem):
        pltpu.make_async_copy(ref, ref, sem).wait()

    g0 = (e // per)

    def group(k):
        return lax.rem(g0 + k, GROUPS)

    def own(k):
        g = group(k)

        @pl.when(k == 0)
        def _():
            await_bytes(rcv.at[pl.ds(0, per - 1), pl.ds(0, MSG)], d_recv.at[g])

        @pl.when(k != 0)
        def _():
            await_bytes(rcv.at[pl.ds(0, per), pl.ds(0, MSG)], d_recv.at[g])

        got = rcv[pl.ds(g * per, per)].reshape(per * 16, LANES)
        rows[t, g] = dot(perm[...], got).astype(BF).reshape(2, rpg, LANES)
        unit = rows.at[t, g]
        remote(unit, unit, ag_rs, ag_l.at[0, g], right).start()
        remote(unit, unit, ag_ls, ag_r.at[0, g], left).start()
        remote(unit, unit, ag_ss, ag_s.at[0], sib).start()

    def passed(h, k):
        g = group(k)
        a, b = chip(-h) * 2 + c, chip(h) * 2 + c
        if h < far:
            ua, ub = rows.at[a, g], rows.at[b, g]
        else:
            ua, ub = rows.at[a, g, 0], rows.at[b, g, 1]
        await_bytes(ua, ag_l.at[h - 1, g])
        if h < far - 1:
            remote(ua, ua, ag_rs, ag_l.at[h, g], right).start()
        elif h == far - 1:
            remote(rows.at[a, g, 0], rows.at[a, g, 0], ag_rh, ag_l.at[h, g], right).start()
        await_bytes(ub, ag_r.at[h - 1, g])
        if h < far - 1:
            remote(ub, ub, ag_ls, ag_r.at[h, g], left).start()
        elif h == far - 1:
            remote(rows.at[b, g, 1], rows.at[b, g, 1], ag_lh, ag_r.at[h, g], left).start()
        remote(ua, ua, ag_ss, ag_s.at[nx - h], sib).start()
        remote(ub, ub, ag_ss, ag_s.at[h], sib).start()

    def sib_slice(d):
        s = chip(d) * 2 + (1 - c)
        await_bytes(rows.at[s], ag_s.at[d])

    def kstep(d, first=False):
        xc = chip(d)
        at = pl.multiple_of(xc * 2 * LANES, 2 * LANES)
        n = GROUPS * rpg

        def slab(which):
            return jnp.concatenate(
                [rows[2 * xc, :, which].reshape(n, LANES), rows[2 * xc + 1, :, which].reshape(n, LANES)], axis=1)

        wgu = jnp.concatenate([gate[pl.ds(at, 2 * LANES), :], up[pl.ds(at, 2 * LANES), :]], axis=1)
        a = dot(slab(0), wgu)
        b = dot_nt(slab(1), down[:, pl.ds(at, 2 * LANES)])
        if first:
            acc[:, 0:2 * LANES] = a
            acc[:, 2 * LANES:] = b
        else:
            acc[:, 0:2 * LANES] += a
            acc[:, 2 * LANES:] += b

    if stage >= 2:
        for s in range(GROUPS + far):
            if s < GROUPS:
                own(s)
            for h in range(1, far + 1):
                if 0 <= s - h < GROUPS:
                    passed(h, s - h)
            if s == GROUPS:
                for cp in weight_copies:
                    cp.wait()
                sib_slice(0)
                kstep(0, True)
            elif s > GROUPS:
                h = s - GROUPS
                sib_slice(h)
                kstep(h)
                sib_slice(nx - h)
                kstep(nx - h)
        sib_slice(far)
        kstep(far)
    else:
        for k in range(GROUPS):
            g = group(k)
            await_bytes(rcv.at[pl.ds(0, per - 1 if k == 0 else per), pl.ds(0, MSG)], d_recv.at[g])
        for cp in weight_copies:
            cp.wait()

    if stage >= 3:
        ones8 = [(iota((8, LANES), 0) == g).astype(BF) for g in range(GROUPS)]
        mixrow = jnp.zeros((8, rpg), F32)
        for g in range(GROUPS):
            rs = pl.ds(g * rpg, rpg)
            pg, pu, bh = acc[rs, 0:LANES], acc[rs, LANES:2 * LANES], acc[rs, 2 * LANES:]
            sig = jax.nn.sigmoid(pg)
            act = pg * sig
            hidden = (act * pu).astype(BF)
            hid[rs, :] = hidden
            hb = hidden.astype(F32) * bh
            hi = hb.astype(BF)
            lo = (hb - hi.astype(F32)).astype(BF)
            mixrow = mixrow + dot_nt(ones8[g], hi) + dot_nt(ones8[g], lo)
            bgu[rs, 0:LANES] = (bh * pu * (sig * (1.0 + pg * (1.0 - sig)))).astype(BF)
            bgu[rs, LANES:] = (bh * act).astype(BF)
        mixs[0, :, 0:rpg] = mixrow[0:GROUPS, :]
        mixs[0, :, rpg:] = jnp.zeros((GROUPS, LANES - rpg), F32)
        remote(mixs.at[0], mixs.at[1], mx_ss, mx_sr, sib).start()

    def part(d):
        xc = chip(d)
        at = pl.multiple_of(xc * 2 * LANES, 2 * LANES)
        wgu = jnp.concatenate([gate[pl.ds(at, 2 * LANES), :], up[pl.ds(at, 2 * LANES), :]], axis=1)
        v = dot_nt(bgu[...], wgu)
        a, b = v[:, 0:LANES], v[:, LANES:]
        pown[d % nx] = jnp.where(c == 0, a, b)
        psend[d % nx] = jnp.where(c == 0, b, a).astype(BF)
        remote(psend.at[d % nx], psib.at[d % nx], ps_send, ps_recv.at[d % nx], sib).start()

    def get_sib(d):
        await_bytes(psib.at[d % nx], ps_recv.at[d % nx])

    def both_cores(d, u):
        rs = pl.ds(u * rpg, rpg)
        return pown[d % nx, rs, :] + psib[d % nx, rs, :].astype(F32)

    def send_rs(val, buf, sem_of, step, u, to):
        buf[step - 1, u] = val.astype(BF)
        here = 0 if buf is sbr else 1
        return remote(buf.at[step - 1, u], (rr if here else rl).at[step - 1, u], rs_send.at[here, step - 1], sem_of.at[step - 1, u], to)

    def grads(xs):
        xc = xs
        n = GROUPS * rpg
        at = xs * 2 * LANES

        def slab(which):
            return jnp.concatenate(
                [rows[2 * xc, :, which].reshape(n, LANES), rows[2 * xc + 1, :, which].reshape(n, LANES)], axis=1)

        v = dot_tn(bgu[...], slab(0))
        gt_ref[:, at:at + 2 * LANES] = v[0:LANES].astype(BF)
        ut_ref[:, at:at + 2 * LANES] = v[LANES:].astype(BF)
        dg_ref[:, at:at + 2 * LANES] = dot_tn(hid[...], slab(1)).astype(BF)

    if stage >= 4:
        half = GROUPS // 2
        part(far)
        part(far - 1)
        part(1 - far)
        await_bytes(mixs.at[1], mx_sr)
        mixv[0] = mixs[0] + mixs[1]

        def tell(d, carry):
            remote(mixv.at[0], mixv.at[d], mx_send, mx_recv, chip(d) * 2 + c).start()
            return carry

        for d in range(1, nx):
            remote(mixv.at[0], mixv.at[d], mx_send, mx_recv, chip(d) * 2 + c).start()
        get_sib(far)
        for u in range(half):
            send_rs(both_cores(far, u), sbr, rs_l, 1, u, right).start()
            send_rs(both_cores(far, u + half), sbl, rs_r, 1, u + half, left).start()
        for step in range(2, far + 1):
            d = far + 1 - step
            if d > 1:
                part(d - 1)
                part(1 - d)
            elif d == 1:
                part(0)
            get_sib(d)
            get_sib(-d)
            ro = range(GROUPS) if step > 2 else [2, 3, 0, 1]
            lo_ = range(GROUPS)
            for ur, ul in zip(ro, lo_):
                v = both_cores(d, ur)
                if step > 2 or ur < half:
                    await_bytes(rl.at[step - 2, ur], rs_l.at[step - 2, ur])
                    v = v + rl[step - 2, ur].astype(F32)
                send_rs(v, sbr, rs_l, step, ur, right).start()
                v = both_cores(-d, ul)
                if step > 2 or ul >= half:
                    await_bytes(rr.at[step - 2, ul], rs_r.at[step - 2, ul])
                    v = v + rr[step - 2, ul].astype(F32)
                send_rs(v, sbl, rs_r, step, ul, left).start()
            grads(2 * step - 4)
            grads(2 * step - 3)
        get_sib(0)
        for i in range(2 * far - 2, nx):
            grads(i)
        await_bytes(mixv.at[pl.ds(0, nx - 1)], mx_recv)
        total_mix = mixv[0]
        for d in range(1, nx):
            total_mix = total_mix + mixv[d]
        mhi = total_mix.astype(BF).astype(F32)
        mlo = total_mix - mhi

        br, bc = iota((LANES, LANES), 0), iota((LANES, LANES), 1)
        src_of = div5(bc)
        slot_of = bc - src_of * CAP
        valid = bc < rpg
        spread = (((br >> 3) == src_of) & ((br & 7) == slot_of) & valid)[:, 0:rpg].astype(BF)
        take = ((br >> 3) == src_of) & ((br & 7) == CAP) & valid
        src_r = div5(br)
        slot_r = br - src_r * CAP
        bhi = (bc == slot_r).astype(BF)
        blo = (bc == slot_r + 8).astype(BF)

        for u in range(GROUPS):
            await_bytes(rl.at[far - 1, u], rs_l.at[far - 1, u])
            await_bytes(rr.at[far - 1, u], rs_r.at[far - 1, u])
            v = both_cores(0, u) + rl[far - 1, u].astype(F32) + rr[far - 1, u].astype(F32)
            m = dot(spread, v.astype(BF))
            m = m + dot(jnp.where(take, mhi[u:u + 1, :], 0.0).astype(BF), bhi)
            m = m + dot(jnp.where(take, mlo[u:u + 1, :], 0.0).astype(BF), blo)
            out[pl.ds(u * per, per)] = m.astype(BF).reshape(per, 8, LANES)

            def back(j, carry):
                i = u * per + j

                @pl.when(i != e)
                def _():
                    pltpu.make_async_remote_copy(
                        src_ref=out.at[i], dst_ref=ret.at[e], send_sem=rt_send, recv_sem=rt_recv,
                        device_id=(i, t), device_id_type=MESH,
                    ).start()
                return carry

            lax.fori_loop(0, per, back, 0)
        ret[e] = out[e]
        await_bytes(ret.at[pl.ds(0, nep - 1)], rt_recv)

        back_rows = ret[...].reshape(nep * 8, LANES)
        tg_ref[...] = dot_tn(p8[...], back_rows).astype(BF)
        sr, sc = iota((nep, nep * 8), 0), iota((nep, nep * 8), 1)
        mixes = dot((sc == sr * 8 + CAP).astype(BF), back_rows).astype(BF)
        lane = iota((LANES, tokn), 0).astype(F32)
        done = []
        for k, (oh, wk) in enumerate(((oh0, w0), (oh1, w1))):
            seen = dot_tn(mixes, oh.astype(BF))
            rank = aux[k:k + 1, :]
            picked = jnp.where((lane == rank) | (lane == rank + 8.0), seen, 0.0)
            done.append(jnp.sum(picked, axis=0, keepdims=True) / wk)
        mg_ref[...] = jnp.concatenate(done, axis=0).astype(BF)

    await_bytes(msg.at[pl.ds(0, nep - 1), pl.ds(0, MSG)], d_send)
    if stage >= 2:
        await_bytes(rows.at[pl.ds(0, far - 1)], ag_rs)
        await_bytes(rows.at[pl.ds(0, far - 1)], ag_ls)
        await_bytes(rows.at[0, :, 0], ag_rh)
        await_bytes(rows.at[0, :, 0], ag_lh)
        await_bytes(rows.at[pl.ds(0, nx)], ag_ss)
    if stage >= 3:
        await_bytes(mixs.at[0], mx_ss)
    if stage == 3:
        await_bytes(mixs.at[1], mx_sr)
    if stage >= 4:
        await_bytes(psend, ps_send)
        await_bytes(mixv.at[pl.ds(0, nx - 1)], mx_send)
        await_bytes(sbr.at[0, pl.ds(0, half)], rs_send.at[0, 0])
        await_bytes(sbl.at[0, pl.ds(half, half)], rs_send.at[1, 0])
        for step in range(1, far):
            await_bytes(sbr.at[step], rs_send.at[0, step])
            await_bytes(sbl.at[step], rs_send.at[1, step])
        await_bytes(out.at[pl.ds(0, nep - 1)], rt_send)


def solution(mesh):
    nep, ntp = mesh.shape["ep"], mesh.shape["tp"]
    nx = ntp // 2
    ny = 8 if nep == 64 else 4

    def on_device(tokens, cotangent, mix_weights, routes, gate_proj, up_proj, down_proj):
        tokn, width = tokens.shape
        ff = gate_proj.shape[2]
        n = nep * CAP
        per = nep // GROUPS
        rpg = per * CAP
        far = nx // 2
        vm = pl.BlockSpec(memory_space=pltpu.VMEM)
        hbm = pl.BlockSpec(memory_space=pl.ANY)
        dma = pltpu.SemaphoreType.DMA
        tg, mg, gt, ut, dg = pl.pallas_call(
            functools.partial(kernel, nep, nx, ny, 4),
            out_shape=(
                jax.ShapeDtypeStruct((tokn, LANES), BF),
                jax.ShapeDtypeStruct((2, tokn), BF),
                jax.ShapeDtypeStruct((ff, width), BF),
                jax.ShapeDtypeStruct((ff, width), BF),
                jax.ShapeDtypeStruct((ff, width), BF),
            ),
            in_specs=[hbm, hbm, vm, vm, hbm, hbm, hbm],
            out_specs=[vm] * 5,
            scratch_shapes=[
                pltpu.VMEM((2, tokn, LANES), BF),
                pltpu.VMEM((nep, 16, LANES), BF),
                pltpu.VMEM((nep, 16, LANES), BF),
                pltpu.VMEM((ntp, GROUPS, 2, rpg, LANES), BF),
                pltpu.VMEM((width, ff), BF),
                pltpu.VMEM((width, ff), BF),
                pltpu.VMEM((ff, width), BF),
                pltpu.VMEM((n, 3 * LANES), F32),
                pltpu.VMEM((nep * 8, tokn), BF),
                pltpu.VMEM((8, tokn), F32),
                pltpu.VMEM((2 * rpg, 16 * per), BF),
                pltpu.VMEM((n, 2 * LANES), BF),
                pltpu.VMEM((n, LANES), BF),
                pltpu.VMEM((nx, n, LANES), F32),
                pltpu.VMEM((nx, n, LANES), BF),
                pltpu.VMEM((nx, n, LANES), BF),
                pltpu.VMEM((far, GROUPS, rpg, LANES), BF),
                pltpu.VMEM((far, GROUPS, rpg, LANES), BF),
                pltpu.VMEM((far, GROUPS, rpg, LANES), BF),
                pltpu.VMEM((far, GROUPS, rpg, LANES), BF),
                pltpu.VMEM((nx, GROUPS, LANES), F32),
                pltpu.VMEM((2, GROUPS, LANES), F32),
                pltpu.VMEM((nep, 8, LANES), BF),
                pltpu.VMEM((nep, 8, LANES), BF),
                dma((2,)), dma((3,)), dma, dma((GROUPS,)),
                dma, dma, dma, dma, dma,
                dma((far, GROUPS)), dma((far, GROUPS)), dma((nx,)),
                dma, dma((nx,)), dma((2, far)), dma((far, GROUPS)), dma((far, GROUPS)),
                dma, dma, dma, dma, dma, dma,
            ],
            compiler_params=pltpu.CompilerParams(
                collective_id=0, has_side_effects=True, vmem_limit_bytes=48 * 1024 * 1024),
        )(tokens, cotangent, routes.T, mix_weights.T, gate_proj, up_proj, down_proj)
        return tg, mg.T, gt.T[None], ut.T[None], dg[None]

    in_specs = (
        P("ep", None), P("ep", None), P("ep", None), P("ep", None),
        P("ep", None, "tp"), P("ep", None, "tp"), P("ep", "tp", None),
    )
    out_specs = (
        P("ep", "tp"), P("ep", None), P("ep", None, "tp"), P("ep", None, "tp"), P("ep", "tp", None),
    )
    return jax.shard_map(on_device, mesh=mesh, in_specs=in_specs, out_specs=out_specs, check_vma=False)
```

```python
import functools

import jax
import jax.numpy as jnp
from jax import lax
from jax.experimental import pallas as pl
from jax.experimental.pallas import tpu as pltpu
from jax.sharding import PartitionSpec as P

MESH = pl.DeviceIdType.MESH
BF = jnp.bfloat16
F32 = jnp.float32
CAP = 5
MSG = 2 * CAP
LANES = 128
NX = NY = NZ = 8
GROUPS = 4
ZB = NZ // GROUPS
HY = NY // 2
PER = ZB * HY
RPG = PER * CAP
TILE = 2 * RPG + 8
CUT = 40
WIDE = 2 * LANES
QUADS = 4
QUAD = 4 * LANES
DIRECT = ()
EARLY = "W r0 r1 r2 s3 A0 A1 B0 t3 B1 P0 A2 H0 C0 A3 P1 B2 H1 P2 E0 B3 P3 H2 C2 F0 C1 H3 C3 E2 E1 E3 F2 F1 F3 T G"
LATE = "W r0 A0 r1 r2 r3 B0 P0 A3 A1 H0 C0 A2 B1 P1 E0 H1 C1 B2 B3 F0 P2 E1 H2 C2 P3 H3 C3 F1 E2 E3 F2 F3 T G"


def iota(shape, dim):
    return lax.broadcasted_iota(jnp.int32, shape, dim)


def dot(a, b):
    return jnp.dot(a, b, preferred_element_type=F32)


def dot_nt(a, b):
    return lax.dot_general(a, b, (((1,), (1,)), ((), ())), preferred_element_type=F32)


def dot_tn(a, b):
    return lax.dot_general(a, b, (((0,), (0,)), ((), ())), preferred_element_type=F32)


def div5(v):
    return (v * 205) >> 10


def kernel(
    tok_hbm, cot_hbm, routes_hbm, mix_hbm, gate_hbm, up_hbm, down_hbm,
    ret, p8, aux, gg_ref, ug_ref, dg_ref,
    routes_ref, mix_ref, share, msg, ybuf, zbuf, rows, w4, dw, w4t, dwt, perm, bgu, hid, obgu, ohid, mixt,
    pre, back, pown, sb, rb, out,
    ready, t_sem, sh_sem, w_sem, x_sem, y_send, y_recv, z_send, z_recv, ag_send, ag_recv, sib_send, sib_recv,
    bh_send, bh_recv, rs_send, rs_recv, rt_send, rt_recv,
):
    e = lax.axis_index("ep")
    t = lax.axis_index("tp")
    z, y = e // NY, e % NY
    x, c = t // 2, t % 2
    tokn = share.shape[1]
    nep = NZ * NY
    active = y % 2 == c

    def chip(d):
        return lax.rem(x + d + NX, NX)

    def quad(d):
        return lax.rem(x + d + NX, QUADS)

    sib = (e, x * 2 + (1 - c))

    def along_x(d):
        return (e, chip(d) * 2 + c)

    def remote(src, dst, ssem, rsem, to):
        return pltpu.make_async_remote_copy(
            src_ref=src, dst_ref=dst, send_sem=ssem, recv_sem=rsem, device_id=to, device_id_type=MESH)

    def await_bytes(ref, sem):
        pltpu.make_async_copy(ref, ref, sem).wait()

    col = pl.multiple_of(quad(0) * QUAD, QUAD)
    table_copies = [
        pltpu.make_async_copy(routes_hbm, routes_ref, t_sem.at[0]),
        pltpu.make_async_copy(mix_hbm, mix_ref, t_sem.at[1]),
    ]
    share_copies = [
        pltpu.make_async_copy(tok_hbm.at[:, pl.ds(col, QUAD)], share.at[0], sh_sem.at[0]),
        pltpu.make_async_copy(cot_hbm.at[:, pl.ds(col, QUAD)], share.at[1], sh_sem.at[1]),
    ]
    lane = pl.multiple_of(c * WIDE, WIDE)
    ours = w4.at[:, pl.ds(lane, WIDE)]
    downs = dw.at[pl.ds(pl.multiple_of(c * LANES, LANES), LANES)]
    weight_copies = [
        pltpu.make_async_copy(gate_hbm.at[0], w4.at[:, pl.ds(lane, LANES)], w_sem.at[0]),
        pltpu.make_async_copy(up_hbm.at[0], w4.at[:, pl.ds(pl.multiple_of(lane + LANES, LANES), LANES)], w_sem.at[1]),
        pltpu.make_async_copy(down_hbm.at[0], downs, w_sem.at[2]),
    ]
    weight_moves = [
        remote(ours, ours, x_sem.at[0], x_sem.at[1], sib),
        remote(downs, downs, x_sem.at[2], x_sem.at[3], sib),
    ]
    barrier = pltpu.get_barrier_semaphore()
    for d in (4, 3, 5, 2, 6, 1, 7):
        pl.semaphore_signal(barrier, inc=1, device_id=(z * NY + lax.rem(y + d, NY), t), device_id_type=MESH)
    for d in (2, -2, 1, -1):
        pl.semaphore_signal(barrier, inc=1, device_id=along_x(d), device_id_type=MESH)
    pl.semaphore_signal(barrier, inc=1, device_id=sib, device_id_type=MESH)
    for cp in table_copies + share_copies + weight_copies:
        cp.start()
    with jax.named_scope("barrier"):
        pl.semaphore_wait(barrier, 12 + jnp.where(z > 0, 1, 0))

    @pl.when(z < NZ - 1)
    def _():
        pl.semaphore_signal(barrier, inc=1, device_id=(e + NY, t), device_id_type=MESH)

    for zz in range(NZ - 1):
        @pl.when(zz < z)
        def _():
            pl.semaphore_signal(ready.at[z], inc=1, device_id=(zz * NY + y, t), device_id_type=MESH)

    for cp in table_copies:
        cp.wait()
    r0, r1 = routes_ref[0:1, :], routes_ref[1:2, :]
    w = mix_ref[...].astype(F32)
    w0, w1 = w[0:1, :], w[1:2, :]
    upper = (iota((tokn, tokn), 0) < iota((tokn, tokn), 1)).astype(BF)
    with jax.named_scope("share"):
        for cp in share_copies:
            cp.wait()

    @pl.when(active)
    def _():
        both = share[...].reshape(2 * tokn, QUAD)
        blk = ZB * NY * 16
        for b in range(GROUPS):
            rw = iota((blk, tokn), 0) + b * blk
            ex = rw >> 4
            q = rw & 15
            h0, h1 = ex == r0, ex == r1
            hit = h0 | h1
            rk = dot(hit.astype(BF), upper)
            wt = jnp.where(h0, w0, 0.0) + jnp.where(h1, w1, 0.0)
            one = jnp.where(hit & (rk == q.astype(F32)) & (q < CAP), 1.0, 0.0)
            two = jnp.where(hit & (rk == (q - CAP).astype(F32)) & (q >= CAP), wt, 0.0)
            sel = jnp.concatenate([one.astype(BF), two.astype(BF)], axis=1)
            v = dot(sel, both).astype(BF)
            for ch in range(4):
                msg[pl.ds(b * ZB, ZB), :, ch] = v[:, ch * LANES:(ch + 1) * LANES].reshape(ZB, NY, 16, LANES)
            for d in (4, 3, 5, 2, 6, 1, 7):
                yd = lax.rem(y + d, NY)
                remote(
                    msg.at[pl.ds(b * ZB, ZB), yd, :, pl.ds(0, MSG)],
                    ybuf.at[pl.ds(b * ZB, ZB), y // 2, :, pl.ds(0, MSG)],
                    y_send, y_recv.at[b], (z * NY + yd, t)).start()
            ybuf[pl.ds(b * ZB, ZB), y // 2] = msg[pl.ds(b * ZB, ZB), y]

    for cp in weight_copies:
        cp.wait()
    for cp in weight_moves:
        cp.start()

    def relay(b):
        with jax.named_scope(f"ywait{b}"):
            @pl.when(active)
            def _():
                await_bytes(ybuf.at[pl.ds(b * ZB, ZB), pl.ds(0, HY - 1), :, pl.ds(0, MSG)], y_recv.at[b])

            @pl.when(jnp.logical_not(active))
            def _():
                await_bytes(ybuf.at[pl.ds(b * ZB, ZB), :, :, pl.ds(0, MSG)], y_recv.at[b])
        for zd in range(b * ZB, (b + 1) * ZB):
            @pl.when(zd == z)
            def _():
                zbuf[zd] = ybuf[zd]

            @pl.when(zd > z)
            def _():
                with jax.named_scope(f"ready{zd}"):
                    pl.semaphore_wait(ready.at[zd], 1)

            @pl.when(zd != z)
            def _():
                remote(
                    ybuf.at[zd, :, :, pl.ds(0, MSG)], zbuf.at[z, :, :, pl.ds(0, MSG)],
                    z_send, z_recv.at[z], (zd * NY + y, t)).start()

    def unit(d, g):
        return rows.at[c, quad(d), :, pl.ds(g * RPG, RPG)]

    def half(d, g, i):
        return rows.at[c, quad(d), i, pl.ds(g * RPG, RPG)]

    def to_sib(d, g):
        u = unit(d, g)
        remote(u, u, sib_send, sib_recv, sib).start()

    def gather_out(g):
        for zs in range(g * ZB, (g + 1) * ZB):
            @pl.when(zs != z)
            def _():
                with jax.named_scope(f"zwait{zs}"):
                    await_bytes(zbuf.at[zs, :, :, pl.ds(0, MSG)], z_recv.at[zs])
        got = jnp.concatenate(
            [zbuf[pl.ds(g * ZB, ZB), :, ch].reshape(PER * 16, LANES) for ch in range(4)], axis=1)
        got = jnp.where((iota(got.shape, 0) & 15) < MSG, got, jnp.zeros_like(got))
        v = dot(perm[...], got)
        rows[c, quad(0), 0, g * RPG:(g + 1) * RPG] = v[0:RPG].astype(BF)
        rows[c, quad(0), 1, g * RPG:(g + 1) * RPG] = v[RPG:].astype(BF)
        u = unit(0, g)
        remote(u, u, ag_send, ag_recv.at[0, g], along_x(1)).start()
        remote(u, u, ag_send, ag_recv.at[1, g], along_x(-1)).start()
        if g in DIRECT:
            for i, d in ((0, 2), (1, -2)):
                h = half(0, g, i)
                remote(h, h, ag_send, ag_recv.at[2 + i, g], along_x(d)).start()
        to_sib(0, g)

    def gather_in(g):
        for i, d in ((0, -1), (1, 1)):
            await_bytes(unit(d, g), ag_recv.at[i, g])
            if g not in DIRECT:
                h = half(d, g, i)
                remote(h, h, ag_send, ag_recv.at[2 + i, g], along_x(-d)).start()
            to_sib(d, g)

    def gather_far(g):
        for i in range(2):
            await_bytes(half(2, g, i), ag_recv.at[2 + i, g])
        to_sib(2, g)

    def send_part(g, i, to):
        remote(sb.at[g, i], rb.at[g, i], rs_send, rs_recv.at[g, i], along_x(to)).start()

    near, past = pl.ds(0, CUT), pl.ds(CUT, TILE - CUT)

    def products(g, d):
        at = pl.ds(g * RPG, RPG)
        q = quad(d)
        features = pl.ds(pl.multiple_of(q * QUAD, QUAD), QUAD)
        return dot(rows[c, q, 0, at], w4[features, :]), dot(rows[c, q, 1, at], dwt[features, :])

    def first_products(g):
        each = [products(g, d) for d in (0, -1, 1)]
        pre[g] = each[0][0] + each[1][0] + each[2][0]
        back[g] = each[0][1] + each[1][1] + each[2][1]

    def compute(g):
        at = pl.ds(g * RPG, RPG)
        pgu, bh = products(g, 2)
        pgu = pgu + pre[g]
        bh = bh + back[g]
        pg = jnp.concatenate([pgu[:, 0:LANES], pgu[:, WIDE:WIDE + LANES]], axis=1)
        pu = jnp.concatenate([pgu[:, LANES:WIDE], pgu[:, WIDE + LANES:]], axis=1)
        sig = jax.nn.sigmoid(pg)
        act = pg * sig
        hidden = (act * pu).astype(BF)
        bg = (bh * pu * (sig * (1.0 + pg * (1.0 - sig)))).astype(BF)
        bu = (bh * act).astype(BF)
        b0 = jnp.concatenate([bg[:, 0:LANES], bu[:, 0:LANES]], axis=1)
        b1 = jnp.concatenate([bg[:, LANES:], bu[:, LANES:]], axis=1)
        b4 = jnp.concatenate([b0, b1], axis=1)
        hb = hidden.astype(F32) * bh
        hi = hb.astype(BF)
        lo = (hb - hi.astype(F32)).astype(BF)
        ones = jnp.ones((8, WIDE), BF)
        sums = dot_nt(ones, hi) + dot_nt(ones, lo)
        shi = sums.astype(BF).astype(F32)
        row = iota((8, RPG), 0)
        mixt[g, :, 0:RPG] = jnp.where(row == 0, shi, jnp.where(row == 1, sums - shi, 0.0))
        tile = mixt[g].astype(BF)
        for d, i, to in ((3, 0, 1), (5, 1, -1), (4, 4, 0), (1, 2, 1), (7, 3, -1), (2, 0, None), (6, 1, None), (0, 2, None)):
            cols = pl.ds(pl.multiple_of(chip(d) * WIDE, WIDE), WIDE)
            v = dot(b4, w4t[:, cols])
            if to is None:
                pown[g, i, 0:RPG] = v[:, 0:LANES]
                pown[g, i, RPG:2 * RPG] = v[:, LANES:]
            else:
                sb[g, i, 0:RPG] = v[:, 0:LANES].astype(BF)
                sb[g, i, RPG:2 * RPG] = v[:, LANES:].astype(BF)
                sb[g, i, 2 * RPG:] = tile
                if to:
                    send_part(g, i, to)
                else:
                    remote(sb.at[g, 4, near], rb.at[g, 4, near], rs_send, rs_recv.at[g, 4], along_x(2)).start()
                    remote(sb.at[g, 4, past], rb.at[g, 4, past], rs_send, rs_recv.at[g, 7], along_x(-2)).start()
        first = c == 0
        bgu[c, at] = jnp.where(first, b0.astype(F32), b1.astype(F32)).astype(BF)
        obgu[g] = jnp.where(first, b1.astype(F32), b0.astype(F32)).astype(BF)
        hf = hidden.astype(F32)
        hid[c, at] = jnp.where(first, hf[:, 0:LANES], hf[:, LANES:]).astype(BF)
        ohid[g] = jnp.where(first, hf[:, LANES:], hf[:, 0:LANES]).astype(BF)
        remote(obgu.at[g], bgu.at[c, at], bh_send.at[0], bh_recv.at[0], sib).start()
        remote(ohid.at[g], hid.at[c, at], bh_send.at[1], bh_recv.at[1], sib).start()

    def chunk(g, i):
        return jnp.concatenate([pown[g, i], mixt[g]], axis=0)

    def scatter_two(g):
        await_bytes(rb.at[g, 0], rs_recv.at[g, 0])
        await_bytes(rb.at[g, 4, near], rs_recv.at[g, 4])
        v = chunk(g, 0) + rb[g, 0].astype(F32)
        sb[g, 5, 0:CUT] = (v[0:CUT] + rb[g, 4, 0:CUT].astype(F32)).astype(BF)
        sb[g, 5, CUT:] = v[CUT:].astype(BF)
        send_part(g, 5, 2)
        await_bytes(rb.at[g, 1], rs_recv.at[g, 1])
        await_bytes(rb.at[g, 4, past], rs_recv.at[g, 7])
        v = chunk(g, 1) + rb[g, 1].astype(F32)
        sb[g, 6, 0:CUT] = v[0:CUT].astype(BF)
        sb[g, 6, CUT:] = (v[CUT:] + rb[g, 4, CUT:].astype(F32)).astype(BF)
        send_part(g, 6, -2)

    def give_back(g):
        v = chunk(g, 2)
        for i in (2, 3, 5, 6):
            await_bytes(rb.at[g, i], rs_recv.at[g, i])
            v = v + rb[g, i].astype(F32)
        sums = v[2 * RPG:2 * RPG + 1] + v[2 * RPG + 1:2 * RPG + 2]
        mhi = sums.astype(BF).astype(F32)
        mlo = sums - mhi
        br, bc = iota((LANES, LANES), 0), iota((LANES, LANES), 1)
        second = bc >= RPG
        row = bc - jnp.where(second, RPG, 0)
        src_of = div5(row)
        slot_of = row - src_of * CAP
        here = ((br >> 3) == src_of + jnp.where(second, PER, 0)) & (bc < 2 * RPG)
        spread = (here & ((br & 7) == slot_of))[:, 0:2 * RPG].astype(BF)
        take = (((br >> 3) & (PER - 1)) == div5(bc)) & ((br & 7) == CAP) & (bc < RPG)
        slot_r = br - div5(br) * CAP
        m = dot(spread, v[0:2 * RPG].astype(BF))
        m = m + dot(jnp.where(take, mhi, 0.0).astype(BF), (bc == slot_r).astype(BF))
        m = m + dot(jnp.where(take, mlo, 0.0).astype(BF), (bc == slot_r + 8).astype(BF))
        out[g] = m.astype(BF).reshape(2, PER, 8, LANES)
        for j in range(PER):
            i = (g * ZB + j // HY) * NY + 2 * (j % HY) + c
            for hf in range(2):
                here_ = (i == e) & (c == hf)

                @pl.when(here_)
                def _():
                    ret[e] = out[g, hf, j]

                @pl.when(jnp.logical_not(here_))
                def _():
                    remote(out.at[g, hf, j], ret.at[e], rt_send, rt_recv, (i, x * 2 + hf)).start()

    def grads():
        await_bytes(rows.at[1 - c], sib_recv)
        await_bytes(bgu.at[1 - c], bh_recv.at[0])
        await_bytes(hid.at[1 - c], bh_recv.at[1])
        for q in range(QUADS):
            at = slice(q * QUAD, (q + 1) * QUAD)
            v = dot_tn(rows[0, q, 0], bgu[0]) + dot_tn(rows[1, q, 0], bgu[1])
            gg_ref[at, :] = v[:, 0:LANES].astype(BF)
            ug_ref[at, :] = v[:, LANES:].astype(BF)
            dg_ref[:, at] = (dot_tn(hid[0], rows[0, q, 1]) + dot_tn(hid[1], rows[1, q, 1])).astype(BF)

    def turn():
        mixt[...] = jnp.zeros_like(mixt)
        pr, pc = iota((2 * RPG, 16 * PER), 0), iota((2 * RPG, 16 * PER), 1)
        second = pr >= RPG
        rest = pr - jnp.where(second, RPG, 0)
        src = div5(rest)
        perm[...] = (pc == src * 16 + (rest - src * CAP) + jnp.where(second, CAP, 0)).astype(BF)
        for cp in weight_moves:
            cp.wait_recv()
        for k in range(8):
            at = slice(k * WIDE, (k + 1) * WIDE)
            dwt[at, :] = dw[:, at].T
            for hf in range(2):
                w4t[hf * WIDE:(hf + 1) * WIDE, at] = w4[at, hf * WIDE:(hf + 1) * WIDE].T

    def tables():
        er = iota((nep, tokn), 0)
        oh0, oh1 = er == r0, er == r1
        ranks = dot((oh0 | oh1).astype(BF), upper)
        aux[0:1, :] = jnp.sum(jnp.where(oh0, ranks, 0.0), axis=0, keepdims=True)
        aux[1:2, :] = jnp.sum(jnp.where(oh1, ranks, 0.0), axis=0, keepdims=True)
        blk8 = 128
        for b in range(nep * 8 // blk8):
            rw = iota((blk8, tokn), 0) + b * blk8
            hit = ((rw >> 3) == r0) | ((rw >> 3) == r1)
            rk = dot(hit.astype(BF), upper)
            s = rw & 7
            p8[pl.ds(b * blk8, blk8), :] = (hit & (rk == s.astype(F32)) & (s < CAP)).astype(BF)
        aux[2:3, :] = w0
        aux[3:4, :] = w1
        aux[4:5, :] = r0.astype(F32)
        aux[5:6, :] = r1.astype(F32)
        aux[6:8, :] = jnp.zeros((2, tokn), F32)

    steps = {"A": gather_out, "B": gather_in, "H": gather_far, "P": first_products, "C": compute, "E": scatter_two, "F": give_back}
    def run(plan):
        for step in plan.split():
            kind, g = step[0], int(step[1:] or 0)
            with jax.named_scope(step):
                if kind == "r":
                    relay(g)
                elif kind == "s":
                    pl.when(z < NZ // 4)(functools.partial(relay, g))
                elif kind == "t":
                    pl.when(z >= NZ // 4)(functools.partial(relay, g))
                elif kind == "G":
                    grads()
                elif kind == "W":
                    turn()
                elif kind == "T":
                    tables()
                else:
                    steps[kind](g)

    early = z < NZ // 2
    pl.when(early)(functools.partial(run, EARLY))
    pl.when(jnp.logical_not(early))(functools.partial(run, LATE))

    for cp in weight_moves:
        cp.wait_send()

    @pl.when(active)
    def _():
        await_bytes(msg.at[:, pl.ds(0, NY - 1), :, pl.ds(0, MSG)], y_send)
        await_bytes(ret.at[pl.ds(0, nep - 1)], rt_send)

    @pl.when(jnp.logical_not(active))
    def _():
        await_bytes(ret, rt_send)

    await_bytes(zbuf.at[pl.ds(0, NZ - 1), :, :, pl.ds(0, MSG)], z_send)
    await_bytes(rows.at[0, pl.ds(0, 3)], ag_send)
    await_bytes(rows.at[0], sib_send)
    await_bytes(obgu, bh_send.at[0])
    await_bytes(ohid, bh_send.at[1])
    await_bytes(sb, rs_send)

    with jax.named_scope("retwait"):
        @pl.when(active)
        def _():
            await_bytes(ret.at[pl.ds(0, nep - 1)], rt_recv)

        @pl.when(jnp.logical_not(active))
        def _():
            await_bytes(ret, rt_recv)


def finish(ret, p8, aux, gg, ug, dg, tg_ref, mg_ref, gg_out, ug_out, dg_out, tg, mg, sem):
    copies = [
        pltpu.make_async_copy(gg, gg_out.at[0], sem.at[0]),
        pltpu.make_async_copy(ug, ug_out.at[0], sem.at[1]),
        pltpu.make_async_copy(dg, dg_out.at[0], sem.at[2]),
    ]
    for cp in copies:
        cp.start()
    nep = ret.shape[0]
    tokn = p8.shape[1]
    back_rows = ret[...].reshape(nep * 8, LANES)
    tg[...] = dot_tn(p8[...], back_rows).astype(BF)
    copies.append(pltpu.make_async_copy(tg, tg_ref, sem.at[3]))
    copies[-1].start()
    sr, sc = iota((nep, nep * 8), 0), iota((nep, nep * 8), 1)
    mixes = dot((sc == sr * 8 + CAP).astype(BF), back_rows).astype(BF)
    lane = iota((LANES, tokn), 0).astype(F32)
    er = iota((nep, tokn), 0).astype(F32)
    done = []
    for k in range(2):
        seen = dot_tn(mixes, (er == aux[4 + k:5 + k, :]).astype(BF))
        rank = aux[k:k + 1, :]
        picked = jnp.where((lane == rank) | (lane == rank + 8.0), seen, 0.0)
        done.append(jnp.sum(picked, axis=0, keepdims=True) / aux[2 + k:3 + k, :])
    mg[...] = jnp.concatenate(done, axis=0).astype(BF)
    copies.append(pltpu.make_async_copy(mg, mg_ref, sem.at[4]))
    copies[-1].start()
    for cp in copies:
        cp.wait()


def solution(mesh):
    nep = NZ * NY

    def on_device(tokens, cotangent, mix_weights, routes, gate_proj, up_proj, down_proj):
        tokn, width = tokens.shape
        ff = gate_proj.shape[2]
        vm = pl.BlockSpec(memory_space=pltpu.VMEM)
        hbm = pl.BlockSpec(memory_space=pltpu.HBM)
        dma = pltpu.SemaphoreType.DMA
        parts = pl.pallas_call(
            kernel,
            out_shape=(
                jax.ShapeDtypeStruct((nep, 8, LANES), BF),
                jax.ShapeDtypeStruct((nep * 8, tokn), BF),
                jax.ShapeDtypeStruct((8, tokn), F32),
                jax.ShapeDtypeStruct((width, ff), BF),
                jax.ShapeDtypeStruct((width, ff), BF),
                jax.ShapeDtypeStruct((ff, width), BF),
            ),
            in_specs=[hbm] * 7,
            out_specs=[vm] * 6,
            scratch_shapes=[
                pltpu.VMEM((2, tokn), jnp.int32),
                pltpu.VMEM((2, tokn), BF),
                pltpu.VMEM((2, tokn, QUAD), BF),
                pltpu.VMEM((NZ, NY, 4, 16, LANES), BF),
                pltpu.VMEM((NZ, HY, 4, 16, LANES), BF),
                pltpu.VMEM((NZ, HY, 4, 16, LANES), BF),
                pltpu.VMEM((2, QUADS, 2, GROUPS * RPG, QUAD), BF),
                pltpu.VMEM((width, 4 * LANES), BF),
                pltpu.VMEM((2 * ff, width), BF),
                pltpu.VMEM((4 * LANES, width), BF),
                pltpu.VMEM((width, 2 * ff), BF),
                pltpu.VMEM((2 * RPG, 16 * PER), BF),
                pltpu.VMEM((2, GROUPS * RPG, WIDE), BF),
                pltpu.VMEM((2, GROUPS * RPG, LANES), BF),
                pltpu.VMEM((GROUPS, RPG, WIDE), BF),
                pltpu.VMEM((GROUPS, RPG, LANES), BF),
                pltpu.VMEM((GROUPS, 8, LANES), F32),
                pltpu.VMEM((GROUPS, RPG, QUAD), F32),
                pltpu.VMEM((GROUPS, RPG, WIDE), F32),
                pltpu.VMEM((GROUPS, 3, 2 * RPG, LANES), F32),
                pltpu.VMEM((GROUPS, 7, TILE, LANES), BF),
                pltpu.VMEM((GROUPS, 7, TILE, LANES), BF),
                pltpu.VMEM((GROUPS, 2, PER, 8, LANES), BF),
                pltpu.SemaphoreType.REGULAR((NZ,)),
                dma((2,)), dma((2,)), dma((3,)), dma((4,)), dma, dma((GROUPS,)), dma, dma((NZ,)),
                dma, dma((4, GROUPS)), dma, dma,
                dma((2,)), dma((2,)), dma, dma((GROUPS, 8)), dma, dma,
            ],
            compiler_params=pltpu.CompilerParams(
                collective_id=0, has_side_effects=True, vmem_limit_bytes=52 * 1024 * 1024),
        )(*(
            pltpu.with_memory_space_constraint(a, pltpu.HBM)
            for a in (tokens, cotangent, routes.T, mix_weights.T, gate_proj, up_proj, down_proj)))
        tg, mg, gg, ug, dg = pl.pallas_call(
            finish,
            out_shape=(
                jax.ShapeDtypeStruct((tokn, LANES), BF),
                jax.ShapeDtypeStruct((2, tokn), BF),
                jax.ShapeDtypeStruct((1, width, ff), BF),
                jax.ShapeDtypeStruct((1, width, ff), BF),
                jax.ShapeDtypeStruct((1, ff, width), BF),
            ),
            in_specs=[vm] * 6,
            out_specs=[hbm] * 5,
            scratch_shapes=[pltpu.VMEM((tokn, LANES), BF), pltpu.VMEM((2, tokn), BF), dma((5,))],
            compiler_params=pltpu.CompilerParams(vmem_limit_bytes=8 * 1024 * 1024),
        )(*parts)
        return tg, mg.T, gg, ug, dg

    in_specs = (
        P("ep", None), P("ep", None), P("ep", None), P("ep", None),
        P("ep", None, "tp"), P("ep", None, "tp"), P("ep", "tp", None),
    )
    out_specs = (
        P("ep", "tp"), P("ep", None), P("ep", None, "tp"), P("ep", None, "tp"), P("ep", "tp", None),
    )
    return jax.shard_map(on_device, mesh=mesh, in_specs=in_specs, out_specs=out_specs, check_vma=False)
```

```python
import functools

import jax
import jax.numpy as jnp
from jax import lax
from jax.experimental import pallas as pl
from jax.experimental.pallas import tpu as pltpu
from jax.sharding import PartitionSpec as P

MESH = pl.DeviceIdType.MESH
BF = jnp.bfloat16
F32 = jnp.float32
CAP = 5
MSG = 2 * CAP
LANES = 128
NX = NY = NZ = 8
GROUPS = 4
ZB = NZ // GROUPS
HY = NY // 2
PER = ZB * HY
RPG = PER * CAP
TILE = 2 * RPG + 8
SENT = 2 * RPG + 2
CUT = 40
WIDE = 2 * LANES
QUADS = 4
QUAD = 4 * LANES
EARLY = "W r0 r1 r2 s3 A0 A1 t3 f0 f1 B0 f2 f3 H0 Q0 C0 A2 E0 A3 B1 Q1 H1 C1 H2 B2 Q2 C2 F0 H3 P3 B3 C3 E1 E3 E2 T G F1 F3 F2"
LATE = "W r0 A0 r1 f0 f1 A1 r2 r3 B0 Q0 H0 C0 A2 H1 f2 E0 f3 B1 P1 C1 H3 B2 H2 A3 P2 C2 F0 E1 P3 E2 B3 F1 C3 F2 E3 F3 T G"


def iota(shape, dim):
    return lax.broadcasted_iota(jnp.int32, shape, dim)


def dot(a, b):
    return jnp.dot(a, b, preferred_element_type=F32)


def dot_nt(a, b):
    return lax.dot_general(a, b, (((1,), (1,)), ((), ())), preferred_element_type=F32)


def dot_tn(a, b):
    return lax.dot_general(a, b, (((0,), (0,)), ((), ())), preferred_element_type=F32)


def div5(v):
    return (v * 205) >> 10


def kernel(
    tok_hbm, cot_hbm, routes_hbm, mix_hbm, gate_hbm, up_hbm, down_hbm,
    ret, p8, aux, gg_ref, ug_ref, dg_ref,
    routes_ref, mix_ref, share, msg, ybuf, zbuf, rows, w4, dw, w4t, dwt, perm, bgu, hid, obgu, ohid, mixt,
    pre, back, pown, sb, rb, out,
    ready, t_sem, sh_sem, w_sem, x_sem, y_send, y_recv, z_send, z_recv, ag_send, ag_recv, sib_send, sib_recv,
    bh_send, bh_recv, rs_send, rs_recv, rt_send, rt_recv,
):
    e = lax.axis_index("ep")
    t = lax.axis_index("tp")
    z, y = e // NY, e % NY
    x, c = t // 2, t % 2
    tokn = share.shape[2]
    nep = NZ * NY
    mine_y = 1 - c
    active = y // HY == mine_y

    def chip(d):
        return lax.rem(x + d + NX, NX)

    def quad(d):
        return lax.rem(x + d + NX, QUADS)

    sib = (e, x * 2 + (1 - c))

    def along_x(d):
        return (e, chip(d) * 2 + c)

    def remote(src, dst, ssem, rsem, to):
        return pltpu.make_async_remote_copy(
            src_ref=src, dst_ref=dst, send_sem=ssem, recv_sem=rsem, device_id=to, device_id_type=MESH)

    def await_bytes(ref, sem):
        pltpu.make_async_copy(ref, ref, sem).wait()

    cols = [pl.ds(pl.multiple_of(quad(d) * QUAD, QUAD), QUAD) for d in (0, 2)]
    table_copies = [
        pltpu.make_async_copy(routes_hbm, routes_ref, t_sem.at[0]),
        pltpu.make_async_copy(mix_hbm, mix_ref, t_sem.at[1]),
    ]
    share_copies = [
        pltpu.make_async_copy(ref.at[:, cols[part]], share.at[part, i], sh_sem)
        for part in range(2) for i, ref in enumerate((tok_hbm, cot_hbm))
    ]
    lane = pl.multiple_of(c * WIDE, WIDE)
    ours = w4.at[:, pl.ds(lane, WIDE)]
    downs = dw.at[pl.ds(pl.multiple_of(c * LANES, LANES), LANES)]
    weight_copies = [
        pltpu.make_async_copy(gate_hbm.at[0], w4.at[:, pl.ds(lane, LANES)], w_sem),
        pltpu.make_async_copy(up_hbm.at[0], w4.at[:, pl.ds(pl.multiple_of(lane + LANES, LANES), LANES)], w_sem),
        pltpu.make_async_copy(down_hbm.at[0], downs, w_sem),
    ]
    weight_moves = [
        remote(ours, ours, x_sem.at[0], x_sem.at[1], sib),
        remote(downs, downs, x_sem.at[2], x_sem.at[3], sib),
    ]
    barrier = pltpu.get_barrier_semaphore()
    for d in (4, 3, 5, 2, 6, 1, 7):
        pl.semaphore_signal(barrier, inc=1, device_id=(z * NY + lax.rem(y + d, NY), t), device_id_type=MESH)
    for d in (2, -2, 1, -1):
        pl.semaphore_signal(barrier, inc=1, device_id=along_x(d), device_id_type=MESH)
    pl.semaphore_signal(barrier, inc=1, device_id=sib, device_id_type=MESH)
    for cp in table_copies + share_copies + weight_copies:
        cp.start()
    with jax.named_scope("barrier"):
        pl.semaphore_wait(barrier, 12 + jnp.where(z > 0, 1, 0))

    @pl.when(z < NZ - 1)
    def _():
        pl.semaphore_signal(barrier, inc=1, device_id=(e + NY, t), device_id_type=MESH)

    for zz in range(NZ - 1):
        @pl.when(zz < z)
        def _():
            pl.semaphore_signal(ready.at[z], inc=1, device_id=(zz * NY + y, t), device_id_type=MESH)

    for cp in table_copies:
        cp.wait()
    r0, r1 = routes_ref[0:1, :], routes_ref[1:2, :]
    w = mix_ref[...].astype(F32)
    w0, w1 = w[0:1, :], w[1:2, :]
    upper = (iota((tokn, tokn), 0) < iota((tokn, tokn), 1)).astype(BF)
    with jax.named_scope("share"):
        await_bytes(share, sh_sem)

    @pl.when(active)
    def _():
        both = jnp.concatenate([share[part].reshape(2 * tokn, QUAD) for part in range(2)], axis=1)
        blk = ZB * NY * 16

        def fill(b):
            rw = iota((blk, tokn), 0) + b * blk
            ex = rw >> 4
            q = rw & 15
            h0, h1 = ex == r0, ex == r1
            hit = h0 | h1
            rk = dot(hit.astype(BF), upper)
            wt = jnp.where(h0, w0, 0.0) + jnp.where(h1, w1, 0.0)
            one = jnp.where(hit & (rk == q.astype(F32)) & (q < CAP), 1.0, 0.0)
            two = jnp.where(hit & (rk == (q - CAP).astype(F32)) & (q >= CAP), wt, 0.0)
            sel = jnp.concatenate([one.astype(BF), two.astype(BF)], axis=1)
            v = dot(sel, both).astype(BF)
            for part in range(2):
                for ch in range(4):
                    at = part * QUAD + ch * LANES
                    msg[part, pl.ds(b * ZB, ZB), :, ch] = v[:, at:at + LANES].reshape(ZB, NY, 16, LANES)

        def tell(b, part):
            zz = pl.ds(b * ZB, ZB)
            for d in (4, 3, 5, 2, 6, 1, 7):
                yd = lax.rem(y + d, NY)
                remote(
                    msg.at[part, zz, yd, :, pl.ds(0, MSG)], ybuf.at[part, zz, y % HY, :, pl.ds(0, MSG)],
                    y_send, y_recv.at[part, b], (z * NY + yd, t)).start()
            ybuf[part, zz, y % HY] = msg[part, zz, y]

        for b in (0, 1):
            fill(b)
            tell(b, 0)

        @pl.when(z >= NZ // 2)
        def _():
            for b in (0, 1):
                tell(b, 1)

        for b in (2, 3):
            fill(b)
            tell(b, 0)

        @pl.when(z < NZ // 2)
        def _():
            for b in (0, 1):
                tell(b, 1)

        for b in (2, 3):
            tell(b, 1)

    await_bytes(w4.at[:, pl.ds(0, 3 * LANES)], w_sem)
    for cp in weight_moves:
        cp.start()

    def relay(b, part=0):
        with jax.named_scope(f"ywait{b}{'f' if part else ''}"):
            zz = pl.ds(b * ZB, ZB)

            @pl.when(active)
            def _():
                await_bytes(ybuf.at[part, zz, pl.ds(0, HY - 1), :, pl.ds(0, MSG)], y_recv.at[part, b])

            @pl.when(jnp.logical_not(active))
            def _():
                await_bytes(ybuf.at[part, zz, :, :, pl.ds(0, MSG)], y_recv.at[part, b])
        for zd in range(b * ZB, (b + 1) * ZB):
            @pl.when(zd == z)
            def _():
                zbuf[part, zd] = ybuf[part, zd]

            if part == 0:
                @pl.when(zd > z)
                def _():
                    with jax.named_scope(f"ready{zd}"):
                        pl.semaphore_wait(ready.at[zd], 1)

            @pl.when(zd != z)
            def _():
                remote(
                    ybuf.at[part, zd, :, :, pl.ds(0, MSG)], zbuf.at[part, z, :, :, pl.ds(0, MSG)],
                    z_send, z_recv.at[part, z // ZB], (zd * NY + y, t)).start()

    def unit(d, g):
        return rows.at[c, quad(d), :, pl.ds(g * RPG, RPG)]

    def to_sib(d, g):
        u = unit(d, g)
        remote(u, u, sib_send, sib_recv, sib).start()

    def landed(g, part):
        with jax.named_scope(f"zwait{g}{'f' if part else ''}"):
            @pl.when(z // ZB == g)
            def _():
                await_bytes(zbuf.at[part, pl.ds(0, ZB - 1), :, :, pl.ds(0, MSG)], z_recv.at[part, g])

            @pl.when(z // ZB != g)
            def _():
                await_bytes(zbuf.at[part, pl.ds(0, ZB), :, :, pl.ds(0, MSG)], z_recv.at[part, g])
        got = jnp.concatenate(
            [zbuf[part, pl.ds(g * ZB, ZB), :, ch].reshape(PER * 16, LANES) for ch in range(4)], axis=1)
        got = jnp.where((iota(got.shape, 0) & 15) < MSG, got, jnp.zeros_like(got))
        v = dot(perm[...], got)
        q = quad(2 * part)
        rows[c, q, 0, g * RPG:(g + 1) * RPG] = v[0:RPG].astype(BF)
        rows[c, q, 1, g * RPG:(g + 1) * RPG] = v[RPG:].astype(BF)

    def gather_out(g):
        landed(g, 0)
        u = unit(0, g)
        remote(u, u, ag_send, ag_recv.at[g], along_x(1)).start()
        remote(u, u, ag_send, ag_recv.at[g], along_x(-1)).start()
        to_sib(0, g)

    def gather_far(g):
        landed(g, 1)
        to_sib(2, g)

    def gather_in(g):
        await_bytes(rows.at[c, pl.ds(0, 2), :, pl.ds(g * RPG, RPG)], ag_recv.at[g])
        to_sib(-1, g)
        to_sib(1, g)

    def send_part(g, first, count, phase, to):
        at = (g, pl.ds(first, count), pl.ds(0, SENT))
        remote(sb.at[at], rb.at[at], rs_send, rs_recv.at[g, phase], along_x(to)).start()

    near, past = pl.ds(0, CUT), pl.ds(CUT, SENT - CUT)

    def products(g, d):
        at = pl.ds(g * RPG, RPG)
        q = quad(d)
        features = pl.ds(pl.multiple_of(q * QUAD, QUAD), QUAD)
        return dot(rows[c, q, 0, at], w4[features, :]), dot(rows[c, q, 1, at], dwt[features, :])

    def first_products(g, ds):
        each = [products(g, d) for d in ds]
        pre[g] = sum((a for a, _ in each[1:]), each[0][0])
        back[g] = sum((b for _, b in each[1:]), each[0][1])

    def compute(g, ds):
        at = pl.ds(g * RPG, RPG)
        pgu, bh = pre[g], back[g]
        for d in ds:
            a, b = products(g, d)
            pgu = pgu + a
            bh = bh + b
        pg = jnp.concatenate([pgu[:, 0:LANES], pgu[:, WIDE:WIDE + LANES]], axis=1)
        pu = jnp.concatenate([pgu[:, LANES:WIDE], pgu[:, WIDE + LANES:]], axis=1)
        sig = jax.nn.sigmoid(pg)
        act = pg * sig
        hidden = (act * pu).astype(BF)
        bg = (bh * pu * (sig * (1.0 + pg * (1.0 - sig)))).astype(BF)
        bu = (bh * act).astype(BF)
        b0 = jnp.concatenate([bg[:, 0:LANES], bu[:, 0:LANES]], axis=1)
        b1 = jnp.concatenate([bg[:, LANES:], bu[:, LANES:]], axis=1)
        b4 = jnp.concatenate([b0, b1], axis=1)
        hb = hidden.astype(F32) * bh
        hi = hb.astype(BF)
        lo = (hb - hi.astype(F32)).astype(BF)
        ones = jnp.ones((8, WIDE), BF)
        sums = dot_nt(ones, hi) + dot_nt(ones, lo)
        shi = sums.astype(BF).astype(F32)
        row = iota((8, RPG), 0)
        mixt[g, :, 0:RPG] = jnp.where(row == 0, shi, jnp.where(row == 1, sums - shi, 0.0))
        tile = mixt[g].astype(BF)
        def part(d):
            cols = pl.ds(pl.multiple_of(chip(d) * WIDE, WIDE), WIDE)
            return dot(b4, w4t[:, cols])

        def stored(d, i):
            v = part(d)
            sb[g, i, 0:RPG] = v[:, 0:LANES].astype(BF)
            sb[g, i, RPG:2 * RPG] = v[:, LANES:].astype(BF)
            sb[g, i, 2 * RPG:] = tile

        stored(4, 4)
        for rows_, to in ((near, 2), (past, -2)):
            remote(sb.at[g, 4, rows_], rb.at[g, 4, rows_], rs_send, rs_recv.at[g, 0], along_x(to)).start()
        for d, i, to in ((3, 0, 1), (5, 2, -1)):
            stored(d, i)
            stored(to % NX, i + 1)
            send_part(g, i, 2, 0, to)
        for d, i in ((2, 0), (6, 1), (0, 2)):
            v = part(d)
            pown[g, i, 0:RPG] = v[:, 0:LANES]
            pown[g, i, RPG:2 * RPG] = v[:, LANES:]
        first = c == 0
        bgu[c, at] = jnp.where(first, b0.astype(F32), b1.astype(F32)).astype(BF)
        obgu[g] = jnp.where(first, b1.astype(F32), b0.astype(F32)).astype(BF)
        hf = hidden.astype(F32)
        hid[c, at] = jnp.where(first, hf[:, 0:LANES], hf[:, LANES:]).astype(BF)
        ohid[g] = jnp.where(first, hf[:, LANES:], hf[:, 0:LANES]).astype(BF)
        remote(obgu.at[g], bgu.at[c, at], bh_send.at[0], bh_recv.at[0], sib).start()
        remote(ohid.at[g], hid.at[c, at], bh_send.at[1], bh_recv.at[1], sib).start()

    def chunk(g, i):
        return jnp.concatenate([pown[g, i], mixt[g]], axis=0)

    def scatter_two(g):
        await_bytes(rb.at[g, pl.ds(0, 5), pl.ds(0, SENT)], rs_recv.at[g, 0])
        v = chunk(g, 0) + rb[g, 0].astype(F32)
        sb[g, 5, 0:CUT] = (v[0:CUT] + rb[g, 4, 0:CUT].astype(F32)).astype(BF)
        sb[g, 5, CUT:] = v[CUT:].astype(BF)
        send_part(g, 5, 1, 1, 2)
        v = chunk(g, 1) + rb[g, 2].astype(F32)
        sb[g, 6, 0:CUT] = v[0:CUT].astype(BF)
        sb[g, 6, CUT:] = (v[CUT:] + rb[g, 4, CUT:].astype(F32)).astype(BF)
        send_part(g, 6, 1, 1, -2)

    def give_back(g):
        await_bytes(rb.at[g, pl.ds(0, 2), pl.ds(0, SENT)], rs_recv.at[g, 1])
        v = chunk(g, 2)
        for i in (1, 3, 5, 6):
            v = v + rb[g, i].astype(F32)
        sums = v[2 * RPG:2 * RPG + 1] + v[2 * RPG + 1:2 * RPG + 2]
        mhi = sums.astype(BF).astype(F32)
        mlo = sums - mhi
        br, bc = iota((LANES, LANES), 0), iota((LANES, LANES), 1)
        second = bc >= RPG
        row = bc - jnp.where(second, RPG, 0)
        src_of = div5(row)
        slot_of = row - src_of * CAP
        here = ((br >> 3) == src_of + jnp.where(second, PER, 0)) & (bc < 2 * RPG)
        spread = (here & ((br & 7) == slot_of))[:, 0:2 * RPG].astype(BF)
        take = (((br >> 3) & (PER - 1)) == div5(bc)) & ((br & 7) == CAP) & (bc < RPG)
        slot_r = br - div5(br) * CAP
        m = dot(spread, v[0:2 * RPG].astype(BF))
        m = m + dot(jnp.where(take, mhi, 0.0).astype(BF), (bc == slot_r).astype(BF))
        m = m + dot(jnp.where(take, mlo, 0.0).astype(BF), (bc == slot_r + 8).astype(BF))
        out[g] = m.astype(BF).reshape(2, PER, 8, LANES)
        for j in range(PER):
            i = (g * ZB + j // HY) * NY + mine_y * HY + j % HY
            for hf in range(2):
                here_ = (i == e) & (c == hf)

                @pl.when(here_)
                def _():
                    ret[e] = out[g, hf, j]

                @pl.when(jnp.logical_not(here_))
                def _():
                    remote(out.at[g, hf, j], ret.at[e], rt_send, rt_recv, (i, x * 2 + hf)).start()

    def grads():
        await_bytes(rows.at[1 - c], sib_recv)
        await_bytes(bgu.at[1 - c], bh_recv.at[0])
        await_bytes(hid.at[1 - c], bh_recv.at[1])
        for q in range(QUADS):
            at = slice(q * QUAD, (q + 1) * QUAD)
            v = dot_tn(rows[0, q, 0], bgu[0]) + dot_tn(rows[1, q, 0], bgu[1])
            gg_ref[at, :] = v[:, 0:LANES].astype(BF)
            ug_ref[at, :] = v[:, LANES:].astype(BF)
            dg_ref[:, at] = (dot_tn(hid[0], rows[0, q, 1]) + dot_tn(hid[1], rows[1, q, 1])).astype(BF)

    def turn():
        mixt[...] = jnp.zeros_like(mixt)
        pr, pc = iota((2 * RPG, 16 * PER), 0), iota((2 * RPG, 16 * PER), 1)
        second = pr >= RPG
        rest = pr - jnp.where(second, RPG, 0)
        src = div5(rest)
        perm[...] = (pc == src * 16 + (rest - src * CAP) + jnp.where(second, CAP, 0)).astype(BF)
        for cp in weight_moves:
            cp.wait_recv()
        for k in range(8):
            at = slice(k * WIDE, (k + 1) * WIDE)
            dwt[at, :] = dw[:, at].T
            for hf in range(2):
                w4t[hf * WIDE:(hf + 1) * WIDE, at] = w4[at, hf * WIDE:(hf + 1) * WIDE].T

    def tables():
        er = iota((nep, tokn), 0)
        oh0, oh1 = er == r0, er == r1
        ranks = dot((oh0 | oh1).astype(BF), upper)
        aux[0:1, :] = jnp.sum(jnp.where(oh0, ranks, 0.0), axis=0, keepdims=True)
        aux[1:2, :] = jnp.sum(jnp.where(oh1, ranks, 0.0), axis=0, keepdims=True)
        blk8 = 128
        for b in range(nep * 8 // blk8):
            rw = iota((blk8, tokn), 0) + b * blk8
            hit = ((rw >> 3) == r0) | ((rw >> 3) == r1)
            rk = dot(hit.astype(BF), upper)
            s = rw & 7
            p8[pl.ds(b * blk8, blk8), :] = (hit & (rk == s.astype(F32)) & (s < CAP)).astype(BF)
        aux[2:3, :] = w0
        aux[3:4, :] = w1
        aux[4:5, :] = r0.astype(F32)
        aux[5:6, :] = r1.astype(F32)
        aux[6:8, :] = jnp.zeros((2, tokn), F32)

    steps = {"A": gather_out, "B": gather_in, "H": gather_far, "E": scatter_two, "F": give_back}
    def run(plan):
        left = {}
        for step in plan.split():
            kind, g = step[0], int(step[1:] or 0)
            with jax.named_scope(step):
                if kind == "r":
                    relay(g)
                elif kind == "f":
                    relay(g, 1)
                elif kind in "st":
                    pl.when((z < NZ // 4) == (kind == "s"))(functools.partial(relay, g))
                elif kind == "P":
                    first_products(g, (0, 2))
                    left[g] = (-1, 1)
                elif kind == "Q":
                    first_products(g, (0, -1, 1))
                    left[g] = (2,)
                elif kind == "C":
                    compute(g, left[g])
                elif kind == "G":
                    grads()
                elif kind == "W":
                    turn()
                elif kind == "T":
                    tables()
                else:
                    steps[kind](g)

    early = z < NZ // 2
    pl.when(early)(functools.partial(run, EARLY))
    pl.when(jnp.logical_not(early))(functools.partial(run, LATE))

    for cp in weight_moves:
        cp.wait_send()

    @pl.when(active)
    def _():
        await_bytes(msg.at[:, :, pl.ds(0, NY - 1), :, pl.ds(0, MSG)], y_send)
        await_bytes(ret.at[pl.ds(0, nep - 1)], rt_send)

    @pl.when(jnp.logical_not(active))
    def _():
        await_bytes(ret, rt_send)

    await_bytes(zbuf.at[:, pl.ds(0, NZ - 1), :, :, pl.ds(0, MSG)], z_send)
    await_bytes(rows.at[0, pl.ds(0, 2)], ag_send)
    await_bytes(rows.at[0], sib_send)
    await_bytes(obgu, bh_send.at[0])
    await_bytes(ohid, bh_send.at[1])
    await_bytes(sb.at[:, :, pl.ds(0, SENT)], rs_send)

    with jax.named_scope("retwait"):
        @pl.when(active)
        def _():
            await_bytes(ret.at[pl.ds(0, nep - 1)], rt_recv)

        @pl.when(jnp.logical_not(active))
        def _():
            await_bytes(ret, rt_recv)


def finish(ret, p8, aux, gg, ug, dg, tg_ref, mg_ref, gg_out, ug_out, dg_out, tg, mg, sem):
    copies = [
        pltpu.make_async_copy(gg, gg_out.at[0], sem.at[0]),
        pltpu.make_async_copy(ug, ug_out.at[0], sem.at[1]),
        pltpu.make_async_copy(dg, dg_out.at[0], sem.at[2]),
    ]
    for cp in copies:
        cp.start()
    nep = ret.shape[0]
    tokn = p8.shape[1]
    back_rows = ret[...].reshape(nep * 8, LANES)
    tg[...] = dot_tn(p8[...], back_rows).astype(BF)
    copies.append(pltpu.make_async_copy(tg, tg_ref, sem.at[3]))
    copies[-1].start()
    sr, sc = iota((nep, nep * 8), 0), iota((nep, nep * 8), 1)
    mixes = dot((sc == sr * 8 + CAP).astype(BF), back_rows).astype(BF)
    lane = iota((LANES, tokn), 0).astype(F32)
    er = iota((nep, tokn), 0).astype(F32)
    done = []
    for k in range(2):
        seen = dot_tn(mixes, (er == aux[4 + k:5 + k, :]).astype(BF))
        rank = aux[k:k + 1, :]
        picked = jnp.where((lane == rank) | (lane == rank + 8.0), seen, 0.0)
        done.append(jnp.sum(picked, axis=0, keepdims=True) / aux[2 + k:3 + k, :])
    mg[...] = jnp.concatenate(done, axis=0).astype(BF)
    copies.append(pltpu.make_async_copy(mg, mg_ref, sem.at[4]))
    copies[-1].start()
    for cp in copies:
        cp.wait()


def solution(mesh):
    nep = NZ * NY

    def on_device(tokens, cotangent, mix_weights, routes, gate_proj, up_proj, down_proj):
        tokn, width = tokens.shape
        ff = gate_proj.shape[2]
        vm = pl.BlockSpec(memory_space=pltpu.VMEM)
        hbm = pl.BlockSpec(memory_space=pltpu.HBM)
        dma = pltpu.SemaphoreType.DMA
        parts = pl.pallas_call(
            kernel,
            out_shape=(
                jax.ShapeDtypeStruct((nep, 8, LANES), BF),
                jax.ShapeDtypeStruct((nep * 8, tokn), BF),
                jax.ShapeDtypeStruct((8, tokn), F32),
                jax.ShapeDtypeStruct((width, ff), BF),
                jax.ShapeDtypeStruct((width, ff), BF),
                jax.ShapeDtypeStruct((ff, width), BF),
            ),
            in_specs=[hbm] * 7,
            out_specs=[vm] * 6,
            scratch_shapes=[
                pltpu.VMEM((2, tokn), jnp.int32),
                pltpu.VMEM((2, tokn), BF),
                pltpu.VMEM((2, 2, tokn, QUAD), BF),
                pltpu.VMEM((2, NZ, NY, 4, 16, LANES), BF),
                pltpu.VMEM((2, NZ, HY, 4, 16, LANES), BF),
                pltpu.VMEM((2, NZ, HY, 4, 16, LANES), BF),
                pltpu.VMEM((2, QUADS, 2, GROUPS * RPG, QUAD), BF),
                pltpu.VMEM((width, 4 * LANES), BF),
                pltpu.VMEM((2 * ff, width), BF),
                pltpu.VMEM((4 * LANES, width), BF),
                pltpu.VMEM((width, 2 * ff), BF),
                pltpu.VMEM((2 * RPG, 16 * PER), BF),
                pltpu.VMEM((2, GROUPS * RPG, WIDE), BF),
                pltpu.VMEM((2, GROUPS * RPG, LANES), BF),
                pltpu.VMEM((GROUPS, RPG, WIDE), BF),
                pltpu.VMEM((GROUPS, RPG, LANES), BF),
                pltpu.VMEM((GROUPS, 8, LANES), F32),
                pltpu.VMEM((GROUPS, RPG, QUAD), F32),
                pltpu.VMEM((GROUPS, RPG, WIDE), F32),
                pltpu.VMEM((GROUPS, 3, 2 * RPG, LANES), F32),
                pltpu.VMEM((GROUPS, 7, TILE, LANES), BF),
                pltpu.VMEM((GROUPS, 7, TILE, LANES), BF),
                pltpu.VMEM((GROUPS, 2, PER, 8, LANES), BF),
                pltpu.SemaphoreType.REGULAR((NZ,)),
                dma((2,)), dma, dma, dma((4,)), dma, dma((2, GROUPS)), dma, dma((2, GROUPS)),
                dma, dma((GROUPS,)), dma, dma,
                dma((2,)), dma((2,)), dma, dma((GROUPS, 2)), dma, dma,
            ],
            compiler_params=pltpu.CompilerParams(
                collective_id=0, has_side_effects=True, vmem_limit_bytes=52 * 1024 * 1024),
        )(*(
            pltpu.with_memory_space_constraint(a, pltpu.HBM)
            for a in (tokens, cotangent, routes.T, mix_weights.T, gate_proj, up_proj, down_proj)))
        tg, mg, gg, ug, dg = pl.pallas_call(
            finish,
            out_shape=(
                jax.ShapeDtypeStruct((tokn, LANES), BF),
                jax.ShapeDtypeStruct((2, tokn), BF),
                jax.ShapeDtypeStruct((1, width, ff), BF),
                jax.ShapeDtypeStruct((1, width, ff), BF),
                jax.ShapeDtypeStruct((1, ff, width), BF),
            ),
            in_specs=[vm] * 6,
            out_specs=[hbm] * 5,
            scratch_shapes=[pltpu.VMEM((tokn, LANES), BF), pltpu.VMEM((2, tokn), BF), dma((5,))],
            compiler_params=pltpu.CompilerParams(vmem_limit_bytes=8 * 1024 * 1024),
        )(*parts)
        return tg, mg.T, gg, ug, dg

    in_specs = (
        P("ep", None), P("ep", None), P("ep", None), P("ep", None),
        P("ep", None, "tp"), P("ep", None, "tp"), P("ep", "tp", None),
    )
    out_specs = (
        P("ep", "tp"), P("ep", None), P("ep", None, "tp"), P("ep", None, "tp"), P("ep", "tp", None),
    )
    return jax.shard_map(on_device, mesh=mesh, in_specs=in_specs, out_specs=out_specs, check_vma=False)
```

```python
import functools

import jax
import jax.numpy as jnp
from jax import lax
from jax.experimental import pallas as pl
from jax.experimental.pallas import tpu as pltpu
from jax.sharding import PartitionSpec as P

MESH = pl.DeviceIdType.MESH
BF = jnp.bfloat16
F32 = jnp.float32
CAP = 5
MSG = 2 * CAP
LANES = 128
NX = NY = NZ = 8
GROUPS = 4
ZB = NZ // GROUPS
HY = NY // 2
PER = ZB * HY
RPG = PER * CAP
TILE = 2 * RPG + 8
SENT = 2 * RPG + 2
CUT = 40
WIDE = 2 * LANES
QUADS = 4
QUAD = 4 * LANES
EARLY = (
    "W r0 r1 D", "r2 s3 A0 A1", "t3 f0 f1 B0", "f2 f3 H0 Q0", "C0 A2 B1 H1",
    "P1 C1 A3 E0", "H2 B2 P2 C2", "H3 P3 B3 C3", "F0 E1 E2 E3", "T G F1 F2",
    "F3",
)
LATE = (
    "W r0 A0 r1", "f0 f1 a1 r2", "r3 B0 z1 Q0", "H0 C0 B1 H1", "P1 C1 A2 f2",
    "f3 E0 B2 y0", "H2 A3 P2 x0", "E1 C2 H3 P3", "B3 F1 C3 E2", "F2 E3 F3 T",
    "G",
)


def iota(shape, dim):
    return lax.broadcasted_iota(jnp.int32, shape, dim)


def dot(a, b):
    return jnp.dot(a, b, preferred_element_type=F32)


def dot_nt(a, b):
    return lax.dot_general(a, b, (((1,), (1,)), ((), ())), preferred_element_type=F32)


def dot_tn(a, b):
    return lax.dot_general(a, b, (((0,), (0,)), ((), ())), preferred_element_type=F32)


def div5(v):
    return (v * 205) >> 10


def kernel(
    tok_hbm, cot_hbm, routes_hbm, mix_hbm, gate_hbm, up_hbm, down_hbm,
    ret, p8, aux, gg_ref, ug_ref, dg_ref,
    routes_ref, mix_ref, share, msg, ybuf, zbuf, rows, w4, dw, w4t, dwt, perm, bgu, hid, obgu, ohid, mixt,
    pre, back, pown, sb, rb, out,
    ready, late, t_sem, sh_sem, w_sem, x_sem, y_send, y_recv, z_send, z_recv, ag_send, ag_recv, sib_send, sib_recv,
    bh_send, bh_recv, rs_send, rs_recv, rt_send, rt_recv,
):
    e = lax.axis_index("ep")
    t = lax.axis_index("tp")
    z, y = e // NY, e % NY
    x, c = t // 2, t % 2
    tokn = share.shape[2]
    nep = NZ * NY
    mine_y = 1 - c
    active = y // HY == mine_y

    def chip(d):
        return lax.rem(x + d + NX, NX)

    def quad(d):
        return lax.rem(x + d + NX, QUADS)

    sib = (e, x * 2 + (1 - c))

    def along_x(d):
        return (e, chip(d) * 2 + c)

    def remote(src, dst, ssem, rsem, to):
        return pltpu.make_async_remote_copy(
            src_ref=src, dst_ref=dst, send_sem=ssem, recv_sem=rsem, device_id=to, device_id_type=MESH)

    def await_bytes(ref, sem):
        pltpu.make_async_copy(ref, ref, sem).wait()

    cols = [pl.ds(pl.multiple_of(quad(d) * QUAD, QUAD), QUAD) for d in (0, 2)]
    table_copies = [
        pltpu.make_async_copy(routes_hbm, routes_ref, t_sem.at[0]),
        pltpu.make_async_copy(mix_hbm, mix_ref, t_sem.at[1]),
    ]
    share_copies = [
        pltpu.make_async_copy(ref.at[:, cols[part]], share.at[part, i], sh_sem)
        for part in range(2) for i, ref in enumerate((tok_hbm, cot_hbm))
    ]
    lane = pl.multiple_of(c * WIDE, WIDE)
    ours = w4.at[:, pl.ds(lane, WIDE)]
    downs = dw.at[pl.ds(pl.multiple_of(c * LANES, LANES), LANES)]
    weight_copies = [
        pltpu.make_async_copy(gate_hbm.at[0], w4.at[:, pl.ds(lane, LANES)], w_sem),
        pltpu.make_async_copy(up_hbm.at[0], w4.at[:, pl.ds(pl.multiple_of(lane + LANES, LANES), LANES)], w_sem),
        pltpu.make_async_copy(down_hbm.at[0], downs, w_sem),
    ]
    weight_moves = [
        remote(ours, ours, x_sem.at[0], x_sem.at[1], sib),
        remote(downs, downs, x_sem.at[2], x_sem.at[3], sib),
    ]
    barrier = pltpu.get_barrier_semaphore()
    column = (z == 0) & (t == 0)
    latecomer = column & (y == 0)

    @pl.when(jnp.logical_not(latecomer))
    def _():
        for d in (4, 3, 5, 2, 6, 1, 7):
            pl.semaphore_signal(barrier, inc=1, device_id=(z * NY + lax.rem(y + d, NY), t), device_id_type=MESH)

    for d in (2, -2, 1, -1):
        pl.semaphore_signal(barrier, inc=1, device_id=along_x(d), device_id_type=MESH)
    pl.semaphore_signal(barrier, inc=1, device_id=sib, device_id_type=MESH)
    for cp in table_copies + share_copies + weight_copies:
        cp.start()
    with jax.named_scope("barrier"):
        pl.semaphore_wait(barrier, 12 + jnp.where(z > 0, 1, 0) - jnp.where(column & (y > 0), 1, 0))

    @pl.when(z < NZ - 1)
    def _():
        pl.semaphore_signal(barrier, inc=1, device_id=(e + NY, t), device_id_type=MESH)

    @pl.when(latecomer)
    def _():
        for yy in range(HY, NY):
            pl.semaphore_signal(late, inc=1, device_id=(yy, t), device_id_type=MESH)

    for zz in range(NZ - 1):
        @pl.when(zz < z)
        def _():
            pl.semaphore_signal(ready.at[z], inc=1, device_id=(zz * NY + y, t), device_id_type=MESH)

    for cp in table_copies:
        cp.wait()
    r0, r1 = routes_ref[0:1, :], routes_ref[1:2, :]
    w = mix_ref[...].astype(F32)
    w0, w1 = w[0:1, :], w[1:2, :]
    upper = (iota((tokn, tokn), 0) < iota((tokn, tokn), 1)).astype(BF)
    with jax.named_scope("share"):
        await_bytes(share, sh_sem)

    def tell_one(b, part, yd):
        zz = pl.ds(b * ZB, ZB)
        remote(
            msg.at[part, zz, yd, :, pl.ds(0, MSG)], ybuf.at[part, zz, y % HY, :, pl.ds(0, MSG)],
            y_send, y_recv.at[part, b], (z * NY + yd, t)).start()

    def tell_latecomer():
        pl.semaphore_wait(late, 1)
        for part in range(2):
            for b in range(GROUPS):
                tell_one(b, part, 0)

    @pl.when(active)
    def _():
        both = jnp.concatenate([share[part].reshape(2 * tokn, QUAD) for part in range(2)], axis=1)
        blk = ZB * NY * 16

        def fill(b):
            rw = iota((blk, tokn), 0) + b * blk
            ex = rw >> 4
            q = rw & 15
            h0, h1 = ex == r0, ex == r1
            hit = h0 | h1
            rk = dot(hit.astype(BF), upper)
            wt = jnp.where(h0, w0, 0.0) + jnp.where(h1, w1, 0.0)
            one = jnp.where(hit & (rk == q.astype(F32)) & (q < CAP), 1.0, 0.0)
            two = jnp.where(hit & (rk == (q - CAP).astype(F32)) & (q >= CAP), wt, 0.0)
            sel = jnp.concatenate([one.astype(BF), two.astype(BF)], axis=1)
            v = dot(sel, both).astype(BF)
            for part in range(2):
                for ch in range(4):
                    at = part * QUAD + ch * LANES
                    msg[part, pl.ds(b * ZB, ZB), :, ch] = v[:, at:at + LANES].reshape(ZB, NY, 16, LANES)

        def tell(b, part):
            zz = pl.ds(b * ZB, ZB)
            for d in (4, 3, 5, 2, 6, 1, 7):
                yd = lax.rem(y + d, NY)
                pl.when(jnp.logical_not(column & (yd == 0)))(functools.partial(tell_one, b, part, yd))
            ybuf[part, zz, y % HY] = msg[part, zz, y]

        for b in (0, 1):
            fill(b)
            tell(b, 0)

        @pl.when(z >= NZ // 2)
        def _():
            for b in (0, 1):
                tell(b, 1)

        for b in (2, 3):
            fill(b)
            tell(b, 0)

        @pl.when(z < NZ // 2)
        def _():
            for b in (0, 1):
                tell(b, 1)

        for b in (2, 3):
            tell(b, 1)

    await_bytes(w4.at[:, pl.ds(0, 3 * LANES)], w_sem)
    for cp in weight_moves:
        cp.start()

    def relay(b, part=0):
        with jax.named_scope(f"ywait{b}{'f' if part else ''}"):
            zz = pl.ds(b * ZB, ZB)

            @pl.when(active)
            def _():
                await_bytes(ybuf.at[part, zz, pl.ds(0, HY - 1), :, pl.ds(0, MSG)], y_recv.at[part, b])

            @pl.when(jnp.logical_not(active))
            def _():
                await_bytes(ybuf.at[part, zz, :, :, pl.ds(0, MSG)], y_recv.at[part, b])
        for zd in range(b * ZB, (b + 1) * ZB):
            @pl.when(zd == z)
            def _():
                zbuf[part, zd] = ybuf[part, zd]

            if part == 0:
                @pl.when(zd > z)
                def _():
                    with jax.named_scope(f"ready{zd}"):
                        pl.semaphore_wait(ready.at[zd], 1)

            @pl.when(zd != z)
            def _():
                remote(
                    ybuf.at[part, zd, :, :, pl.ds(0, MSG)], zbuf.at[part, z, :, :, pl.ds(0, MSG)],
                    z_send, z_recv.at[part, z // ZB], (zd * NY + y, t)).start()

    def unit(d, g):
        return rows.at[c, quad(d), :, pl.ds(g * RPG, RPG)]

    def to_sib(d, g):
        u = unit(d, g)
        remote(u, u, sib_send, sib_recv, sib).start()

    def landed(g, part):
        with jax.named_scope(f"zwait{g}{'f' if part else ''}"):
            @pl.when(z // ZB == g)
            def _():
                await_bytes(zbuf.at[part, pl.ds(0, ZB - 1), :, :, pl.ds(0, MSG)], z_recv.at[part, g])

            @pl.when(z // ZB != g)
            def _():
                await_bytes(zbuf.at[part, pl.ds(0, ZB), :, :, pl.ds(0, MSG)], z_recv.at[part, g])
        got = jnp.concatenate(
            [zbuf[part, pl.ds(g * ZB, ZB), :, ch].reshape(PER * 16, LANES) for ch in range(4)], axis=1)
        got = jnp.where((iota(got.shape, 0) & 15) < MSG, got, jnp.zeros_like(got))
        v = dot(perm[...], got)
        q = quad(2 * part)
        rows[c, q, 0, g * RPG:(g + 1) * RPG] = v[0:RPG].astype(BF)
        rows[c, q, 1, g * RPG:(g + 1) * RPG] = v[RPG:].astype(BF)

    def gather_out(g):
        landed(g, 0)
        u = unit(0, g)
        remote(u, u, ag_send, ag_recv.at[g], along_x(1)).start()
        remote(u, u, ag_send, ag_recv.at[g], along_x(-1)).start()
        to_sib(0, g)

    def gather_far(g):
        landed(g, 1)
        to_sib(2, g)

    def gather_in(g):
        await_bytes(rows.at[c, pl.ds(0, 2), :, pl.ds(g * RPG, RPG)], ag_recv.at[g])
        to_sib(-1, g)
        to_sib(1, g)

    def send_part(g, first, count, phase, to):
        at = (g, pl.ds(first, count), pl.ds(0, SENT))
        remote(sb.at[at], rb.at[at], rs_send, rs_recv.at[g, phase], along_x(to)).start()

    near, past = pl.ds(0, CUT), pl.ds(CUT, SENT - CUT)

    def products(g, d):
        at = pl.ds(g * RPG, RPG)
        q = quad(d)
        features = pl.ds(pl.multiple_of(q * QUAD, QUAD), QUAD)
        return dot(rows[c, q, 0, at], w4[features, :]), dot(rows[c, q, 1, at], dwt[features, :])

    def first_products(g, ds):
        each = [products(g, d) for d in ds]
        pre[g] = sum((a for a, _ in each[1:]), each[0][0])
        back[g] = sum((b for _, b in each[1:]), each[0][1])

    def compute(g, ds):
        at = pl.ds(g * RPG, RPG)
        pgu, bh = pre[g], back[g]
        for d in ds:
            a, b = products(g, d)
            pgu = pgu + a
            bh = bh + b
        pg = jnp.concatenate([pgu[:, 0:LANES], pgu[:, WIDE:WIDE + LANES]], axis=1)
        pu = jnp.concatenate([pgu[:, LANES:WIDE], pgu[:, WIDE + LANES:]], axis=1)
        sig = jax.nn.sigmoid(pg)
        act = pg * sig
        hidden = (act * pu).astype(BF)
        bg = (bh * pu * (sig * (1.0 + pg * (1.0 - sig)))).astype(BF)
        bu = (bh * act).astype(BF)
        b0 = jnp.concatenate([bg[:, 0:LANES], bu[:, 0:LANES]], axis=1)
        b1 = jnp.concatenate([bg[:, LANES:], bu[:, LANES:]], axis=1)
        b4 = jnp.concatenate([b0, b1], axis=1)
        hb = hidden.astype(F32) * bh
        hi = hb.astype(BF)
        lo = (hb - hi.astype(F32)).astype(BF)
        ones = jnp.ones((8, WIDE), BF)
        sums = dot_nt(ones, hi) + dot_nt(ones, lo)
        shi = sums.astype(BF).astype(F32)
        row = iota((8, RPG), 0)
        mixt[g, :, 0:RPG] = jnp.where(row == 0, shi, jnp.where(row == 1, sums - shi, 0.0))
        tile = mixt[g].astype(BF)
        def part(d):
            cols = pl.ds(pl.multiple_of(chip(d) * WIDE, WIDE), WIDE)
            return dot(b4, w4t[:, cols])

        def stored(d, i):
            v = part(d)
            sb[g, i, 0:RPG] = v[:, 0:LANES].astype(BF)
            sb[g, i, RPG:2 * RPG] = v[:, LANES:].astype(BF)
            sb[g, i, 2 * RPG:] = tile

        stored(4, 4)
        for rows_, to in ((near, 2), (past, -2)):
            remote(sb.at[g, 4, rows_], rb.at[g, 4, rows_], rs_send, rs_recv.at[g, 0], along_x(to)).start()
        for d, i, to in ((3, 0, 1), (5, 2, -1)):
            stored(d, i)
            stored(to % NX, i + 1)
            send_part(g, i, 2, 0, to)
        for d, i in ((2, 0), (6, 1), (0, 2)):
            v = part(d)
            pown[g, i, 0:RPG] = v[:, 0:LANES]
            pown[g, i, RPG:2 * RPG] = v[:, LANES:]
        first = c == 0
        bgu[c, at] = jnp.where(first, b0.astype(F32), b1.astype(F32)).astype(BF)
        obgu[g] = jnp.where(first, b1.astype(F32), b0.astype(F32)).astype(BF)
        hf = hidden.astype(F32)
        hid[c, at] = jnp.where(first, hf[:, 0:LANES], hf[:, LANES:]).astype(BF)
        ohid[g] = jnp.where(first, hf[:, LANES:], hf[:, 0:LANES]).astype(BF)
        remote(obgu.at[g], bgu.at[c, at], bh_send.at[0], bh_recv.at[0], sib).start()
        remote(ohid.at[g], hid.at[c, at], bh_send.at[1], bh_recv.at[1], sib).start()

    def chunk(g, i):
        return jnp.concatenate([pown[g, i], mixt[g]], axis=0)

    def scatter_two(g):
        await_bytes(rb.at[g, pl.ds(0, 5), pl.ds(0, SENT)], rs_recv.at[g, 0])
        v = chunk(g, 0) + rb[g, 0].astype(F32)
        sb[g, 5, 0:CUT] = (v[0:CUT] + rb[g, 4, 0:CUT].astype(F32)).astype(BF)
        sb[g, 5, CUT:] = v[CUT:].astype(BF)
        send_part(g, 5, 1, 1, 2)
        v = chunk(g, 1) + rb[g, 2].astype(F32)
        sb[g, 6, 0:CUT] = v[0:CUT].astype(BF)
        sb[g, 6, CUT:] = (v[CUT:] + rb[g, 4, CUT:].astype(F32)).astype(BF)
        send_part(g, 6, 1, 1, -2)

    def give_back(g):
        await_bytes(rb.at[g, pl.ds(0, 2), pl.ds(0, SENT)], rs_recv.at[g, 1])
        v = chunk(g, 2)
        for i in (1, 3, 5, 6):
            v = v + rb[g, i].astype(F32)
        sums = v[2 * RPG:2 * RPG + 1] + v[2 * RPG + 1:2 * RPG + 2]
        mhi = sums.astype(BF).astype(F32)
        mlo = sums - mhi
        br, bc = iota((LANES, LANES), 0), iota((LANES, LANES), 1)
        second = bc >= RPG
        row = bc - jnp.where(second, RPG, 0)
        src_of = div5(row)
        slot_of = row - src_of * CAP
        here = ((br >> 3) == src_of + jnp.where(second, PER, 0)) & (bc < 2 * RPG)
        spread = (here & ((br & 7) == slot_of))[:, 0:2 * RPG].astype(BF)
        take = (((br >> 3) & (PER - 1)) == div5(bc)) & ((br & 7) == CAP) & (bc < RPG)
        slot_r = br - div5(br) * CAP
        m = dot(spread, v[0:2 * RPG].astype(BF))
        m = m + dot(jnp.where(take, mhi, 0.0).astype(BF), (bc == slot_r).astype(BF))
        m = m + dot(jnp.where(take, mlo, 0.0).astype(BF), (bc == slot_r + 8).astype(BF))
        out[g] = m.astype(BF).reshape(2, PER, 8, LANES)
        for j in range(PER):
            i = (g * ZB + j // HY) * NY + mine_y * HY + j % HY
            for hf in range(2):
                here_ = (i == e) & (c == hf)

                @pl.when(here_)
                def _():
                    ret[e] = out[g, hf, j]

                @pl.when(jnp.logical_not(here_))
                def _():
                    remote(out.at[g, hf, j], ret.at[e], rt_send, rt_recv, (i, x * 2 + hf)).start()

    def grads():
        await_bytes(rows.at[1 - c], sib_recv)
        await_bytes(bgu.at[1 - c], bh_recv.at[0])
        await_bytes(hid.at[1 - c], bh_recv.at[1])
        for q in range(QUADS):
            at = slice(q * QUAD, (q + 1) * QUAD)
            v = dot_tn(rows[0, q, 0], bgu[0]) + dot_tn(rows[1, q, 0], bgu[1])
            gg_ref[at, :] = v[:, 0:LANES].astype(BF)
            ug_ref[at, :] = v[:, LANES:].astype(BF)
            dg_ref[:, at] = (dot_tn(hid[0], rows[0, q, 1]) + dot_tn(hid[1], rows[1, q, 1])).astype(BF)

    def turn():
        mixt[...] = jnp.zeros_like(mixt)
        pr, pc = iota((2 * RPG, 16 * PER), 0), iota((2 * RPG, 16 * PER), 1)
        second = pr >= RPG
        rest = pr - jnp.where(second, RPG, 0)
        src = div5(rest)
        perm[...] = (pc == src * 16 + (rest - src * CAP) + jnp.where(second, CAP, 0)).astype(BF)
        for cp in weight_moves:
            cp.wait_recv()
        for k in range(8):
            at = slice(k * WIDE, (k + 1) * WIDE)
            dwt[at, :] = dw[:, at].T
            for hf in range(2):
                w4t[hf * WIDE:(hf + 1) * WIDE, at] = w4[at, hf * WIDE:(hf + 1) * WIDE].T

    def tables():
        er = iota((nep, tokn), 0)
        oh0, oh1 = er == r0, er == r1
        ranks = dot((oh0 | oh1).astype(BF), upper)
        aux[0:1, :] = jnp.sum(jnp.where(oh0, ranks, 0.0), axis=0, keepdims=True)
        aux[1:2, :] = jnp.sum(jnp.where(oh1, ranks, 0.0), axis=0, keepdims=True)
        blk8 = 128
        for b in range(nep * 8 // blk8):
            rw = iota((blk8, tokn), 0) + b * blk8
            hit = ((rw >> 3) == r0) | ((rw >> 3) == r1)
            rk = dot(hit.astype(BF), upper)
            s = rw & 7
            p8[pl.ds(b * blk8, blk8), :] = (hit & (rk == s.astype(F32)) & (s < CAP)).astype(BF)
        aux[2:3, :] = w0
        aux[3:4, :] = w1
        aux[4:5, :] = r0.astype(F32)
        aux[5:6, :] = r1.astype(F32)
        aux[6:8, :] = jnp.zeros((2, tokn), F32)

    steps = {"A": gather_out, "B": gather_in, "H": gather_far, "E": scatter_two, "F": give_back}
    def run(plan):
        left = {}
        for step in " ".join(plan).split():
            kind, g = step[0], int(step[1:] or 0)
            with jax.named_scope(step):
                if kind == "r":
                    relay(g)
                elif kind == "f":
                    relay(g, 1)
                elif kind in "st":
                    pl.when((z < NZ // 4) == (kind == "s"))(functools.partial(relay, g))
                elif kind in "az":
                    pl.when(c == int(kind == "z"))(functools.partial(gather_out, g))
                elif kind == "D":
                    pl.when(column & active)(tell_latecomer)
                elif kind in "xy":
                    pl.when(c == int(kind == "y"))(functools.partial(give_back, g))
                elif kind == "P":
                    first_products(g, (0, 2))
                    left[g] = (-1, 1)
                elif kind == "Q":
                    first_products(g, (0, -1, 1))
                    left[g] = (2,)
                elif kind == "C":
                    compute(g, left[g])
                elif kind == "G":
                    grads()
                elif kind == "W":
                    turn()
                elif kind == "T":
                    tables()
                else:
                    steps[kind](g)

    early = z < NZ // 2
    pl.when(early)(functools.partial(run, EARLY))
    pl.when(jnp.logical_not(early))(functools.partial(run, LATE))

    for cp in weight_moves:
        cp.wait_send()

    @pl.when(active)
    def _():
        await_bytes(msg.at[:, :, pl.ds(0, NY - 1), :, pl.ds(0, MSG)], y_send)
        await_bytes(ret.at[pl.ds(0, nep - 1)], rt_send)

    @pl.when(jnp.logical_not(active))
    def _():
        await_bytes(ret, rt_send)

    await_bytes(zbuf.at[:, pl.ds(0, NZ - 1), :, :, pl.ds(0, MSG)], z_send)
    await_bytes(rows.at[0, pl.ds(0, 2)], ag_send)
    await_bytes(rows.at[0], sib_send)
    await_bytes(obgu, bh_send.at[0])
    await_bytes(ohid, bh_send.at[1])
    await_bytes(sb.at[:, :, pl.ds(0, SENT)], rs_send)

    with jax.named_scope("retwait"):
        @pl.when(active)
        def _():
            await_bytes(ret.at[pl.ds(0, nep - 1)], rt_recv)

        @pl.when(jnp.logical_not(active))
        def _():
            await_bytes(ret, rt_recv)


def finish(ret, p8, aux, gg, ug, dg, tg_ref, mg_ref, gg_out, ug_out, dg_out, tg, mg, sem):
    copies = [
        pltpu.make_async_copy(gg, gg_out.at[0], sem.at[0]),
        pltpu.make_async_copy(ug, ug_out.at[0], sem.at[1]),
        pltpu.make_async_copy(dg, dg_out.at[0], sem.at[2]),
    ]
    for cp in copies:
        cp.start()
    nep = ret.shape[0]
    tokn = p8.shape[1]
    back_rows = ret[...].reshape(nep * 8, LANES)
    tg[...] = dot_tn(p8[...], back_rows).astype(BF)
    copies.append(pltpu.make_async_copy(tg, tg_ref, sem.at[3]))
    copies[-1].start()
    sr, sc = iota((nep, nep * 8), 0), iota((nep, nep * 8), 1)
    mixes = dot((sc == sr * 8 + CAP).astype(BF), back_rows).astype(BF)
    lane = iota((LANES, tokn), 0).astype(F32)
    er = iota((nep, tokn), 0).astype(F32)
    done = []
    for k in range(2):
        seen = dot_tn(mixes, (er == aux[4 + k:5 + k, :]).astype(BF))
        rank = aux[k:k + 1, :]
        picked = jnp.where((lane == rank) | (lane == rank + 8.0), seen, 0.0)
        done.append(jnp.sum(picked, axis=0, keepdims=True) / aux[2 + k:3 + k, :])
    mg[...] = jnp.concatenate(done, axis=0).astype(BF)
    copies.append(pltpu.make_async_copy(mg, mg_ref, sem.at[4]))
    copies[-1].start()
    for cp in copies:
        cp.wait()


def solution(mesh):
    nep = NZ * NY

    def on_device(tokens, cotangent, mix_weights, routes, gate_proj, up_proj, down_proj):
        tokn, width = tokens.shape
        ff = gate_proj.shape[2]
        vm = pl.BlockSpec(memory_space=pltpu.VMEM)
        hbm = pl.BlockSpec(memory_space=pltpu.HBM)
        dma = pltpu.SemaphoreType.DMA
        parts = pl.pallas_call(
            kernel,
            out_shape=(
                jax.ShapeDtypeStruct((nep, 8, LANES), BF),
                jax.ShapeDtypeStruct((nep * 8, tokn), BF),
                jax.ShapeDtypeStruct((8, tokn), F32),
                jax.ShapeDtypeStruct((width, ff), BF),
                jax.ShapeDtypeStruct((width, ff), BF),
                jax.ShapeDtypeStruct((ff, width), BF),
            ),
            in_specs=[hbm] * 7,
            out_specs=[vm] * 6,
            scratch_shapes=[
                pltpu.VMEM((2, tokn), jnp.int32),
                pltpu.VMEM((2, tokn), BF),
                pltpu.VMEM((2, 2, tokn, QUAD), BF),
                pltpu.VMEM((2, NZ, NY, 4, 16, LANES), BF),
                pltpu.VMEM((2, NZ, HY, 4, 16, LANES), BF),
                pltpu.VMEM((2, NZ, HY, 4, 16, LANES), BF),
                pltpu.VMEM((2, QUADS, 2, GROUPS * RPG, QUAD), BF),
                pltpu.VMEM((width, 4 * LANES), BF),
                pltpu.VMEM((2 * ff, width), BF),
                pltpu.VMEM((4 * LANES, width), BF),
                pltpu.VMEM((width, 2 * ff), BF),
                pltpu.VMEM((2 * RPG, 16 * PER), BF),
                pltpu.VMEM((2, GROUPS * RPG, WIDE), BF),
                pltpu.VMEM((2, GROUPS * RPG, LANES), BF),
                pltpu.VMEM((GROUPS, RPG, WIDE), BF),
                pltpu.VMEM((GROUPS, RPG, LANES), BF),
                pltpu.VMEM((GROUPS, 8, LANES), F32),
                pltpu.VMEM((GROUPS, RPG, QUAD), F32),
                pltpu.VMEM((GROUPS, RPG, WIDE), F32),
                pltpu.VMEM((GROUPS, 3, 2 * RPG, LANES), F32),
                pltpu.VMEM((GROUPS, 7, TILE, LANES), BF),
                pltpu.VMEM((GROUPS, 7, TILE, LANES), BF),
                pltpu.VMEM((GROUPS, 2, PER, 8, LANES), BF),
                pltpu.SemaphoreType.REGULAR((NZ,)),
                pltpu.SemaphoreType.REGULAR,
                dma((2,)), dma, dma, dma((4,)), dma, dma((2, GROUPS)), dma, dma((2, GROUPS)),
                dma, dma((GROUPS,)), dma, dma,
                dma((2,)), dma((2,)), dma, dma((GROUPS, 2)), dma, dma,
            ],
            compiler_params=pltpu.CompilerParams(
                collective_id=0, has_side_effects=True, vmem_limit_bytes=52 * 1024 * 1024),
        )(*(
            pltpu.with_memory_space_constraint(a, pltpu.HBM)
            for a in (tokens, cotangent, routes.T, mix_weights.T, gate_proj, up_proj, down_proj)))
        tg, mg, gg, ug, dg = pl.pallas_call(
            finish,
            out_shape=(
                jax.ShapeDtypeStruct((tokn, LANES), BF),
                jax.ShapeDtypeStruct((2, tokn), BF),
                jax.ShapeDtypeStruct((1, width, ff), BF),
                jax.ShapeDtypeStruct((1, width, ff), BF),
                jax.ShapeDtypeStruct((1, ff, width), BF),
            ),
            in_specs=[vm] * 6,
            out_specs=[hbm] * 5,
            scratch_shapes=[pltpu.VMEM((tokn, LANES), BF), pltpu.VMEM((2, tokn), BF), dma((5,))],
            compiler_params=pltpu.CompilerParams(vmem_limit_bytes=8 * 1024 * 1024),
        )(*parts)
        return tg, mg.T, gg, ug, dg

    in_specs = (
        P("ep", None), P("ep", None), P("ep", None), P("ep", None),
        P("ep", None, "tp"), P("ep", None, "tp"), P("ep", "tp", None),
    )
    out_specs = (
        P("ep", "tp"), P("ep", None), P("ep", None, "tp"), P("ep", None, "tp"), P("ep", "tp", None),
    )
    return jax.shard_map(on_device, mesh=mesh, in_specs=in_specs, out_specs=out_specs, check_vma=False)
```

```python
import functools

import jax
import jax.numpy as jnp
from jax import lax
from jax.experimental import pallas as pl
from jax.experimental.pallas import tpu as pltpu
from jax.sharding import PartitionSpec as P

MESH = pl.DeviceIdType.MESH
BF = jnp.bfloat16
F32 = jnp.float32
CAP = 5
MSG = 2 * CAP
LANES = 128
NX = NY = NZ = 8
GROUPS = 4
ZB = NZ // GROUPS
HY = NY // 2
PER = ZB * HY
RPG = PER * CAP
TILE = 2 * RPG + 8
SENT = 2 * RPG + 2
CUT = 40
WIDE = 2 * LANES
QUADS = 4
QUAD = 4 * LANES
EARLY = (
    "W r0 r1 D", "r2 s3 A0 A1", "t3 f0 f1 B0", "f2 f3 H0 Q0", "C0 A2 B1 H1",
    "P1 C1 A3 E0", "H2 B2 P2 C2", "H3 P3 B3 C3", "F0 E1 E2 E3", "T G F1 F2",
    "F3",
)
LATE = (
    "W r0 A0 r1", "f0 f1 a1 r2", "r3 B0 z1 Q0", "H0 C0 B1 H1", "P1 C1 A2 f2",
    "f3 E0 A3 E1", "y0 H2 B2 P2", "x0 C2 H3 P3", "F1 B3 C3 E2", "E3 F2 F3 T",
    "G",
)


def iota(shape, dim):
    return lax.broadcasted_iota(jnp.int32, shape, dim)


def dot(a, b):
    return jnp.dot(a, b, preferred_element_type=F32)


def dot_nt(a, b):
    return lax.dot_general(a, b, (((1,), (1,)), ((), ())), preferred_element_type=F32)


def dot_tn(a, b):
    return lax.dot_general(a, b, (((0,), (0,)), ((), ())), preferred_element_type=F32)


def div5(v):
    return (v * 205) >> 10


def kernel(
    tok_hbm, cot_hbm, routes_hbm, mix_hbm, gate_hbm, up_hbm, down_hbm,
    ret, p8, aux, gg_ref, ug_ref, dg_ref,
    routes_ref, mix_ref, share, msg, ybuf, zbuf, rows, w4, dw, w4t, dwt, perm, bgu, hid, obgu, ohid, mixt,
    pre, back, pown, sb, rb, out,
    ready, late, t_sem, sh_sem, w_sem, x_sem, y_send, y_recv, z_send, z_recv, ag_send, ag_recv, sib_send, sib_recv,
    bh_send, bh_recv, rs_send, rs_recv, rt_send, rt_recv,
):
    e = lax.axis_index("ep")
    t = lax.axis_index("tp")
    z, y = e // NY, e % NY
    x, c = t // 2, t % 2
    tokn = share.shape[2]
    nep = NZ * NY
    mine_y = 1 - c
    active = y // HY == mine_y

    def chip(d):
        return lax.rem(x + d + NX, NX)

    def quad(d):
        return lax.rem(x + d + NX, QUADS)

    sib = (e, x * 2 + (1 - c))

    def along_x(d):
        return (e, chip(d) * 2 + c)

    def remote(src, dst, ssem, rsem, to):
        return pltpu.make_async_remote_copy(
            src_ref=src, dst_ref=dst, send_sem=ssem, recv_sem=rsem, device_id=to, device_id_type=MESH)

    def await_bytes(ref, sem):
        pltpu.make_async_copy(ref, ref, sem).wait()

    cols = [pl.ds(pl.multiple_of(quad(d) * QUAD, QUAD), QUAD) for d in (0, 2)]
    table_copies = [
        pltpu.make_async_copy(routes_hbm, routes_ref, t_sem.at[0]),
        pltpu.make_async_copy(mix_hbm, mix_ref, t_sem.at[1]),
    ]
    share_copies = [
        pltpu.make_async_copy(ref.at[:, cols[part]], share.at[part, i], sh_sem)
        for part in range(2) for i, ref in enumerate((tok_hbm, cot_hbm))
    ]
    lane = pl.multiple_of(c * WIDE, WIDE)
    ours = w4.at[:, pl.ds(lane, WIDE)]
    downs = dw.at[pl.ds(pl.multiple_of(c * LANES, LANES), LANES)]
    weight_copies = [
        pltpu.make_async_copy(gate_hbm.at[0], w4.at[:, pl.ds(lane, LANES)], w_sem),
        pltpu.make_async_copy(up_hbm.at[0], w4.at[:, pl.ds(pl.multiple_of(lane + LANES, LANES), LANES)], w_sem),
        pltpu.make_async_copy(down_hbm.at[0], downs, w_sem),
    ]
    weight_moves = [
        remote(ours, ours, x_sem.at[0], x_sem.at[1], sib),
        remote(downs, downs, x_sem.at[2], x_sem.at[3], sib),
    ]
    barrier = pltpu.get_barrier_semaphore()
    column = (z == 0) & (t == 0)
    latecomer = column & (y == 0)

    @pl.when(jnp.logical_not(latecomer))
    def _():
        for d in (4, 3, 5, 2, 6, 1, 7):
            pl.semaphore_signal(barrier, inc=1, device_id=(z * NY + lax.rem(y + d, NY), t), device_id_type=MESH)

    for d in (2, -2, 1, -1):
        pl.semaphore_signal(barrier, inc=1, device_id=along_x(d), device_id_type=MESH)
    pl.semaphore_signal(barrier, inc=1, device_id=sib, device_id_type=MESH)
    for cp in table_copies + share_copies + weight_copies:
        cp.start()
    with jax.named_scope("barrier"):
        pl.semaphore_wait(barrier, 12 + jnp.where(z > 0, 1, 0) - jnp.where(column & (y > 0), 1, 0))

    @pl.when(z < NZ - 1)
    def _():
        pl.semaphore_signal(barrier, inc=1, device_id=(e + NY, t), device_id_type=MESH)

    @pl.when(latecomer)
    def _():
        for yy in range(HY, NY):
            pl.semaphore_signal(late, inc=1, device_id=(yy, t), device_id_type=MESH)

    for zz in range(NZ - 1):
        @pl.when(zz < z)
        def _():
            pl.semaphore_signal(ready.at[z], inc=1, device_id=(zz * NY + y, t), device_id_type=MESH)

    for cp in table_copies:
        cp.wait()
    r0, r1 = routes_ref[0:1, :], routes_ref[1:2, :]
    w = mix_ref[...].astype(F32)
    w0, w1 = w[0:1, :], w[1:2, :]
    upper = (iota((tokn, tokn), 0) < iota((tokn, tokn), 1)).astype(BF)
    with jax.named_scope("share"):
        await_bytes(share, sh_sem)

    def tell_one(b, part, yd):
        zz = pl.ds(b * ZB, ZB)
        remote(
            msg.at[part, zz, yd, :, pl.ds(0, MSG)], ybuf.at[part, zz, y % HY, :, pl.ds(0, MSG)],
            y_send, y_recv.at[part, b], (z * NY + yd, t)).start()

    def tell_latecomer():
        pl.semaphore_wait(late, 1)
        for part in range(2):
            for b in range(GROUPS):
                tell_one(b, part, 0)

    @pl.when(active)
    def _():
        both = jnp.concatenate([share[part].reshape(2 * tokn, QUAD) for part in range(2)], axis=1)
        blk = ZB * NY * 16

        def fill(b):
            rw = iota((blk, tokn), 0) + b * blk
            ex = rw >> 4
            q = rw & 15
            h0, h1 = ex == r0, ex == r1
            hit = h0 | h1
            rk = dot(hit.astype(BF), upper)
            wt = jnp.where(h0, w0, 0.0) + jnp.where(h1, w1, 0.0)
            one = jnp.where(hit & (rk == q.astype(F32)) & (q < CAP), 1.0, 0.0)
            two = jnp.where(hit & (rk == (q - CAP).astype(F32)) & (q >= CAP), wt, 0.0)
            sel = jnp.concatenate([one.astype(BF), two.astype(BF)], axis=1)
            v = dot(sel, both).astype(BF)
            for part in range(2):
                for ch in range(4):
                    at = part * QUAD + ch * LANES
                    msg[part, pl.ds(b * ZB, ZB), :, ch] = v[:, at:at + LANES].reshape(ZB, NY, 16, LANES)

        def tell(b, part):
            zz = pl.ds(b * ZB, ZB)
            for d in (4, 3, 5, 2, 6, 1, 7):
                yd = lax.rem(y + d, NY)
                pl.when(jnp.logical_not(column & (yd == 0)))(functools.partial(tell_one, b, part, yd))
            ybuf[part, zz, y % HY] = msg[part, zz, y]

        for b in (0, 1):
            fill(b)
            tell(b, 0)

        @pl.when(z >= NZ // 2)
        def _():
            for b in (0, 1):
                tell(b, 1)

        for b in (2, 3):
            fill(b)
            tell(b, 0)

        @pl.when(z < NZ // 2)
        def _():
            for b in (0, 1):
                tell(b, 1)

        for b in (2, 3):
            tell(b, 1)

    await_bytes(w4.at[:, pl.ds(0, 3 * LANES)], w_sem)
    for cp in weight_moves:
        cp.start()

    def relay(b, part=0):
        with jax.named_scope(f"ywait{b}{'f' if part else ''}"):
            zz = pl.ds(b * ZB, ZB)

            @pl.when(active)
            def _():
                await_bytes(ybuf.at[part, zz, pl.ds(0, HY - 1), :, pl.ds(0, MSG)], y_recv.at[part, b])

            @pl.when(jnp.logical_not(active))
            def _():
                await_bytes(ybuf.at[part, zz, :, :, pl.ds(0, MSG)], y_recv.at[part, b])
        for zd in range(b * ZB, (b + 1) * ZB):
            @pl.when(zd == z)
            def _():
                zbuf[part, zd] = ybuf[part, zd]

            if part == 0:
                @pl.when(zd > z)
                def _():
                    with jax.named_scope(f"ready{zd}"):
                        pl.semaphore_wait(ready.at[zd], 1)

            @pl.when(zd != z)
            def _():
                remote(
                    ybuf.at[part, zd, :, :, pl.ds(0, MSG)], zbuf.at[part, z, :, :, pl.ds(0, MSG)],
                    z_send, z_recv.at[part, z // ZB], (zd * NY + y, t)).start()

    def unit(d, g):
        return rows.at[c, quad(d), :, pl.ds(g * RPG, RPG)]

    def to_sib(d, g):
        u = unit(d, g)
        remote(u, u, sib_send, sib_recv, sib).start()

    def landed(g, part):
        with jax.named_scope(f"zwait{g}{'f' if part else ''}"):
            @pl.when(z // ZB == g)
            def _():
                await_bytes(zbuf.at[part, pl.ds(0, ZB - 1), :, :, pl.ds(0, MSG)], z_recv.at[part, g])

            @pl.when(z // ZB != g)
            def _():
                await_bytes(zbuf.at[part, pl.ds(0, ZB), :, :, pl.ds(0, MSG)], z_recv.at[part, g])
        got = jnp.concatenate(
            [zbuf[part, pl.ds(g * ZB, ZB), :, ch].reshape(PER * 16, LANES) for ch in range(4)], axis=1)
        got = jnp.where((iota(got.shape, 0) & 15) < MSG, got, jnp.zeros_like(got))
        v = dot(perm[...], got)
        q = quad(2 * part)
        rows[c, q, 0, g * RPG:(g + 1) * RPG] = v[0:RPG].astype(BF)
        rows[c, q, 1, g * RPG:(g + 1) * RPG] = v[RPG:].astype(BF)

    def gather_out(g):
        landed(g, 0)
        u = unit(0, g)
        remote(u, u, ag_send, ag_recv.at[g], along_x(1)).start()
        remote(u, u, ag_send, ag_recv.at[g], along_x(-1)).start()
        to_sib(0, g)

    def gather_far(g):
        landed(g, 1)
        to_sib(2, g)

    def gather_in(g):
        await_bytes(rows.at[c, pl.ds(0, 2), :, pl.ds(g * RPG, RPG)], ag_recv.at[g])
        to_sib(-1, g)
        to_sib(1, g)

    def send_part(g, first, count, phase, to):
        at = (g, pl.ds(first, count), pl.ds(0, SENT))
        remote(sb.at[at], rb.at[at], rs_send, rs_recv.at[g, phase], along_x(to)).start()

    near, past = pl.ds(0, CUT), pl.ds(CUT, SENT - CUT)

    def products(g, d):
        at = pl.ds(g * RPG, RPG)
        q = quad(d)
        features = pl.ds(pl.multiple_of(q * QUAD, QUAD), QUAD)
        return dot(rows[c, q, 0, at], w4[features, :]), dot(rows[c, q, 1, at], dwt[features, :])

    def first_products(g, ds):
        each = [products(g, d) for d in ds]
        pre[g] = sum((a for a, _ in each[1:]), each[0][0])
        back[g] = sum((b for _, b in each[1:]), each[0][1])

    def compute(g, ds):
        at = pl.ds(g * RPG, RPG)
        pgu, bh = pre[g], back[g]
        for d in ds:
            a, b = products(g, d)
            pgu = pgu + a
            bh = bh + b
        pg = jnp.concatenate([pgu[:, 0:LANES], pgu[:, WIDE:WIDE + LANES]], axis=1)
        pu = jnp.concatenate([pgu[:, LANES:WIDE], pgu[:, WIDE + LANES:]], axis=1)
        sig = jax.nn.sigmoid(pg)
        act = pg * sig
        hidden = (act * pu).astype(BF)
        bg = (bh * pu * (sig * (1.0 + pg * (1.0 - sig)))).astype(BF)
        bu = (bh * act).astype(BF)
        b0 = jnp.concatenate([bg[:, 0:LANES], bu[:, 0:LANES]], axis=1)
        b1 = jnp.concatenate([bg[:, LANES:], bu[:, LANES:]], axis=1)
        b4 = jnp.concatenate([b0, b1], axis=1)
        hb = hidden.astype(F32) * bh
        hi = hb.astype(BF)
        lo = (hb - hi.astype(F32)).astype(BF)
        ones = jnp.ones((8, WIDE), BF)
        sums = dot_nt(ones, hi) + dot_nt(ones, lo)
        shi = sums.astype(BF).astype(F32)
        row = iota((8, RPG), 0)
        mixt[g, :, 0:RPG] = jnp.where(row == 0, shi, jnp.where(row == 1, sums - shi, 0.0))
        tile = mixt[g].astype(BF)
        def part(d):
            cols = pl.ds(pl.multiple_of(chip(d) * WIDE, WIDE), WIDE)
            return dot(b4, w4t[:, cols])

        def stored(d, i):
            v = part(d)
            sb[g, i, 0:RPG] = v[:, 0:LANES].astype(BF)
            sb[g, i, RPG:2 * RPG] = v[:, LANES:].astype(BF)
            sb[g, i, 2 * RPG:] = tile

        stored(4, 4)
        for rows_, to in ((near, 2), (past, -2)):
            remote(sb.at[g, 4, rows_], rb.at[g, 4, rows_], rs_send, rs_recv.at[g, 0], along_x(to)).start()
        for d, i, to in ((3, 0, 1), (5, 2, -1)):
            stored(d, i)
            stored(to % NX, i + 1)
            send_part(g, i, 2, 0, to)
        for d, i in ((2, 0), (6, 1), (0, 2)):
            v = part(d)
            pown[g, i, 0:RPG] = v[:, 0:LANES]
            pown[g, i, RPG:2 * RPG] = v[:, LANES:]
        first = c == 0
        bgu[c, at] = jnp.where(first, b0.astype(F32), b1.astype(F32)).astype(BF)
        obgu[g] = jnp.where(first, b1.astype(F32), b0.astype(F32)).astype(BF)
        hf = hidden.astype(F32)
        hid[c, at] = jnp.where(first, hf[:, 0:LANES], hf[:, LANES:]).astype(BF)
        ohid[g] = jnp.where(first, hf[:, LANES:], hf[:, 0:LANES]).astype(BF)
        remote(obgu.at[g], bgu.at[c, at], bh_send.at[0], bh_recv.at[0], sib).start()
        remote(ohid.at[g], hid.at[c, at], bh_send.at[1], bh_recv.at[1], sib).start()

    def chunk(g, i):
        return jnp.concatenate([pown[g, i], mixt[g]], axis=0)

    def scatter_two(g):
        await_bytes(rb.at[g, pl.ds(0, 5), pl.ds(0, SENT)], rs_recv.at[g, 0])
        v = chunk(g, 0) + rb[g, 0].astype(F32)
        sb[g, 5, 0:CUT] = (v[0:CUT] + rb[g, 4, 0:CUT].astype(F32)).astype(BF)
        sb[g, 5, CUT:] = v[CUT:].astype(BF)
        send_part(g, 5, 1, 1, 2)
        v = chunk(g, 1) + rb[g, 2].astype(F32)
        sb[g, 6, 0:CUT] = v[0:CUT].astype(BF)
        sb[g, 6, CUT:] = (v[CUT:] + rb[g, 4, CUT:].astype(F32)).astype(BF)
        send_part(g, 6, 1, 1, -2)

    def give_back(g):
        await_bytes(rb.at[g, pl.ds(0, 2), pl.ds(0, SENT)], rs_recv.at[g, 1])
        v = chunk(g, 2)
        for i in (1, 3, 5, 6):
            v = v + rb[g, i].astype(F32)
        sums = v[2 * RPG:2 * RPG + 1] + v[2 * RPG + 1:2 * RPG + 2]
        mhi = sums.astype(BF).astype(F32)
        mlo = sums - mhi
        br, bc = iota((LANES, LANES), 0), iota((LANES, LANES), 1)
        second = bc >= RPG
        row = bc - jnp.where(second, RPG, 0)
        src_of = div5(row)
        slot_of = row - src_of * CAP
        here = ((br >> 3) == src_of + jnp.where(second, PER, 0)) & (bc < 2 * RPG)
        spread = (here & ((br & 7) == slot_of))[:, 0:2 * RPG].astype(BF)
        take = (((br >> 3) & (PER - 1)) == div5(bc)) & ((br & 7) == CAP) & (bc < RPG)
        slot_r = br - div5(br) * CAP
        m = dot(spread, v[0:2 * RPG].astype(BF))
        m = m + dot(jnp.where(take, mhi, 0.0).astype(BF), (bc == slot_r).astype(BF))
        m = m + dot(jnp.where(take, mlo, 0.0).astype(BF), (bc == slot_r + 8).astype(BF))
        out[g] = m.astype(BF).reshape(2, PER, 8, LANES)
        for j in range(PER):
            i = (g * ZB + j // HY) * NY + mine_y * HY + j % HY
            for hf in range(2):
                here_ = (i == e) & (c == hf)

                @pl.when(here_)
                def _():
                    ret[e] = out[g, hf, j]

                @pl.when(jnp.logical_not(here_))
                def _():
                    remote(out.at[g, hf, j], ret.at[e], rt_send, rt_recv, (i, x * 2 + hf)).start()

    def grads():
        await_bytes(rows.at[1 - c], sib_recv)
        await_bytes(bgu.at[1 - c], bh_recv.at[0])
        await_bytes(hid.at[1 - c], bh_recv.at[1])
        for q in range(QUADS):
            at = slice(q * QUAD, (q + 1) * QUAD)
            v = dot_tn(rows[0, q, 0], bgu[0]) + dot_tn(rows[1, q, 0], bgu[1])
            gg_ref[at, :] = v[:, 0:LANES].astype(BF)
            ug_ref[at, :] = v[:, LANES:].astype(BF)
            dg_ref[:, at] = (dot_tn(hid[0], rows[0, q, 1]) + dot_tn(hid[1], rows[1, q, 1])).astype(BF)

    def turn():
        mixt[...] = jnp.zeros_like(mixt)
        pr, pc = iota((2 * RPG, 16 * PER), 0), iota((2 * RPG, 16 * PER), 1)
        second = pr >= RPG
        rest = pr - jnp.where(second, RPG, 0)
        src = div5(rest)
        perm[...] = (pc == src * 16 + (rest - src * CAP) + jnp.where(second, CAP, 0)).astype(BF)
        for cp in weight_moves:
            cp.wait_recv()
        for k in range(8):
            at = slice(k * WIDE, (k + 1) * WIDE)
            dwt[at, :] = dw[:, at].T
            for hf in range(2):
                w4t[hf * WIDE:(hf + 1) * WIDE, at] = w4[at, hf * WIDE:(hf + 1) * WIDE].T

    def tables():
        er = iota((nep, tokn), 0)
        oh0, oh1 = er == r0, er == r1
        ranks = dot((oh0 | oh1).astype(BF), upper)
        aux[0:1, :] = jnp.sum(jnp.where(oh0, ranks, 0.0), axis=0, keepdims=True)
        aux[1:2, :] = jnp.sum(jnp.where(oh1, ranks, 0.0), axis=0, keepdims=True)
        blk8 = 128
        for b in range(nep * 8 // blk8):
            rw = iota((blk8, tokn), 0) + b * blk8
            hit = ((rw >> 3) == r0) | ((rw >> 3) == r1)
            rk = dot(hit.astype(BF), upper)
            s = rw & 7
            p8[pl.ds(b * blk8, blk8), :] = (hit & (rk == s.astype(F32)) & (s < CAP)).astype(BF)
        aux[2:3, :] = w0
        aux[3:4, :] = w1
        aux[4:5, :] = r0.astype(F32)
        aux[5:6, :] = r1.astype(F32)
        aux[6:8, :] = jnp.zeros((2, tokn), F32)

    steps = {"A": gather_out, "B": gather_in, "H": gather_far, "E": scatter_two, "F": give_back}
    def run(plan):
        left = {}
        for step in " ".join(plan).split():
            kind, g = step[0], int(step[1:] or 0)
            with jax.named_scope(step):
                if kind == "r":
                    relay(g)
                elif kind == "f":
                    relay(g, 1)
                elif kind in "st":
                    pl.when((z < NZ // 4) == (kind == "s"))(functools.partial(relay, g))
                elif kind in "az":
                    pl.when(c == int(kind == "z"))(functools.partial(gather_out, g))
                elif kind == "D":
                    pl.when(column & active)(tell_latecomer)
                elif kind in "xy":
                    pl.when(c == int(kind == "y"))(functools.partial(give_back, g))
                elif kind == "P":
                    first_products(g, (0, 2))
                    left[g] = (-1, 1)
                elif kind == "Q":
                    first_products(g, (0, -1, 1))
                    left[g] = (2,)
                elif kind == "C":
                    compute(g, left[g])
                elif kind == "G":
                    grads()
                elif kind == "W":
                    turn()
                elif kind == "T":
                    tables()
                else:
                    steps[kind](g)

    early = z < NZ // 2
    pl.when(early)(functools.partial(run, EARLY))
    pl.when(jnp.logical_not(early))(functools.partial(run, LATE))

    for cp in weight_moves:
        cp.wait_send()

    @pl.when(active)
    def _():
        await_bytes(msg.at[:, :, pl.ds(0, NY - 1), :, pl.ds(0, MSG)], y_send)
        await_bytes(ret.at[pl.ds(0, nep - 1)], rt_send)

    @pl.when(jnp.logical_not(active))
    def _():
        await_bytes(ret, rt_send)

    await_bytes(zbuf.at[:, pl.ds(0, NZ - 1), :, :, pl.ds(0, MSG)], z_send)
    await_bytes(rows.at[0, pl.ds(0, 2)], ag_send)
    await_bytes(rows.at[0], sib_send)
    await_bytes(obgu, bh_send.at[0])
    await_bytes(ohid, bh_send.at[1])
    await_bytes(sb.at[:, :, pl.ds(0, SENT)], rs_send)

    with jax.named_scope("retwait"):
        @pl.when(active)
        def _():
            await_bytes(ret.at[pl.ds(0, nep - 1)], rt_recv)

        @pl.when(jnp.logical_not(active))
        def _():
            await_bytes(ret, rt_recv)


def finish(ret, p8, aux, gg, ug, dg, tg_ref, mg_ref, gg_out, ug_out, dg_out, tg, mg, sem):
    copies = [
        pltpu.make_async_copy(gg, gg_out.at[0], sem.at[0]),
        pltpu.make_async_copy(ug, ug_out.at[0], sem.at[1]),
        pltpu.make_async_copy(dg, dg_out.at[0], sem.at[2]),
    ]
    for cp in copies:
        cp.start()
    nep = ret.shape[0]
    tokn = p8.shape[1]
    back_rows = ret[...].reshape(nep * 8, LANES)
    tg[...] = dot_tn(p8[...], back_rows).astype(BF)
    copies.append(pltpu.make_async_copy(tg, tg_ref, sem.at[3]))
    copies[-1].start()
    sr, sc = iota((nep, nep * 8), 0), iota((nep, nep * 8), 1)
    mixes = dot((sc == sr * 8 + CAP).astype(BF), back_rows).astype(BF)
    lane = iota((LANES, tokn), 0).astype(F32)
    er = iota((nep, tokn), 0).astype(F32)
    done = []
    for k in range(2):
        seen = dot_tn(mixes, (er == aux[4 + k:5 + k, :]).astype(BF))
        rank = aux[k:k + 1, :]
        picked = jnp.where((lane == rank) | (lane == rank + 8.0), seen, 0.0)
        done.append(jnp.sum(picked, axis=0, keepdims=True) / aux[2 + k:3 + k, :])
    mg[...] = jnp.concatenate(done, axis=0).astype(BF)
    copies.append(pltpu.make_async_copy(mg, mg_ref, sem.at[4]))
    copies[-1].start()
    for cp in copies:
        cp.wait()


def solution(mesh):
    nep = NZ * NY

    def on_device(tokens, cotangent, mix_weights, routes, gate_proj, up_proj, down_proj):
        tokn, width = tokens.shape
        ff = gate_proj.shape[2]
        vm = pl.BlockSpec(memory_space=pltpu.VMEM)
        hbm = pl.BlockSpec(memory_space=pltpu.HBM)
        dma = pltpu.SemaphoreType.DMA
        parts = pl.pallas_call(
            kernel,
            out_shape=(
                jax.ShapeDtypeStruct((nep, 8, LANES), BF),
                jax.ShapeDtypeStruct((nep * 8, tokn), BF),
                jax.ShapeDtypeStruct((8, tokn), F32),
                jax.ShapeDtypeStruct((width, ff), BF),
                jax.ShapeDtypeStruct((width, ff), BF),
                jax.ShapeDtypeStruct((ff, width), BF),
            ),
            in_specs=[hbm] * 7,
            out_specs=[vm] * 6,
            scratch_shapes=[
                pltpu.VMEM((2, tokn), jnp.int32),
                pltpu.VMEM((2, tokn), BF),
                pltpu.VMEM((2, 2, tokn, QUAD), BF),
                pltpu.VMEM((2, NZ, NY, 4, 16, LANES), BF),
                pltpu.VMEM((2, NZ, HY, 4, 16, LANES), BF),
                pltpu.VMEM((2, NZ, HY, 4, 16, LANES), BF),
                pltpu.VMEM((2, QUADS, 2, GROUPS * RPG, QUAD), BF),
                pltpu.VMEM((width, 4 * LANES), BF),
                pltpu.VMEM((2 * ff, width), BF),
                pltpu.VMEM((4 * LANES, width), BF),
                pltpu.VMEM((width, 2 * ff), BF),
                pltpu.VMEM((2 * RPG, 16 * PER), BF),
                pltpu.VMEM((2, GROUPS * RPG, WIDE), BF),
                pltpu.VMEM((2, GROUPS * RPG, LANES), BF),
                pltpu.VMEM((GROUPS, RPG, WIDE), BF),
                pltpu.VMEM((GROUPS, RPG, LANES), BF),
                pltpu.VMEM((GROUPS, 8, LANES), F32),
                pltpu.VMEM((GROUPS, RPG, QUAD), F32),
                pltpu.VMEM((GROUPS, RPG, WIDE), F32),
                pltpu.VMEM((GROUPS, 3, 2 * RPG, LANES), F32),
                pltpu.VMEM((GROUPS, 7, TILE, LANES), BF),
                pltpu.VMEM((GROUPS, 7, TILE, LANES), BF),
                pltpu.VMEM((GROUPS, 2, PER, 8, LANES), BF),
                pltpu.SemaphoreType.REGULAR((NZ,)),
                pltpu.SemaphoreType.REGULAR,
                dma((2,)), dma, dma, dma((4,)), dma, dma((2, GROUPS)), dma, dma((2, GROUPS)),
                dma, dma((GROUPS,)), dma, dma,
                dma((2,)), dma((2,)), dma, dma((GROUPS, 2)), dma, dma,
            ],
            compiler_params=pltpu.CompilerParams(
                collective_id=0, has_side_effects=True, vmem_limit_bytes=52 * 1024 * 1024),
        )(*(
            pltpu.with_memory_space_constraint(a, pltpu.HBM)
            for a in (tokens, cotangent, routes.T, mix_weights.T, gate_proj, up_proj, down_proj)))
        tg, mg, gg, ug, dg = pl.pallas_call(
            finish,
            out_shape=(
                jax.ShapeDtypeStruct((tokn, LANES), BF),
                jax.ShapeDtypeStruct((2, tokn), BF),
                jax.ShapeDtypeStruct((1, width, ff), BF),
                jax.ShapeDtypeStruct((1, width, ff), BF),
                jax.ShapeDtypeStruct((1, ff, width), BF),
            ),
            in_specs=[vm] * 6,
            out_specs=[hbm] * 5,
            scratch_shapes=[pltpu.VMEM((tokn, LANES), BF), pltpu.VMEM((2, tokn), BF), dma((5,))],
            compiler_params=pltpu.CompilerParams(vmem_limit_bytes=8 * 1024 * 1024),
        )(*parts)
        return tg, mg.T, gg, ug, dg

    in_specs = (
        P("ep", None), P("ep", None), P("ep", None), P("ep", None),
        P("ep", None, "tp"), P("ep", None, "tp"), P("ep", "tp", None),
    )
    out_specs = (
        P("ep", "tp"), P("ep", None), P("ep", None, "tp"), P("ep", None, "tp"), P("ep", "tp", None),
    )
    return jax.shard_map(on_device, mesh=mesh, in_specs=in_specs, out_specs=out_specs, check_vma=False)
```

```python
import functools

import jax
import jax.numpy as jnp
from jax import lax
from jax.experimental import pallas as pl
from jax.experimental.pallas import tpu as pltpu
from jax.sharding import PartitionSpec as P

MESH = pl.DeviceIdType.MESH
BF = jnp.bfloat16
F32 = jnp.float32
CAP = 5
MSG = 2 * CAP
LANES = 128
NX = NY = NZ = 8
GROUPS = 4
ZB = NZ // GROUPS
HY = NY // 2
PER = ZB * HY
RPG = PER * CAP
TILE = 2 * RPG + 8
SENT = 2 * RPG + 2
CUT = 40
WIDE = 2 * LANES
QUADS = 4
QUAD = 4 * LANES
EARLY = (
    "W r0 r1 r2", "s3 A0 A1 t3", "f0 f1 B0 f2", "f3 H0 Q0 C0", "A2 E0 A3 B1",
    "Q1 H1 C1 H2", "B2 Q2 C2 F0", "H3 P3 B3 C3", "E1 E3 E2 T", "G F1 F3 F2",
)
LATE = (
    "W r0 A0 r1", "f0 f1 A1 r2", "r3 B0 Q0 H0", "C0 A2 H1 f2", "E0 f3 B1 P1",
    "C1 H3 B2 H2", "A3 P2 C2 F0", "E1 P3 E2 B3", "F1 C3 F2 E3", "F3 T G",
)


def iota(shape, dim):
    return lax.broadcasted_iota(jnp.int32, shape, dim)


def dot(a, b):
    return jnp.dot(a, b, preferred_element_type=F32)


def dot_nt(a, b):
    return lax.dot_general(a, b, (((1,), (1,)), ((), ())), preferred_element_type=F32)


def dot_tn(a, b):
    return lax.dot_general(a, b, (((0,), (0,)), ((), ())), preferred_element_type=F32)


def div5(v):
    return (v * 205) >> 10


def kernel(
    tok_hbm, cot_hbm, routes_hbm, mix_hbm, gate_hbm, up_hbm, down_hbm,
    ret, p8, aux, gg_ref, ug_ref, dg_ref,
    routes_ref, mix_ref, share, msg, ybuf, zbuf, rows, w4, dw, w4t, dwt, perm, bgu, hid, obgu, ohid, mixt,
    pre, back, pown, sb, rb, out,
    ready, t_sem, sh_sem, w_sem, x_sem, y_send, y_recv, z_send, z_recv, ag_send, ag_recv, sib_send, sib_recv,
    bh_send, bh_recv, rs_send, rs_recv, rt_send, rt_recv,
):
    e = lax.axis_index("ep")
    t = lax.axis_index("tp")
    z, y = e // NY, e % NY
    x, c = t // 2, t % 2
    tokn = share.shape[2]
    nep = NZ * NY
    mine_y = 1 - c
    active = y // HY == mine_y

    def chip(d):
        return lax.rem(x + d + NX, NX)

    def quad(d):
        return lax.rem(x + d + NX, QUADS)

    sib = (e, x * 2 + (1 - c))

    def along_x(d):
        return (e, chip(d) * 2 + c)

    def remote(src, dst, ssem, rsem, to):
        return pltpu.make_async_remote_copy(
            src_ref=src, dst_ref=dst, send_sem=ssem, recv_sem=rsem, device_id=to, device_id_type=MESH)

    def await_bytes(ref, sem):
        pltpu.make_async_copy(ref, ref, sem).wait()

    cols = [pl.ds(pl.multiple_of(quad(d) * QUAD, QUAD), QUAD) for d in (0, 2)]
    table_copies = [
        pltpu.make_async_copy(routes_hbm, routes_ref, t_sem.at[0]),
        pltpu.make_async_copy(mix_hbm, mix_ref, t_sem.at[1]),
    ]
    share_copies = [
        pltpu.make_async_copy(ref.at[:, cols[part]], share.at[part, i], sh_sem)
        for part in range(2) for i, ref in enumerate((tok_hbm, cot_hbm))
    ]
    lane = pl.multiple_of(c * WIDE, WIDE)
    ours = w4.at[:, pl.ds(lane, WIDE)]
    downs = dw.at[pl.ds(pl.multiple_of(c * LANES, LANES), LANES)]
    weight_copies = [
        pltpu.make_async_copy(gate_hbm.at[0], w4.at[:, pl.ds(lane, LANES)], w_sem),
        pltpu.make_async_copy(up_hbm.at[0], w4.at[:, pl.ds(pl.multiple_of(lane + LANES, LANES), LANES)], w_sem),
        pltpu.make_async_copy(down_hbm.at[0], downs, w_sem),
    ]
    weight_moves = [
        remote(ours, ours, x_sem.at[0], x_sem.at[1], sib),
        remote(downs, downs, x_sem.at[2], x_sem.at[3], sib),
    ]
    barrier = pltpu.get_barrier_semaphore()
    for d in (4, 3, 5, 2, 6, 1, 7):
        pl.semaphore_signal(barrier, inc=1, device_id=(z * NY + lax.rem(y + d, NY), t), device_id_type=MESH)
    for d in (2, -2, 1, -1):
        pl.semaphore_signal(barrier, inc=1, device_id=along_x(d), device_id_type=MESH)
    pl.semaphore_signal(barrier, inc=1, device_id=sib, device_id_type=MESH)
    for cp in table_copies + share_copies + weight_copies:
        cp.start()
    with jax.named_scope("barrier"):
        pl.semaphore_wait(barrier, 12 + jnp.where(z > 0, 1, 0))

    @pl.when(z < NZ - 1)
    def _():
        pl.semaphore_signal(barrier, inc=1, device_id=(e + NY, t), device_id_type=MESH)

    for zz in range(NZ - 1):
        @pl.when(zz < z)
        def _():
            pl.semaphore_signal(ready.at[z], inc=1, device_id=(zz * NY + y, t), device_id_type=MESH)

    for cp in table_copies:
        cp.wait()
    r0, r1 = routes_ref[0:1, :], routes_ref[1:2, :]
    w = mix_ref[...].astype(F32)
    w0, w1 = w[0:1, :], w[1:2, :]
    upper = (iota((tokn, tokn), 0) < iota((tokn, tokn), 1)).astype(BF)
    with jax.named_scope("share"):
        await_bytes(share, sh_sem)

    @pl.when(active)
    def _():
        both = jnp.concatenate([share[part].reshape(2 * tokn, QUAD) for part in range(2)], axis=1)
        blk = ZB * NY * 16

        def fill(b):
            rw = iota((blk, tokn), 0) + b * blk
            ex = rw >> 4
            q = rw & 15
            h0, h1 = ex == r0, ex == r1
            hit = h0 | h1
            rk = dot(hit.astype(BF), upper)
            wt = jnp.where(h0, w0, 0.0) + jnp.where(h1, w1, 0.0)
            one = jnp.where(hit & (rk == q.astype(F32)) & (q < CAP), 1.0, 0.0)
            two = jnp.where(hit & (rk == (q - CAP).astype(F32)) & (q >= CAP), wt, 0.0)
            sel = jnp.concatenate([one.astype(BF), two.astype(BF)], axis=1)
            v = dot(sel, both).astype(BF)
            for part in range(2):
                for ch in range(4):
                    at = part * QUAD + ch * LANES
                    msg[part, pl.ds(b * ZB, ZB), :, ch] = v[:, at:at + LANES].reshape(ZB, NY, 16, LANES)

        def tell(b, part):
            zz = pl.ds(b * ZB, ZB)
            for d in (4, 3, 5, 2, 6, 1, 7):
                yd = lax.rem(y + d, NY)
                remote(
                    msg.at[part, zz, yd, :, pl.ds(0, MSG)], ybuf.at[part, zz, y % HY, :, pl.ds(0, MSG)],
                    y_send, y_recv.at[part, b], (z * NY + yd, t)).start()
            ybuf[part, zz, y % HY] = msg[part, zz, y]

        for b in (0, 1):
            fill(b)
            tell(b, 0)

        @pl.when(z >= NZ // 2)
        def _():
            for b in (0, 1):
                tell(b, 1)

        for b in (2, 3):
            fill(b)
            tell(b, 0)

        @pl.when(z < NZ // 2)
        def _():
            for b in (0, 1):
                tell(b, 1)

        for b in (2, 3):
            tell(b, 1)

    await_bytes(w4.at[:, pl.ds(0, 3 * LANES)], w_sem)
    for cp in weight_moves:
        cp.start()

    def relay(b, part=0):
        with jax.named_scope(f"ywait{b}{'f' if part else ''}"):
            zz = pl.ds(b * ZB, ZB)

            @pl.when(active)
            def _():
                await_bytes(ybuf.at[part, zz, pl.ds(0, HY - 1), :, pl.ds(0, MSG)], y_recv.at[part, b])

            @pl.when(jnp.logical_not(active))
            def _():
                await_bytes(ybuf.at[part, zz, :, :, pl.ds(0, MSG)], y_recv.at[part, b])
        for zd in range(b * ZB, (b + 1) * ZB):
            @pl.when(zd == z)
            def _():
                zbuf[part, zd] = ybuf[part, zd]

            if part == 0:
                @pl.when(zd > z)
                def _():
                    with jax.named_scope(f"ready{zd}"):
                        pl.semaphore_wait(ready.at[zd], 1)

            @pl.when(zd != z)
            def _():
                remote(
                    ybuf.at[part, zd, :, :, pl.ds(0, MSG)], zbuf.at[part, z, :, :, pl.ds(0, MSG)],
                    z_send, z_recv.at[part, z // ZB], (zd * NY + y, t)).start()

    def unit(d, g):
        return rows.at[c, quad(d), :, pl.ds(g * RPG, RPG)]

    def to_sib(d, g):
        u = unit(d, g)
        remote(u, u, sib_send, sib_recv, sib).start()

    def landed(g, part):
        with jax.named_scope(f"zwait{g}{'f' if part else ''}"):
            @pl.when(z // ZB == g)
            def _():
                await_bytes(zbuf.at[part, pl.ds(0, ZB - 1), :, :, pl.ds(0, MSG)], z_recv.at[part, g])

            @pl.when(z // ZB != g)
            def _():
                await_bytes(zbuf.at[part, pl.ds(0, ZB), :, :, pl.ds(0, MSG)], z_recv.at[part, g])
        got = jnp.concatenate(
            [zbuf[part, pl.ds(g * ZB, ZB), :, ch].reshape(PER * 16, LANES) for ch in range(4)], axis=1)
        got = jnp.where((iota(got.shape, 0) & 15) < MSG, got, jnp.zeros_like(got))
        v = dot(perm[...], got)
        q = quad(2 * part)
        rows[c, q, 0, g * RPG:(g + 1) * RPG] = v[0:RPG].astype(BF)
        rows[c, q, 1, g * RPG:(g + 1) * RPG] = v[RPG:].astype(BF)

    def gather_out(g):
        landed(g, 0)
        u = unit(0, g)
        remote(u, u, ag_send, ag_recv.at[g], along_x(1)).start()
        remote(u, u, ag_send, ag_recv.at[g], along_x(-1)).start()
        to_sib(0, g)

    def gather_far(g):
        landed(g, 1)
        to_sib(2, g)

    def gather_in(g):
        await_bytes(rows.at[c, pl.ds(0, 2), :, pl.ds(g * RPG, RPG)], ag_recv.at[g])
        to_sib(-1, g)
        to_sib(1, g)

    def send_part(g, first, count, phase, to):
        at = (g, pl.ds(first, count), pl.ds(0, SENT))
        remote(sb.at[at], rb.at[at], rs_send, rs_recv.at[g, phase], along_x(to)).start()

    near, past = pl.ds(0, CUT), pl.ds(CUT, SENT - CUT)

    def products(g, d):
        at = pl.ds(g * RPG, RPG)
        q = quad(d)
        features = pl.ds(pl.multiple_of(q * QUAD, QUAD), QUAD)
        return dot(rows[c, q, 0, at], w4[features, :]), dot(rows[c, q, 1, at], dwt[features, :])

    def first_products(g, ds):
        each = [products(g, d) for d in ds]
        pre[g] = sum((a for a, _ in each[1:]), each[0][0])
        back[g] = sum((b for _, b in each[1:]), each[0][1])

    def compute(g, ds):
        at = pl.ds(g * RPG, RPG)
        pgu, bh = pre[g], back[g]
        for d in ds:
            a, b = products(g, d)
            pgu = pgu + a
            bh = bh + b
        pg = jnp.concatenate([pgu[:, 0:LANES], pgu[:, WIDE:WIDE + LANES]], axis=1)
        pu = jnp.concatenate([pgu[:, LANES:WIDE], pgu[:, WIDE + LANES:]], axis=1)
        sig = jax.nn.sigmoid(pg)
        act = pg * sig
        hidden = (act * pu).astype(BF)
        bg = (bh * pu * (sig * (1.0 + pg * (1.0 - sig)))).astype(BF)
        bu = (bh * act).astype(BF)
        b0 = jnp.concatenate([bg[:, 0:LANES], bu[:, 0:LANES]], axis=1)
        b1 = jnp.concatenate([bg[:, LANES:], bu[:, LANES:]], axis=1)
        b4 = jnp.concatenate([b0, b1], axis=1)
        hb = hidden.astype(F32) * bh
        hi = hb.astype(BF)
        lo = (hb - hi.astype(F32)).astype(BF)
        ones = jnp.ones((8, WIDE), BF)
        sums = dot_nt(ones, hi) + dot_nt(ones, lo)
        shi = sums.astype(BF).astype(F32)
        row = iota((8, RPG), 0)
        mixt[g, :, 0:RPG] = jnp.where(row == 0, shi, jnp.where(row == 1, sums - shi, 0.0))
        tile = mixt[g].astype(BF)
        def part(d):
            cols = pl.ds(pl.multiple_of(chip(d) * WIDE, WIDE), WIDE)
            return dot(b4, w4t[:, cols])

        def stored(d, i):
            v = part(d)
            sb[g, i, 0:RPG] = v[:, 0:LANES].astype(BF)
            sb[g, i, RPG:2 * RPG] = v[:, LANES:].astype(BF)
            sb[g, i, 2 * RPG:] = tile

        stored(4, 4)
        for rows_, to in ((near, 2), (past, -2)):
            remote(sb.at[g, 4, rows_], rb.at[g, 4, rows_], rs_send, rs_recv.at[g, 0], along_x(to)).start()
        for d, i, to in ((3, 0, 1), (5, 2, -1)):
            stored(d, i)
            stored(to % NX, i + 1)
            send_part(g, i, 2, 0, to)
        for d, i in ((2, 0), (6, 1), (0, 2)):
            v = part(d)
            pown[g, i, 0:RPG] = v[:, 0:LANES]
            pown[g, i, RPG:2 * RPG] = v[:, LANES:]
        first = c == 0
        bgu[c, at] = jnp.where(first, b0.astype(F32), b1.astype(F32)).astype(BF)
        obgu[g] = jnp.where(first, b1.astype(F32), b0.astype(F32)).astype(BF)
        hf = hidden.astype(F32)
        hid[c, at] = jnp.where(first, hf[:, 0:LANES], hf[:, LANES:]).astype(BF)
        ohid[g] = jnp.where(first, hf[:, LANES:], hf[:, 0:LANES]).astype(BF)
        remote(obgu.at[g], bgu.at[c, at], bh_send.at[0], bh_recv.at[0], sib).start()
        remote(ohid.at[g], hid.at[c, at], bh_send.at[1], bh_recv.at[1], sib).start()

    def chunk(g, i):
        return jnp.concatenate([pown[g, i], mixt[g]], axis=0)

    def scatter_two(g):
        await_bytes(rb.at[g, pl.ds(0, 5), pl.ds(0, SENT)], rs_recv.at[g, 0])
        v = chunk(g, 0) + rb[g, 0].astype(F32)
        sb[g, 5, 0:CUT] = (v[0:CUT] + rb[g, 4, 0:CUT].astype(F32)).astype(BF)
        sb[g, 5, CUT:] = v[CUT:].astype(BF)
        send_part(g, 5, 1, 1, 2)
        v = chunk(g, 1) + rb[g, 2].astype(F32)
        sb[g, 6, 0:CUT] = v[0:CUT].astype(BF)
        sb[g, 6, CUT:] = (v[CUT:] + rb[g, 4, CUT:].astype(F32)).astype(BF)
        send_part(g, 6, 1, 1, -2)

    def give_back(g):
        await_bytes(rb.at[g, pl.ds(0, 2), pl.ds(0, SENT)], rs_recv.at[g, 1])
        v = chunk(g, 2)
        for i in (1, 3, 5, 6):
            v = v + rb[g, i].astype(F32)
        sums = v[2 * RPG:2 * RPG + 1] + v[2 * RPG + 1:2 * RPG + 2]
        mhi = sums.astype(BF).astype(F32)
        mlo = sums - mhi
        br, bc = iota((LANES, LANES), 0), iota((LANES, LANES), 1)
        second = bc >= RPG
        row = bc - jnp.where(second, RPG, 0)
        src_of = div5(row)
        slot_of = row - src_of * CAP
        here = ((br >> 3) == src_of + jnp.where(second, PER, 0)) & (bc < 2 * RPG)
        spread = (here & ((br & 7) == slot_of))[:, 0:2 * RPG].astype(BF)
        take = (((br >> 3) & (PER - 1)) == div5(bc)) & ((br & 7) == CAP) & (bc < RPG)
        slot_r = br - div5(br) * CAP
        m = dot(spread, v[0:2 * RPG].astype(BF))
        m = m + dot(jnp.where(take, mhi, 0.0).astype(BF), (bc == slot_r).astype(BF))
        m = m + dot(jnp.where(take, mlo, 0.0).astype(BF), (bc == slot_r + 8).astype(BF))
        out[g] = m.astype(BF).reshape(2, PER, 8, LANES)
        for j in range(PER):
            i = (g * ZB + j // HY) * NY + mine_y * HY + j % HY
            for hf in range(2):
                here_ = (i == e) & (c == hf)

                @pl.when(here_)
                def _():
                    ret[e] = out[g, hf, j]

                @pl.when(jnp.logical_not(here_))
                def _():
                    remote(out.at[g, hf, j], ret.at[e], rt_send, rt_recv, (i, x * 2 + hf)).start()

    def grads():
        await_bytes(rows.at[1 - c], sib_recv)
        await_bytes(bgu.at[1 - c], bh_recv.at[0])
        await_bytes(hid.at[1 - c], bh_recv.at[1])
        for q in range(QUADS):
            at = slice(q * QUAD, (q + 1) * QUAD)
            v = dot_tn(rows[0, q, 0], bgu[0]) + dot_tn(rows[1, q, 0], bgu[1])
            gg_ref[at, :] = v[:, 0:LANES].astype(BF)
            ug_ref[at, :] = v[:, LANES:].astype(BF)
            dg_ref[:, at] = (dot_tn(hid[0], rows[0, q, 1]) + dot_tn(hid[1], rows[1, q, 1])).astype(BF)

    def turn():
        mixt[...] = jnp.zeros_like(mixt)
        pr, pc = iota((2 * RPG, 16 * PER), 0), iota((2 * RPG, 16 * PER), 1)
        second = pr >= RPG
        rest = pr - jnp.where(second, RPG, 0)
        src = div5(rest)
        perm[...] = (pc == src * 16 + (rest - src * CAP) + jnp.where(second, CAP, 0)).astype(BF)
        for cp in weight_moves:
            cp.wait_recv()
        for k in range(8):
            at = slice(k * WIDE, (k + 1) * WIDE)
            dwt[at, :] = dw[:, at].T
            for hf in range(2):
                w4t[hf * WIDE:(hf + 1) * WIDE, at] = w4[at, hf * WIDE:(hf + 1) * WIDE].T

    def tables():
        er = iota((nep, tokn), 0)
        oh0, oh1 = er == r0, er == r1
        ranks = dot((oh0 | oh1).astype(BF), upper)
        aux[0:1, :] = jnp.sum(jnp.where(oh0, ranks, 0.0), axis=0, keepdims=True)
        aux[1:2, :] = jnp.sum(jnp.where(oh1, ranks, 0.0), axis=0, keepdims=True)
        blk8 = 128
        for b in range(nep * 8 // blk8):
            rw = iota((blk8, tokn), 0) + b * blk8
            hit = ((rw >> 3) == r0) | ((rw >> 3) == r1)
            rk = dot(hit.astype(BF), upper)
            s = rw & 7
            p8[pl.ds(b * blk8, blk8), :] = (hit & (rk == s.astype(F32)) & (s < CAP)).astype(BF)
        aux[2:3, :] = w0
        aux[3:4, :] = w1
        aux[4:5, :] = r0.astype(F32)
        aux[5:6, :] = r1.astype(F32)
        aux[6:8, :] = jnp.zeros((2, tokn), F32)

    steps = {"A": gather_out, "B": gather_in, "H": gather_far, "E": scatter_two, "F": give_back}
    def run(plan):
        left = {}
        for step in " ".join(plan).split():
            kind, g = step[0], int(step[1:] or 0)
            with jax.named_scope(step):
                if kind == "r":
                    relay(g)
                elif kind == "f":
                    relay(g, 1)
                elif kind in "st":
                    pl.when((z < NZ // 4) == (kind == "s"))(functools.partial(relay, g))
                elif kind == "P":
                    first_products(g, (0, 2))
                    left[g] = (-1, 1)
                elif kind == "Q":
                    first_products(g, (0, -1, 1))
                    left[g] = (2,)
                elif kind == "C":
                    compute(g, left[g])
                elif kind == "G":
                    grads()
                elif kind == "W":
                    turn()
                elif kind == "T":
                    tables()
                else:
                    steps[kind](g)

    early = z < NZ // 2
    pl.when(early)(functools.partial(run, EARLY))
    pl.when(jnp.logical_not(early))(functools.partial(run, LATE))

    for cp in weight_moves:
        cp.wait_send()

    @pl.when(active)
    def _():
        await_bytes(msg.at[:, :, pl.ds(0, NY - 1), :, pl.ds(0, MSG)], y_send)
        await_bytes(ret.at[pl.ds(0, nep - 1)], rt_send)

    @pl.when(jnp.logical_not(active))
    def _():
        await_bytes(ret, rt_send)

    await_bytes(zbuf.at[:, pl.ds(0, NZ - 1), :, :, pl.ds(0, MSG)], z_send)
    await_bytes(rows.at[0, pl.ds(0, 2)], ag_send)
    await_bytes(rows.at[0], sib_send)
    await_bytes(obgu, bh_send.at[0])
    await_bytes(ohid, bh_send.at[1])
    await_bytes(sb.at[:, :, pl.ds(0, SENT)], rs_send)

    with jax.named_scope("retwait"):
        @pl.when(active)
        def _():
            await_bytes(ret.at[pl.ds(0, nep - 1)], rt_recv)

        @pl.when(jnp.logical_not(active))
        def _():
            await_bytes(ret, rt_recv)


def finish(ret, p8, aux, gg, ug, dg, tg_ref, mg_ref, gg_out, ug_out, dg_out, tg, mg, sem):
    copies = [
        pltpu.make_async_copy(gg, gg_out.at[0], sem.at[0]),
        pltpu.make_async_copy(ug, ug_out.at[0], sem.at[1]),
        pltpu.make_async_copy(dg, dg_out.at[0], sem.at[2]),
    ]
    for cp in copies:
        cp.start()
    nep = ret.shape[0]
    tokn = p8.shape[1]
    back_rows = ret[...].reshape(nep * 8, LANES)
    tg[...] = dot_tn(p8[...], back_rows).astype(BF)
    copies.append(pltpu.make_async_copy(tg, tg_ref, sem.at[3]))
    copies[-1].start()
    sr, sc = iota((nep, nep * 8), 0), iota((nep, nep * 8), 1)
    mixes = dot((sc == sr * 8 + CAP).astype(BF), back_rows).astype(BF)
    lane = iota((LANES, tokn), 0).astype(F32)
    er = iota((nep, tokn), 0).astype(F32)
    done = []
    for k in range(2):
        seen = dot_tn(mixes, (er == aux[4 + k:5 + k, :]).astype(BF))
        rank = aux[k:k + 1, :]
        picked = jnp.where((lane == rank) | (lane == rank + 8.0), seen, 0.0)
        done.append(jnp.sum(picked, axis=0, keepdims=True) / aux[2 + k:3 + k, :])
    mg[...] = jnp.concatenate(done, axis=0).astype(BF)
    copies.append(pltpu.make_async_copy(mg, mg_ref, sem.at[4]))
    copies[-1].start()
    for cp in copies:
        cp.wait()


def solution(mesh):
    nep = NZ * NY

    def on_device(tokens, cotangent, mix_weights, routes, gate_proj, up_proj, down_proj):
        tokn, width = tokens.shape
        ff = gate_proj.shape[2]
        vm = pl.BlockSpec(memory_space=pltpu.VMEM)
        hbm = pl.BlockSpec(memory_space=pltpu.HBM)
        dma = pltpu.SemaphoreType.DMA
        parts = pl.pallas_call(
            kernel,
            out_shape=(
                jax.ShapeDtypeStruct((nep, 8, LANES), BF),
                jax.ShapeDtypeStruct((nep * 8, tokn), BF),
                jax.ShapeDtypeStruct((8, tokn), F32),
                jax.ShapeDtypeStruct((width, ff), BF),
                jax.ShapeDtypeStruct((width, ff), BF),
                jax.ShapeDtypeStruct((ff, width), BF),
            ),
            in_specs=[hbm] * 7,
            out_specs=[vm] * 6,
            scratch_shapes=[
                pltpu.VMEM((2, tokn), jnp.int32),
                pltpu.VMEM((2, tokn), BF),
                pltpu.VMEM((2, 2, tokn, QUAD), BF),
                pltpu.VMEM((2, NZ, NY, 4, 16, LANES), BF),
                pltpu.VMEM((2, NZ, HY, 4, 16, LANES), BF),
                pltpu.VMEM((2, NZ, HY, 4, 16, LANES), BF),
                pltpu.VMEM((2, QUADS, 2, GROUPS * RPG, QUAD), BF),
                pltpu.VMEM((width, 4 * LANES), BF),
                pltpu.VMEM((2 * ff, width), BF),
                pltpu.VMEM((4 * LANES, width), BF),
                pltpu.VMEM((width, 2 * ff), BF),
                pltpu.VMEM((2 * RPG, 16 * PER), BF),
                pltpu.VMEM((2, GROUPS * RPG, WIDE), BF),
                pltpu.VMEM((2, GROUPS * RPG, LANES), BF),
                pltpu.VMEM((GROUPS, RPG, WIDE), BF),
                pltpu.VMEM((GROUPS, RPG, LANES), BF),
                pltpu.VMEM((GROUPS, 8, LANES), F32),
                pltpu.VMEM((GROUPS, RPG, QUAD), F32),
                pltpu.VMEM((GROUPS, RPG, WIDE), F32),
                pltpu.VMEM((GROUPS, 3, 2 * RPG, LANES), F32),
                pltpu.VMEM((GROUPS, 7, TILE, LANES), BF),
                pltpu.VMEM((GROUPS, 7, TILE, LANES), BF),
                pltpu.VMEM((GROUPS, 2, PER, 8, LANES), BF),
                pltpu.SemaphoreType.REGULAR((NZ,)),
                dma((2,)), dma, dma, dma((4,)), dma, dma((2, GROUPS)), dma, dma((2, GROUPS)),
                dma, dma((GROUPS,)), dma, dma,
                dma((2,)), dma((2,)), dma, dma((GROUPS, 2)), dma, dma,
            ],
            compiler_params=pltpu.CompilerParams(
                collective_id=0, has_side_effects=True, vmem_limit_bytes=52 * 1024 * 1024),
        )(*(
            pltpu.with_memory_space_constraint(a, pltpu.HBM)
            for a in (tokens, cotangent, routes.T, mix_weights.T, gate_proj, up_proj, down_proj)))
        tg, mg, gg, ug, dg = pl.pallas_call(
            finish,
            out_shape=(
                jax.ShapeDtypeStruct((tokn, LANES), BF),
                jax.ShapeDtypeStruct((2, tokn), BF),
                jax.ShapeDtypeStruct((1, width, ff), BF),
                jax.ShapeDtypeStruct((1, width, ff), BF),
                jax.ShapeDtypeStruct((1, ff, width), BF),
            ),
            in_specs=[vm] * 6,
            out_specs=[hbm] * 5,
            scratch_shapes=[pltpu.VMEM((tokn, LANES), BF), pltpu.VMEM((2, tokn), BF), dma((5,))],
            compiler_params=pltpu.CompilerParams(vmem_limit_bytes=8 * 1024 * 1024),
        )(*parts)
        return tg, mg.T, gg, ug, dg

    in_specs = (
        P("ep", None), P("ep", None), P("ep", None), P("ep", None),
        P("ep", None, "tp"), P("ep", None, "tp"), P("ep", "tp", None),
    )
    out_specs = (
        P("ep", "tp"), P("ep", None), P("ep", None, "tp"), P("ep", None, "tp"), P("ep", "tp", None),
    )
    return jax.shard_map(on_device, mesh=mesh, in_specs=in_specs, out_specs=out_specs, check_vma=False)
```

```python
import functools

import jax
import jax.numpy as jnp
from jax import lax
from jax.experimental import pallas as pl
from jax.experimental.pallas import tpu as pltpu
from jax.sharding import PartitionSpec as P

MESH = pl.DeviceIdType.MESH
BF = jnp.bfloat16
F32 = jnp.float32
CAP = 5
MSG = 2 * CAP
LANES = 128
NX = NY = NZ = 8
GROUPS = 4
ZB = NZ // GROUPS
HY = NY // 2
PER = ZB * HY
RPG = PER * CAP
TILE = 2 * RPG + 8
SENT = 2 * RPG + 2
CUT = 40
WIDE = 2 * LANES
QUADS = 4
QUAD = 4 * LANES
EARLY = (
    "W r0 r1 D", "r2 s3 A0 A1", "t3 f0 f1 B0", "f2 f3 H0 Q0", "C0 A2 B1 H1",
    "P1 C1 A3 E0", "H2 B2 P2 C2", "H3 P3 B3 C3", "F0 E1 E2 E3", "T G F1 F2",
    "F3",
)
LATE = (
    "W r0 A0 r1", "f0 f1 a1 r2", "r3 B0 z1 Q0", "H0 C0 B1 H1", "P1 C1 A2 f2",
    "f3 E0 A3 E1", "F0 H2 B2 P2", "C2 H3 P3 F1", "B3 C3 E2 E3", "F2 F3 T G",
)


def iota(shape, dim):
    return lax.broadcasted_iota(jnp.int32, shape, dim)


def dot(a, b):
    return jnp.dot(a, b, preferred_element_type=F32)


def dot_nt(a, b):
    return lax.dot_general(a, b, (((1,), (1,)), ((), ())), preferred_element_type=F32)


def dot_tn(a, b):
    return lax.dot_general(a, b, (((0,), (0,)), ((), ())), preferred_element_type=F32)


def div5(v):
    return (v * 205) >> 10


def kernel(
    tok_hbm, cot_hbm, routes_hbm, mix_hbm, gate_hbm, up_hbm, down_hbm,
    ret, p8, aux, gg_ref, ug_ref, dg_ref,
    routes_ref, mix_ref, share, msg, ybuf, zbuf, rows, w4, dw, w4t, dwt, perm, bgu, hid, obgu, ohid, mixt,
    pre, back, pown, sb, rb, out,
    ready, late, t_sem, sh_sem, w_sem, x_sem, y_send, y_recv, z_send, z_recv, ag_send, ag_recv, sib_send, sib_recv,
    bh_send, bh_recv, rs_send, rs_recv, rt_send, rt_recv,
):
    e = lax.axis_index("ep")
    t = lax.axis_index("tp")
    z, y = e // NY, e % NY
    x, c = t // 2, t % 2
    tokn = share.shape[2]
    nep = NZ * NY
    mine_y = 1 - c
    active = y // HY == mine_y

    def chip(d):
        return lax.rem(x + d + NX, NX)

    def quad(d):
        return lax.rem(x + d + NX, QUADS)

    sib = (e, x * 2 + (1 - c))

    def along_x(d):
        return (e, chip(d) * 2 + c)

    def remote(src, dst, ssem, rsem, to):
        return pltpu.make_async_remote_copy(
            src_ref=src, dst_ref=dst, send_sem=ssem, recv_sem=rsem, device_id=to, device_id_type=MESH)

    def await_bytes(ref, sem):
        pltpu.make_async_copy(ref, ref, sem).wait()

    cols = [pl.ds(pl.multiple_of(quad(d) * QUAD, QUAD), QUAD) for d in (0, 2)]
    table_copies = [
        pltpu.make_async_copy(routes_hbm, routes_ref, t_sem.at[0]),
        pltpu.make_async_copy(mix_hbm, mix_ref, t_sem.at[1]),
    ]
    share_copies = [
        pltpu.make_async_copy(ref.at[:, cols[part]], share.at[part, i], sh_sem)
        for part in range(2) for i, ref in enumerate((tok_hbm, cot_hbm))
    ]
    lane = pl.multiple_of(c * WIDE, WIDE)
    ours = w4.at[:, pl.ds(lane, WIDE)]
    downs = dw.at[pl.ds(pl.multiple_of(c * LANES, LANES), LANES)]
    weight_copies = [
        pltpu.make_async_copy(gate_hbm.at[0], w4.at[:, pl.ds(lane, LANES)], w_sem),
        pltpu.make_async_copy(up_hbm.at[0], w4.at[:, pl.ds(pl.multiple_of(lane + LANES, LANES), LANES)], w_sem),
        pltpu.make_async_copy(down_hbm.at[0], downs, w_sem),
    ]
    weight_moves = [
        remote(ours, ours, x_sem.at[0], x_sem.at[1], sib),
        remote(downs, downs, x_sem.at[2], x_sem.at[3], sib),
    ]
    barrier = pltpu.get_barrier_semaphore()
    column = (z == 0) & (t == 0)
    latecomer = column & (y == 0)

    @pl.when(jnp.logical_not(latecomer))
    def _():
        for d in (4, 3, 5, 2, 6, 1, 7):
            pl.semaphore_signal(barrier, inc=1, device_id=(z * NY + lax.rem(y + d, NY), t), device_id_type=MESH)

    for d in (2, -2, 1, -1):
        pl.semaphore_signal(barrier, inc=1, device_id=along_x(d), device_id_type=MESH)
    pl.semaphore_signal(barrier, inc=1, device_id=sib, device_id_type=MESH)
    for cp in table_copies + share_copies + weight_copies:
        cp.start()
    with jax.named_scope("barrier"):
        pl.semaphore_wait(barrier, 12 + jnp.where(z > 0, 1, 0) - jnp.where(column & (y > 0), 1, 0))

    @pl.when(z < NZ - 1)
    def _():
        pl.semaphore_signal(barrier, inc=1, device_id=(e + NY, t), device_id_type=MESH)

    @pl.when(latecomer)
    def _():
        for yy in range(HY, NY):
            pl.semaphore_signal(late, inc=1, device_id=(yy, t), device_id_type=MESH)

    for zz in range(NZ - 1):
        @pl.when(zz < z)
        def _():
            pl.semaphore_signal(ready.at[z], inc=1, device_id=(zz * NY + y, t), device_id_type=MESH)

    for cp in table_copies:
        cp.wait()
    r0, r1 = routes_ref[0:1, :], routes_ref[1:2, :]
    w = mix_ref[...].astype(F32)
    w0, w1 = w[0:1, :], w[1:2, :]
    upper = (iota((tokn, tokn), 0) < iota((tokn, tokn), 1)).astype(BF)
    with jax.named_scope("share"):
        await_bytes(share, sh_sem)

    def tell_one(b, part, yd):
        zz = pl.ds(b * ZB, ZB)
        remote(
            msg.at[part, zz, yd, :, pl.ds(0, MSG)], ybuf.at[part, zz, y % HY, :, pl.ds(0, MSG)],
            y_send, y_recv.at[part, b], (z * NY + yd, t)).start()

    def tell_latecomer():
        pl.semaphore_wait(late, 1)
        for part in range(2):
            for b in range(GROUPS):
                tell_one(b, part, 0)

    @pl.when(active)
    def _():
        both = jnp.concatenate([share[part].reshape(2 * tokn, QUAD) for part in range(2)], axis=1)
        blk = ZB * NY * 16

        def fill(b):
            rw = iota((blk, tokn), 0) + b * blk
            ex = rw >> 4
            q = rw & 15
            h0, h1 = ex == r0, ex == r1
            hit = h0 | h1
            rk = dot(hit.astype(BF), upper)
            wt = jnp.where(h0, w0, 0.0) + jnp.where(h1, w1, 0.0)
            one = jnp.where(hit & (rk == q.astype(F32)) & (q < CAP), 1.0, 0.0)
            two = jnp.where(hit & (rk == (q - CAP).astype(F32)) & (q >= CAP), wt, 0.0)
            sel = jnp.concatenate([one.astype(BF), two.astype(BF)], axis=1)
            v = dot(sel, both).astype(BF)
            for part in range(2):
                for ch in range(4):
                    at = part * QUAD + ch * LANES
                    msg[part, pl.ds(b * ZB, ZB), :, ch] = v[:, at:at + LANES].reshape(ZB, NY, 16, LANES)

        def tell(b, part):
            zz = pl.ds(b * ZB, ZB)
            for d in (4, 3, 5, 2, 6, 1, 7):
                yd = lax.rem(y + d, NY)
                pl.when(jnp.logical_not(column & (yd == 0)))(functools.partial(tell_one, b, part, yd))
            ybuf[part, zz, y % HY] = msg[part, zz, y]

        for b in (0, 1):
            fill(b)
            tell(b, 0)

        @pl.when(z >= NZ // 2)
        def _():
            for b in (0, 1):
                tell(b, 1)

        for b in (2, 3):
            fill(b)
            tell(b, 0)

        @pl.when(z < NZ // 2)
        def _():
            for b in (0, 1):
                tell(b, 1)

        for b in (2, 3):
            tell(b, 1)

    await_bytes(w4.at[:, pl.ds(0, 3 * LANES)], w_sem)
    for cp in weight_moves:
        cp.start()

    def relay(b, part=0):
        with jax.named_scope(f"ywait{b}{'f' if part else ''}"):
            zz = pl.ds(b * ZB, ZB)

            @pl.when(active)
            def _():
                await_bytes(ybuf.at[part, zz, pl.ds(0, HY - 1), :, pl.ds(0, MSG)], y_recv.at[part, b])

            @pl.when(jnp.logical_not(active))
            def _():
                await_bytes(ybuf.at[part, zz, :, :, pl.ds(0, MSG)], y_recv.at[part, b])
        for zd in range(b * ZB, (b + 1) * ZB):
            @pl.when(zd == z)
            def _():
                zbuf[part, zd] = ybuf[part, zd]

            if part == 0:
                @pl.when(zd > z)
                def _():
                    with jax.named_scope(f"ready{zd}"):
                        pl.semaphore_wait(ready.at[zd], 1)

            @pl.when(zd != z)
            def _():
                remote(
                    ybuf.at[part, zd, :, :, pl.ds(0, MSG)], zbuf.at[part, z, :, :, pl.ds(0, MSG)],
                    z_send, z_recv.at[part, z // ZB], (zd * NY + y, t)).start()

    def unit(d, g):
        return rows.at[c, quad(d), :, pl.ds(g * RPG, RPG)]

    def to_sib(d, g):
        u = unit(d, g)
        remote(u, u, sib_send, sib_recv, sib).start()

    def landed(g, part):
        with jax.named_scope(f"zwait{g}{'f' if part else ''}"):
            @pl.when(z // ZB == g)
            def _():
                await_bytes(zbuf.at[part, pl.ds(0, ZB - 1), :, :, pl.ds(0, MSG)], z_recv.at[part, g])

            @pl.when(z // ZB != g)
            def _():
                await_bytes(zbuf.at[part, pl.ds(0, ZB), :, :, pl.ds(0, MSG)], z_recv.at[part, g])
        got = jnp.concatenate(
            [zbuf[part, pl.ds(g * ZB, ZB), :, ch].reshape(PER * 16, LANES) for ch in range(4)], axis=1)
        got = jnp.where((iota(got.shape, 0) & 15) < MSG, got, jnp.zeros_like(got))
        v = dot(perm[...], got)
        q = quad(2 * part)
        rows[c, q, 0, g * RPG:(g + 1) * RPG] = v[0:RPG].astype(BF)
        rows[c, q, 1, g * RPG:(g + 1) * RPG] = v[RPG:].astype(BF)

    def gather_out(g):
        landed(g, 0)
        u = unit(0, g)
        remote(u, u, ag_send, ag_recv.at[g], along_x(1)).start()
        remote(u, u, ag_send, ag_recv.at[g], along_x(-1)).start()
        to_sib(0, g)

    def gather_far(g):
        landed(g, 1)
        to_sib(2, g)

    def gather_in(g):
        await_bytes(rows.at[c, pl.ds(0, 2), :, pl.ds(g * RPG, RPG)], ag_recv.at[g])
        to_sib(-1, g)
        to_sib(1, g)

    def send_part(g, first, count, phase, to):
        at = (g, pl.ds(first, count), pl.ds(0, SENT))
        remote(sb.at[at], rb.at[at], rs_send, rs_recv.at[g, phase], along_x(to)).start()

    near, past = pl.ds(0, CUT), pl.ds(CUT, SENT - CUT)

    def products(g, d):
        at = pl.ds(g * RPG, RPG)
        q = quad(d)
        features = pl.ds(pl.multiple_of(q * QUAD, QUAD), QUAD)
        return dot(rows[c, q, 0, at], w4[features, :]), dot(rows[c, q, 1, at], dwt[features, :])

    def first_products(g, ds):
        each = [products(g, d) for d in ds]
        pre[g] = sum((a for a, _ in each[1:]), each[0][0])
        back[g] = sum((b for _, b in each[1:]), each[0][1])

    def compute(g, ds):
        at = pl.ds(g * RPG, RPG)
        pgu, bh = pre[g], back[g]
        for d in ds:
            a, b = products(g, d)
            pgu = pgu + a
            bh = bh + b
        pg = jnp.concatenate([pgu[:, 0:LANES], pgu[:, WIDE:WIDE + LANES]], axis=1)
        pu = jnp.concatenate([pgu[:, LANES:WIDE], pgu[:, WIDE + LANES:]], axis=1)
        sig = jax.nn.sigmoid(pg)
        act = pg * sig
        hidden = (act * pu).astype(BF)
        bg = (bh * pu * (sig * (1.0 + pg * (1.0 - sig)))).astype(BF)
        bu = (bh * act).astype(BF)
        b0 = jnp.concatenate([bg[:, 0:LANES], bu[:, 0:LANES]], axis=1)
        b1 = jnp.concatenate([bg[:, LANES:], bu[:, LANES:]], axis=1)
        b4 = jnp.concatenate([b0, b1], axis=1)
        hb = hidden.astype(F32) * bh
        hi = hb.astype(BF)
        lo = (hb - hi.astype(F32)).astype(BF)
        ones = jnp.ones((8, WIDE), BF)
        sums = dot_nt(ones, hi) + dot_nt(ones, lo)
        shi = sums.astype(BF).astype(F32)
        row = iota((8, RPG), 0)
        mixt[g, :, 0:RPG] = jnp.where(row == 0, shi, jnp.where(row == 1, sums - shi, 0.0))
        tile = mixt[g].astype(BF)
        def part(d):
            cols = pl.ds(pl.multiple_of(chip(d) * WIDE, WIDE), WIDE)
            return dot(b4, w4t[:, cols])

        def stored(d, i):
            v = part(d)
            sb[g, i, 0:RPG] = v[:, 0:LANES].astype(BF)
            sb[g, i, RPG:2 * RPG] = v[:, LANES:].astype(BF)
            sb[g, i, 2 * RPG:] = tile

        stored(4, 4)
        for rows_, to in ((near, 2), (past, -2)):
            remote(sb.at[g, 4, rows_], rb.at[g, 4, rows_], rs_send, rs_recv.at[g, 0], along_x(to)).start()
        for d, i, to in ((3, 0, 1), (5, 2, -1)):
            stored(d, i)
            stored(to % NX, i + 1)
            send_part(g, i, 2, 0, to)
        for d, i in ((2, 0), (6, 1), (0, 2)):
            v = part(d)
            pown[g, i, 0:RPG] = v[:, 0:LANES]
            pown[g, i, RPG:2 * RPG] = v[:, LANES:]
        first = c == 0
        bgu[c, at] = jnp.where(first, b0.astype(F32), b1.astype(F32)).astype(BF)
        obgu[g] = jnp.where(first, b1.astype(F32), b0.astype(F32)).astype(BF)
        hf = hidden.astype(F32)
        hid[c, at] = jnp.where(first, hf[:, 0:LANES], hf[:, LANES:]).astype(BF)
        ohid[g] = jnp.where(first, hf[:, LANES:], hf[:, 0:LANES]).astype(BF)
        remote(obgu.at[g], bgu.at[c, at], bh_send.at[0], bh_recv.at[0], sib).start()
        remote(ohid.at[g], hid.at[c, at], bh_send.at[1], bh_recv.at[1], sib).start()

    def chunk(g, i):
        return jnp.concatenate([pown[g, i], mixt[g]], axis=0)

    def scatter_two(g):
        await_bytes(rb.at[g, pl.ds(0, 5), pl.ds(0, SENT)], rs_recv.at[g, 0])
        v = chunk(g, 0) + rb[g, 0].astype(F32)
        sb[g, 5, 0:CUT] = (v[0:CUT] + rb[g, 4, 0:CUT].astype(F32)).astype(BF)
        sb[g, 5, CUT:] = v[CUT:].astype(BF)
        send_part(g, 5, 1, 1, 2)
        v = chunk(g, 1) + rb[g, 2].astype(F32)
        sb[g, 6, 0:CUT] = v[0:CUT].astype(BF)
        sb[g, 6, CUT:] = (v[CUT:] + rb[g, 4, CUT:].astype(F32)).astype(BF)
        send_part(g, 6, 1, 1, -2)

    def give_back(g):
        await_bytes(rb.at[g, pl.ds(0, 2), pl.ds(0, SENT)], rs_recv.at[g, 1])
        v = chunk(g, 2)
        for i in (1, 3, 5, 6):
            v = v + rb[g, i].astype(F32)
        sums = v[2 * RPG:2 * RPG + 1] + v[2 * RPG + 1:2 * RPG + 2]
        mhi = sums.astype(BF).astype(F32)
        mlo = sums - mhi
        br, bc = iota((LANES, LANES), 0), iota((LANES, LANES), 1)
        second = bc >= RPG
        row = bc - jnp.where(second, RPG, 0)
        src_of = div5(row)
        slot_of = row - src_of * CAP
        here = ((br >> 3) == src_of + jnp.where(second, PER, 0)) & (bc < 2 * RPG)
        spread = (here & ((br & 7) == slot_of))[:, 0:2 * RPG].astype(BF)
        take = (((br >> 3) & (PER - 1)) == div5(bc)) & ((br & 7) == CAP) & (bc < RPG)
        slot_r = br - div5(br) * CAP
        m = dot(spread, v[0:2 * RPG].astype(BF))
        m = m + dot(jnp.where(take, mhi, 0.0).astype(BF), (bc == slot_r).astype(BF))
        m = m + dot(jnp.where(take, mlo, 0.0).astype(BF), (bc == slot_r + 8).astype(BF))
        out[g] = m.astype(BF).reshape(2, PER, 8, LANES)
        for j in range(PER):
            i = (g * ZB + j // HY) * NY + mine_y * HY + j % HY
            for hf in range(2):
                here_ = (i == e) & (c == hf)

                @pl.when(here_)
                def _():
                    ret[e] = out[g, hf, j]

                @pl.when(jnp.logical_not(here_))
                def _():
                    remote(out.at[g, hf, j], ret.at[e], rt_send, rt_recv, (i, x * 2 + hf)).start()

    def grads():
        await_bytes(rows.at[1 - c], sib_recv)
        await_bytes(bgu.at[1 - c], bh_recv.at[0])
        await_bytes(hid.at[1 - c], bh_recv.at[1])
        for q in range(QUADS):
            at = slice(q * QUAD, (q + 1) * QUAD)
            v = dot_tn(rows[0, q, 0], bgu[0]) + dot_tn(rows[1, q, 0], bgu[1])
            gg_ref[at, :] = v[:, 0:LANES].astype(BF)
            ug_ref[at, :] = v[:, LANES:].astype(BF)
            dg_ref[:, at] = (dot_tn(hid[0], rows[0, q, 1]) + dot_tn(hid[1], rows[1, q, 1])).astype(BF)

    def turn():
        mixt[...] = jnp.zeros_like(mixt)
        pr, pc = iota((2 * RPG, 16 * PER), 0), iota((2 * RPG, 16 * PER), 1)
        second = pr >= RPG
        rest = pr - jnp.where(second, RPG, 0)
        src = div5(rest)
        perm[...] = (pc == src * 16 + (rest - src * CAP) + jnp.where(second, CAP, 0)).astype(BF)
        for cp in weight_moves:
            cp.wait_recv()
        for k in range(8):
            at = slice(k * WIDE, (k + 1) * WIDE)
            dwt[at, :] = dw[:, at].T
            for hf in range(2):
                w4t[hf * WIDE:(hf + 1) * WIDE, at] = w4[at, hf * WIDE:(hf + 1) * WIDE].T

    def tables():
        er = iota((nep, tokn), 0)
        oh0, oh1 = er == r0, er == r1
        ranks = dot((oh0 | oh1).astype(BF), upper)
        aux[0:1, :] = jnp.sum(jnp.where(oh0, ranks, 0.0), axis=0, keepdims=True)
        aux[1:2, :] = jnp.sum(jnp.where(oh1, ranks, 0.0), axis=0, keepdims=True)
        blk8 = 128
        for b in range(nep * 8 // blk8):
            rw = iota((blk8, tokn), 0) + b * blk8
            hit = ((rw >> 3) == r0) | ((rw >> 3) == r1)
            rk = dot(hit.astype(BF), upper)
            s = rw & 7
            p8[pl.ds(b * blk8, blk8), :] = (hit & (rk == s.astype(F32)) & (s < CAP)).astype(BF)
        aux[2:3, :] = w0
        aux[3:4, :] = w1
        aux[4:5, :] = r0.astype(F32)
        aux[5:6, :] = r1.astype(F32)
        aux[6:8, :] = jnp.zeros((2, tokn), F32)

    steps = {"A": gather_out, "B": gather_in, "H": gather_far, "E": scatter_two, "F": give_back}
    def run(plan):
        left = {}
        for step in " ".join(plan).split():
            kind, g = step[0], int(step[1:] or 0)
            with jax.named_scope(step):
                if kind == "r":
                    relay(g)
                elif kind == "f":
                    relay(g, 1)
                elif kind in "st":
                    pl.when((z < NZ // 4) == (kind == "s"))(functools.partial(relay, g))
                elif kind in "az":
                    pl.when(c == int(kind == "z"))(functools.partial(gather_out, g))
                elif kind == "D":
                    pl.when(column & active)(tell_latecomer)
                elif kind in "xy":
                    pl.when(c == int(kind == "y"))(functools.partial(give_back, g))
                elif kind == "P":
                    first_products(g, (0, 2))
                    left[g] = (-1, 1)
                elif kind == "Q":
                    first_products(g, (0, -1, 1))
                    left[g] = (2,)
                elif kind == "C":
                    compute(g, left[g])
                elif kind == "G":
                    grads()
                elif kind == "W":
                    turn()
                elif kind == "T":
                    tables()
                else:
                    steps[kind](g)

    early = z < NZ // 2
    pl.when(early)(functools.partial(run, EARLY))
    pl.when(jnp.logical_not(early))(functools.partial(run, LATE))

    for cp in weight_moves:
        cp.wait_send()

    @pl.when(active)
    def _():
        await_bytes(msg.at[:, :, pl.ds(0, NY - 1), :, pl.ds(0, MSG)], y_send)
        await_bytes(ret.at[pl.ds(0, nep - 1)], rt_send)

    @pl.when(jnp.logical_not(active))
    def _():
        await_bytes(ret, rt_send)

    await_bytes(zbuf.at[:, pl.ds(0, NZ - 1), :, :, pl.ds(0, MSG)], z_send)
    await_bytes(rows.at[0, pl.ds(0, 2)], ag_send)
    await_bytes(rows.at[0], sib_send)
    await_bytes(obgu, bh_send.at[0])
    await_bytes(ohid, bh_send.at[1])
    await_bytes(sb.at[:, :, pl.ds(0, SENT)], rs_send)

    with jax.named_scope("retwait"):
        @pl.when(active)
        def _():
            await_bytes(ret.at[pl.ds(0, nep - 1)], rt_recv)

        @pl.when(jnp.logical_not(active))
        def _():
            await_bytes(ret, rt_recv)


def finish(ret, p8, aux, gg, ug, dg, tg_ref, mg_ref, gg_out, ug_out, dg_out, tg, mg, sem):
    copies = [
        pltpu.make_async_copy(gg, gg_out.at[0], sem.at[0]),
        pltpu.make_async_copy(ug, ug_out.at[0], sem.at[1]),
        pltpu.make_async_copy(dg, dg_out.at[0], sem.at[2]),
    ]
    for cp in copies:
        cp.start()
    nep = ret.shape[0]
    tokn = p8.shape[1]
    back_rows = ret[...].reshape(nep * 8, LANES)
    tg[...] = dot_tn(p8[...], back_rows).astype(BF)
    copies.append(pltpu.make_async_copy(tg, tg_ref, sem.at[3]))
    copies[-1].start()
    sr, sc = iota((nep, nep * 8), 0), iota((nep, nep * 8), 1)
    mixes = dot((sc == sr * 8 + CAP).astype(BF), back_rows).astype(BF)
    lane = iota((LANES, tokn), 0).astype(F32)
    er = iota((nep, tokn), 0).astype(F32)
    done = []
    for k in range(2):
        seen = dot_tn(mixes, (er == aux[4 + k:5 + k, :]).astype(BF))
        rank = aux[k:k + 1, :]
        picked = jnp.where((lane == rank) | (lane == rank + 8.0), seen, 0.0)
        done.append(jnp.sum(picked, axis=0, keepdims=True) / aux[2 + k:3 + k, :])
    mg[...] = jnp.concatenate(done, axis=0).astype(BF)
    copies.append(pltpu.make_async_copy(mg, mg_ref, sem.at[4]))
    copies[-1].start()
    for cp in copies:
        cp.wait()


def solution(mesh):
    nep = NZ * NY

    def on_device(tokens, cotangent, mix_weights, routes, gate_proj, up_proj, down_proj):
        tokn, width = tokens.shape
        ff = gate_proj.shape[2]
        vm = pl.BlockSpec(memory_space=pltpu.VMEM)
        hbm = pl.BlockSpec(memory_space=pltpu.HBM)
        dma = pltpu.SemaphoreType.DMA
        parts = pl.pallas_call(
            kernel,
            out_shape=(
                jax.ShapeDtypeStruct((nep, 8, LANES), BF),
                jax.ShapeDtypeStruct((nep * 8, tokn), BF),
                jax.ShapeDtypeStruct((8, tokn), F32),
                jax.ShapeDtypeStruct((width, ff), BF),
                jax.ShapeDtypeStruct((width, ff), BF),
                jax.ShapeDtypeStruct((ff, width), BF),
            ),
            in_specs=[hbm] * 7,
            out_specs=[vm] * 6,
            scratch_shapes=[
                pltpu.VMEM((2, tokn), jnp.int32),
                pltpu.VMEM((2, tokn), BF),
                pltpu.VMEM((2, 2, tokn, QUAD), BF),
                pltpu.VMEM((2, NZ, NY, 4, 16, LANES), BF),
                pltpu.VMEM((2, NZ, HY, 4, 16, LANES), BF),
                pltpu.VMEM((2, NZ, HY, 4, 16, LANES), BF),
                pltpu.VMEM((2, QUADS, 2, GROUPS * RPG, QUAD), BF),
                pltpu.VMEM((width, 4 * LANES), BF),
                pltpu.VMEM((2 * ff, width), BF),
                pltpu.VMEM((4 * LANES, width), BF),
                pltpu.VMEM((width, 2 * ff), BF),
                pltpu.VMEM((2 * RPG, 16 * PER), BF),
                pltpu.VMEM((2, GROUPS * RPG, WIDE), BF),
                pltpu.VMEM((2, GROUPS * RPG, LANES), BF),
                pltpu.VMEM((GROUPS, RPG, WIDE), BF),
                pltpu.VMEM((GROUPS, RPG, LANES), BF),
                pltpu.VMEM((GROUPS, 8, LANES), F32),
                pltpu.VMEM((GROUPS, RPG, QUAD), F32),
                pltpu.VMEM((GROUPS, RPG, WIDE), F32),
                pltpu.VMEM((GROUPS, 3, 2 * RPG, LANES), F32),
                pltpu.VMEM((GROUPS, 7, TILE, LANES), BF),
                pltpu.VMEM((GROUPS, 7, TILE, LANES), BF),
                pltpu.VMEM((GROUPS, 2, PER, 8, LANES), BF),
                pltpu.SemaphoreType.REGULAR((NZ,)),
                pltpu.SemaphoreType.REGULAR,
                dma((2,)), dma, dma, dma((4,)), dma, dma((2, GROUPS)), dma, dma((2, GROUPS)),
                dma, dma((GROUPS,)), dma, dma,
                dma((2,)), dma((2,)), dma, dma((GROUPS, 2)), dma, dma,
            ],
            compiler_params=pltpu.CompilerParams(
                collective_id=0, has_side_effects=True, vmem_limit_bytes=52 * 1024 * 1024),
        )(*(
            pltpu.with_memory_space_constraint(a, pltpu.HBM)
            for a in (tokens, cotangent, routes.T, mix_weights.T, gate_proj, up_proj, down_proj)))
        tg, mg, gg, ug, dg = pl.pallas_call(
            finish,
            out_shape=(
                jax.ShapeDtypeStruct((tokn, LANES), BF),
                jax.ShapeDtypeStruct((2, tokn), BF),
                jax.ShapeDtypeStruct((1, width, ff), BF),
                jax.ShapeDtypeStruct((1, width, ff), BF),
                jax.ShapeDtypeStruct((1, ff, width), BF),
            ),
            in_specs=[vm] * 6,
            out_specs=[hbm] * 5,
            scratch_shapes=[pltpu.VMEM((tokn, LANES), BF), pltpu.VMEM((2, tokn), BF), dma((5,))],
            compiler_params=pltpu.CompilerParams(vmem_limit_bytes=8 * 1024 * 1024),
        )(*parts)
        return tg, mg.T, gg, ug, dg

    in_specs = (
        P("ep", None), P("ep", None), P("ep", None), P("ep", None),
        P("ep", None, "tp"), P("ep", None, "tp"), P("ep", "tp", None),
    )
    out_specs = (
        P("ep", "tp"), P("ep", None), P("ep", None, "tp"), P("ep", None, "tp"), P("ep", "tp", None),
    )
    return jax.shard_map(on_device, mesh=mesh, in_specs=in_specs, out_specs=out_specs, check_vma=False)
```
